32 devices in a mesh: fs: 16 (over z, y, core), tp: 2 (over x).
Axes of the slice: x: 2, y: 2, z: 4, core: 2. Of those that a mesh axis runs over, the one named last changes fastest.
Arguments:
- tokens: bfloat16 [16384, 2048], P(('fs', 'tp')), may hold values from -8 to 8
- pre_mix_gain: float32 [2048], replicated, may hold values from 0.1 to 1.9
- post_mix_gain: float32 [2048], replicated, may hold values from 0.1 to 1.9
- pre_ffn_gain: float32 [2048], replicated, may hold values from 0.1 to 1.9
- post_ffn_gain: float32 [2048], replicated, may hold values from 0.1 to 1.9
- w_branch: bfloat16 [2048, 1024], P('fs', 'tp'), may hold values from -0.125 to 0.125
- w_gelu: bfloat16 [2048, 1024], P('fs', 'tp'), may hold values from -0.125 to 0.125
- conv_weight: bfloat16 [4, 1024], P(None, 'tp'), may hold values from -3 to 3
- w_rec: bfloat16 [2, 8, 128, 128], P(None, 'tp'), may hold values from -0.5 to 0.5
- w_inp: bfloat16 [2, 8, 128, 128], P(None, 'tp'), may hold values from -0.5 to 0.5
- decay: float32 [2, 1024], P(None, 'tp'), may hold values from 3 to 10
- out_weight_t: bfloat16 [2048, 1024], P('fs', 'tp'), may hold values from -0.1875 to 0.1875
- w_gate: bfloat16 [2048, 3072], P('fs', 'tp'), may hold values from -0.125 to 0.125
- w_up: bfloat16 [2048, 3072], P('fs', 'tp'), may hold values from -0.125 to 0.125
- down_weight_t: bfloat16 [2048, 3072], P('fs', 'tp'), may hold values from -0.109375 to 0.109375
Outputs:
- layer_out: bfloat16 [16384, 2048], P(('fs', 'tp'))
The draws below stay inside these ranges and needn't reach their ends.
All inputs are finite; a program needn't handle non-finite values.
Results may differ from the reference program's by a relative error of at most 0.014.
Values may be sent and summed in bfloat16 or wider, within the bound.
A program may use at most 128 MiB of HBM per device.

```python
import math
import jax
import jax.numpy as jnp
from jax import lax

D = 2048
BLOCKS = 8
BW = 128
FF = 3072
SEQ_LEN = 1024
D_LRU = 1024
TOKENS = 16384
N_FS = 16
N_TP = 2


def draw_tokens(key, part):
    noise_key = jax.random.fold_in(key, 11)
    common_key = jax.random.fold_in(key, 12)
    block_count = (TOKENS + 15) // 16
    block_index = jnp.arange(TOKENS) // 16
    common = jax.random.normal(common_key, (block_count, D), jnp.float32)
    noise = jax.random.normal(noise_key, (TOKENS, D), jnp.float32)
    values = noise + 1.2 * common[block_index]
    return jnp.clip(values, -8.0, 8.0).astype(jnp.bfloat16)


def draw_decay(key, part):
    choose_key = jax.random.fold_in(key, 21)
    slow_key = jax.random.fold_in(key, 22)
    fast_key = jax.random.fold_in(key, 23)
    fast_share = 0.5
    fast = jax.random.uniform(choose_key, (2, D_LRU), jnp.float32) < fast_share
    slow_rate = jnp.exp(jax.random.uniform(slow_key, (2, D_LRU), jnp.float32, math.log(0.3), math.log(1.5))) / SEQ_LEN
    fast_rate = 1.0 / jnp.exp(jax.random.uniform(fast_key, (2, D_LRU), jnp.float32, math.log(15.0), math.log(50.0)))
    per_step = jnp.where(fast, fast_rate, slow_rate)
    return (-jnp.log(jnp.expm1(per_step / 4.0))).astype(jnp.float32)


def steps_of(rng, shape, cuts, smallest, high):
    level, own = 1.0, jax.random.fold_in(rng, 6)
    for dim, blocks in cuts:
        steps = jnp.exp(jax.random.uniform(jax.random.fold_in(own, dim), (blocks,), jnp.float32, smallest / len(cuts), high / len(cuts)))
        level = level * jnp.repeat(steps, shape[dim] // blocks).reshape([-1 if axis == dim else 1 for axis in range(len(shape))])
    return level


def gaussian(own_key, dims, deviation, reach, split=(), held_as=jnp.bfloat16):
    values = deviation * jax.random.normal(own_key, dims, jnp.float32)
    if split:
        values = values * steps_of(own_key, dims, split, -0.22, 0.18)
    return jnp.clip(values, -reach, reach).astype(held_as)


def setup_inputs(seed: int = 0) -> dict:
    key_list = jax.random.split(jax.random.key(seed), 16)
    return {
        "tokens": draw_tokens(jax.random.fold_in(key_list[15], 71), 0),
        "pre_mix_gain": jnp.clip(1.0 + 0.18 * jax.random.normal(key_list[1], (D,), jnp.float32), 0.1, 1.9),
        "post_mix_gain": jnp.clip(1.0 + 0.18 * jax.random.normal(key_list[2], (D,), jnp.float32), 0.1, 1.9),
        "pre_ffn_gain": jnp.clip(1.0 + 0.18 * jax.random.normal(key_list[3], (D,), jnp.float32), 0.1, 1.9),
        "post_ffn_gain": jnp.clip(1.0 + 0.18 * jax.random.normal(key_list[4], (D,), jnp.float32), 0.1, 1.9),
        "w_branch": gaussian(key_list[5], (D, D_LRU), D ** -0.5, 0.125, ((0, 16), (1, 2))),
        "w_gelu": gaussian(key_list[6], (D, D_LRU), D ** -0.5, 0.125, ((0, 16), (1, 2))),
        "conv_weight": gaussian(key_list[7], (4, D_LRU), 0.5, 3.0, ((1, 2),)),
        "w_rec": gaussian(key_list[8], (2, BLOCKS, BW, BW), BW ** -0.5, 0.5, ((1, 2),)),
        "w_inp": gaussian(key_list[9], (2, BLOCKS, BW, BW), BW ** -0.5, 0.5, ((1, 2),)),
        "decay": draw_decay(jax.random.fold_in(key_list[15], 71), 0),
        "out_weight_t": gaussian(key_list[11], (D, D_LRU), D_LRU ** -0.5, 0.1875, ((0, 16), (1, 2))),
        "w_gate": gaussian(key_list[12], (D, FF), D ** -0.5, 0.125, ((0, 16), (1, 2))),
        "w_up": gaussian(key_list[13], (D, FF), D ** -0.5, 0.125, ((0, 16), (1, 2))),
        "down_weight_t": gaussian(key_list[14], (D, FF), FF ** -0.5, 0.109375, ((0, 16), (1, 2))),
    }


EPS = 1e-06

def normed(values, gain):
    factor = lax.rsqrt(lax.optimization_barrier(jnp.mean(values * values, axis=-1, keepdims=True)) + EPS)
    return values * factor * gain

def conv_short(branch, conv_weight):
    length = branch.shape[0]
    padded = jnp.pad(branch.astype(jnp.float32), ((2, 1), (0, 0)))
    weights = conv_weight.astype(jnp.float32)
    summed = weights[0] * padded[0:length]
    for offset in range(1, 4):
        summed = summed + weights[offset] * padded[offset:offset + length]
    return summed.astype(jnp.bfloat16)

def combine(earlier, later):
    return (earlier[0] * later[0], later[0] * earlier[1] + later[1])

def recurrence(conv_out, w_rec, w_inp, decay):
    length, channels = conv_out.shape
    blocks = w_rec.shape[0]
    grouped = conv_out.astype(jnp.float32).reshape(length, blocks, channels // blocks)
    rate_gate = jax.nn.sigmoid(jnp.einsum('lnc,ncd->lnd', grouped, w_rec.astype(jnp.float32)).reshape(length, channels))
    inflow = jax.nn.sigmoid(jnp.einsum('lnc,ncd->lnd', grouped, w_inp.astype(jnp.float32)).reshape(length, channels))
    log_retain = -8.0 * rate_gate * jax.nn.softplus(-decay)
    retain = jnp.exp(log_retain)
    feed = jnp.sqrt(-jnp.expm1(2.0 * log_retain)) * inflow * conv_out.astype(jnp.float32)
    unused_decay, states = lax.associative_scan(combine, (retain, feed), axis=0)
    return states

def grouped_sum(hidden, weight_t):
    group_cols = hidden.shape[1] // N_TP

    def add_group(index, summed):
        first_col = (index * group_cols).astype(jnp.int32)
        part_rows = lax.dynamic_slice_in_dim(hidden, first_col, group_cols, 1)
        part_cols = lax.dynamic_slice_in_dim(weight_t, first_col, group_cols, 1)
        partial_value = lax.dot_general(part_rows, part_cols, (((1,), (1,)), ((), ())), preferred_element_type=jnp.float32)
        rounded = lax.optimization_barrier(partial_value.astype(jnp.bfloat16))
        return summed + rounded.astype(jnp.float32)
    zero_block = jnp.zeros((hidden.shape[0], weight_t.shape[0]), jnp.float32)
    return lax.fori_loop(0, N_TP, add_group, zero_block)

def reference(tokens, pre_mix_gain, post_mix_gain, pre_ffn_gain, post_ffn_gain, w_branch, w_gelu, conv_weight, w_rec, w_inp, decay, out_weight_t, w_gate, w_up, down_weight_t):

    def one_sequence(seq_tokens):
        stream = seq_tokens.astype(jnp.float32)
        normed_in = normed(stream, pre_mix_gain).astype(jnp.bfloat16)
        branch_in = jnp.dot(normed_in, w_branch, preferred_element_type=jnp.float32).astype(jnp.bfloat16)
        gelu_in = jnp.dot(normed_in, w_gelu, preferred_element_type=jnp.float32).astype(jnp.bfloat16)
        conv_out = conv_short(branch_in, conv_weight)
        forward = recurrence(conv_out, w_rec[0], w_inp[0], decay[0])
        backward = jnp.flip(recurrence(jnp.flip(conv_out, 0), w_rec[1], w_inp[1], decay[1]), 0)
        mixer_hidden = (jax.nn.gelu(gelu_in.astype(jnp.float32)) * (forward + backward)).astype(jnp.bfloat16)
        mixer_sum = lax.dot_general(mixer_hidden, out_weight_t, (((1,), (1,)), ((), ())), preferred_element_type=jnp.float32)
        residual = (stream + normed(mixer_sum, post_mix_gain)).astype(jnp.bfloat16)
        middle = residual.astype(jnp.float32)
        normed_mid = normed(middle, pre_ffn_gain).astype(jnp.bfloat16)
        gate_proj = jnp.dot(normed_mid, w_gate, preferred_element_type=jnp.float32)
        up_proj = jnp.dot(normed_mid, w_up, preferred_element_type=jnp.float32)
        ffn_hidden = (jax.nn.silu(gate_proj) * up_proj).astype(jnp.bfloat16)
        ffn_sum = grouped_sum(ffn_hidden, down_weight_t)
        return (middle + normed(ffn_sum, post_ffn_gain)).astype(jnp.bfloat16)
    sequences = tokens.reshape(N_FS, SEQ_LEN, D)
    outputs = lax.map(one_sequence, sequences)
    return outputs.reshape(N_FS * SEQ_LEN, D)
```

```python
import functools

import jax
import jax.numpy as jnp
from jax import lax
from jax.experimental import pallas as pl
from jax.experimental.pallas import tpu as pltpu
from jax.sharding import PartitionSpec as P

EPS = 1e-06
SEGMENTS = 8
DOWN_PIECES = 2
VMEM_BYTES = 60 * 1024 * 1024


def normed(values, gain):
    factor = lax.rsqrt(jnp.mean(values * values, axis=-1, keepdims=True) + EPS)
    return values * factor * gain


def one_minus_exp(y, exp_y):
    series = 1.0 + y * (1.0 / 8.0)
    for order in (7, 6, 5, 4, 3, 2):
        series = 1.0 + y * (1.0 / order) * series
    return jnp.where(y > -0.5, -y * series, 1.0 - exp_y)


def mixer_kernel(
    x_ref, wb_ref, wg_ref, conv_ref, gates_ref, coef_ref, out_ref, pad, gel, a0, u0, a1, u1
):
    length, width = out_ref.shape
    group = gates_ref.shape[1]
    rows = 256
    pad[0:8, :] = jnp.zeros((8, width), jnp.float32)
    pad[8 + length : 16 + length, :] = jnp.zeros((8, width), jnp.float32)
    sources = ((x_ref, 0),)
    for source, base in sources:
        for start in range(0, source.shape[0], rows):
            piece = source[start : start + rows, :]
            branch = jnp.dot(piece, wb_ref[...], preferred_element_type=jnp.float32)
            gelu_in = jnp.dot(piece, wg_ref[...], preferred_element_type=jnp.float32)
            at = pl.multiple_of(base + start, rows)
            pad[pl.ds(8 + at, rows), :] = branch.astype(jnp.bfloat16).astype(jnp.float32)
            gel[pl.ds(at, rows), :] = jax.nn.gelu(
                gelu_in.astype(jnp.bfloat16).astype(jnp.float32)
            )

    for part in range(width // group):
        cols = slice(part * group, (part + 1) * group)
        taps = conv_ref[:, cols].astype(jnp.float32)
        coef = coef_ref[:, cols]
        for start in range(0, length, rows):
            summed = taps[0:1] * pad[6 + start : 6 + start + rows, cols]
            for j in range(1, 4):
                summed = summed + taps[j : j + 1] * pad[6 + j + start : 6 + j + start + rows, cols]
            conv = summed.astype(jnp.bfloat16)
            wide = conv.astype(jnp.float32)
            for d, (a_ref, u_ref) in enumerate(((a0, u0), (a1, u1))):
                gate = jnp.dot(
                    conv,
                    gates_ref[part, :, 2 * d * group : 2 * (d + 1) * group],
                    preferred_element_type=jnp.float32,
                )
                rate = jax.nn.sigmoid(gate[:, :group])
                inflow = jax.nn.sigmoid(gate[:, group:])
                log_retain = rate * coef[d : d + 1]
                retain = jnp.exp(log_retain)
                left = one_minus_exp(2.0 * log_retain, retain * retain)
                a_ref[part, start : start + rows, :] = retain
                u_ref[part, start : start + rows, :] = jnp.sqrt(left) * inflow * wide

    steps = length // SEGMENTS

    def step(t, carry):
        out = []
        for (state, decayed), (a_ref, u_ref), at in (
            (carry[0], (a0, u0), t),
            (carry[1], (a1, u1), steps - 1 - t),
        ):
            where = pl.ds(at, SEGMENTS, stride=steps)
            nstate, ndecayed = [], []
            for c in range(n):
                retain = a_ref[c, where, :]
                h = retain * state[c] + u_ref[c, where, :]
                p = retain * decayed[c]
                u_ref[c, where, :] = h
                a_ref[c, where, :] = p
                nstate.append(h)
                ndecayed.append(p)
            out.append((tuple(nstate), tuple(ndecayed)))
        return tuple(out)

    n = width // group
    zero = tuple(jnp.zeros((SEGMENTS, group), jnp.float32) for c in range(n))
    one = tuple(jnp.ones((SEGMENTS, group), jnp.float32) for c in range(n))
    ended = lax.fori_loop(0, steps, step, ((zero, one), (zero, one)), unroll=8)
    for c in range(n):
        lanes = slice(c * group, (c + 1) * group)
        blank = jnp.zeros((1, group), jnp.float32)
        entry = [[None] * SEGMENTS, [None] * SEGMENTS]
        for d, order in ((0, range(SEGMENTS)), (1, range(SEGMENTS - 1, -1, -1))):
            carry = blank
            for s in order:
                entry[d][s] = carry
                carry = ended[d][0][c][s : s + 1] + ended[d][1][c][s : s + 1] * carry
        for s in range(SEGMENTS):
            span = slice(s * steps, (s + 1) * steps)
            forward = u0[c, span, :] + a0[c, span, :] * entry[0][s]
            backward = u1[c, span, :] + a1[c, span, :] * entry[1][s]
            out_ref[span, lanes] = (gel[span, lanes] * (forward + backward)).astype(jnp.bfloat16)


def mixer(x, weights, conv_weight, w_rec, w_inp, decay):
    length, model = x.shape
    channels = conv_weight.shape[1]
    group = w_rec.shape[2]
    width = min(256, channels)
    count = channels // width
    gates = jnp.concatenate([w_rec[0], w_inp[0], w_rec[1], w_inp[1]], axis=-1)
    coef = -8.0 * jax.nn.softplus(-decay)
    f32 = functools.partial(pltpu.VMEM, dtype=jnp.float32)
    return pl.pallas_call(
        mixer_kernel,
        grid=(count,),
        out_shape=jax.ShapeDtypeStruct((length, channels), jnp.bfloat16),
        in_specs=[
            pl.BlockSpec((length, model), lambda j: (0, 0)),
            pl.BlockSpec((model, width), lambda j: (0, j)),
            pl.BlockSpec((model, width), lambda j: (0, count + j)),
            pl.BlockSpec((4, width), lambda j: (0, j)),
            pl.BlockSpec((width // group, group, 4 * group), lambda j: (j, 0, 0)),
            pl.BlockSpec((2, width), lambda j: (0, j)),
        ],
        out_specs=pl.BlockSpec((length, width), lambda j: (0, j)),
        scratch_shapes=[f32((length + 16, width)), f32((length, width))]
        + [f32((width // group, length, group)) for i in range(4)],
        compiler_params=pltpu.CompilerParams(vmem_limit_bytes=VMEM_BYTES),
        cost_estimate=pl.CostEstimate(
            flops=4 * length * model * channels + 16 * length * group * channels * 8,
            bytes_accessed=2 * (length * model + 2 * model * channels + length * channels),
            transcendentals=12 * length * channels,
        ),
    )(x, weights, weights, conv_weight, gates, coef)


def ffn_kernel(x_ref, gate_ref, up_ref, down_ref, out_ref, total):
    step = pl.program_id(0)
    gate = jnp.dot(x_ref[...], gate_ref[...], preferred_element_type=jnp.float32)
    up = jnp.dot(x_ref[...], up_ref[...], preferred_element_type=jnp.float32)
    hidden = (jax.nn.silu(gate) * up).astype(jnp.bfloat16)
    partial = lax.dot_general(
        hidden, down_ref[...], (((1,), (1,)), ((), ())), preferred_element_type=jnp.float32
    )

    @pl.when(step == 0)
    def _():
        total[...] = partial

    @pl.when(step > 0)
    def _():
        total[...] += partial

    @pl.when(step == pl.num_programs(0) - 1)
    def _():
        out_ref[...] = total[...].astype(jnp.bfloat16)


def ffn(x, weights):
    rows, model = x.shape
    units = weights.shape[1] // 3
    width = 256 if units % 256 == 0 else 128
    count = units // width
    return pl.pallas_call(
        ffn_kernel,
        grid=(count,),
        out_shape=jax.ShapeDtypeStruct((rows, model), jnp.bfloat16),
        in_specs=[
            pl.BlockSpec((rows, model), lambda j: (0, 0)),
            pl.BlockSpec((model, width), lambda j: (0, j)),
            pl.BlockSpec((model, width), lambda j: (0, count + j)),
            pl.BlockSpec((model, width), lambda j: (0, 2 * count + j)),
        ],
        out_specs=pl.BlockSpec((rows, model), lambda j: (0, 0)),
        scratch_shapes=[pltpu.VMEM((rows, model), jnp.float32)],
        compiler_params=pltpu.CompilerParams(vmem_limit_bytes=VMEM_BYTES),
        cost_estimate=pl.CostEstimate(
            flops=6 * rows * model * units,
            bytes_accessed=2 * (2 * rows * model + 3 * model * units),
            transcendentals=rows * units,
        ),
    )(x, weights, weights, weights)


def swap(values):
    return lax.ppermute(values, "tp", [(0, 1), (1, 0)])


def matmul_t(rows, weight_t):
    return lax.dot_general(
        rows, weight_t, (((1,), (1,)), ((), ())), preferred_element_type=jnp.float32
    )


def project_kernel(x_ref, gain_ref, weight_ref, branch_ref, gel_ref):
    width = branch_ref.shape[1]
    x = normed(x_ref[...].astype(jnp.float32), gain_ref[...]).astype(jnp.bfloat16)
    both = jnp.dot(x, weight_ref[...], preferred_element_type=jnp.float32)
    branch_ref[...] = both[:, :width].astype(jnp.bfloat16)
    gelu_in = both[:, width:].astype(jnp.bfloat16).astype(jnp.float32)
    gel_ref[...] = jax.nn.gelu(gelu_in).astype(jnp.bfloat16)


def project(tokens, gain, weights):
    rows, model = tokens.shape
    channels = weights.shape[1] // 2
    block = min(256, rows)
    return pl.pallas_call(
        project_kernel,
        grid=(rows // block,),
        out_shape=(jax.ShapeDtypeStruct((rows, channels), jnp.bfloat16),) * 2,
        in_specs=[
            pl.BlockSpec((block, model), lambda i: (i, 0)),
            pl.BlockSpec((1, model), lambda i: (0, 0)),
            pl.BlockSpec((model, 2 * channels), lambda i: (0, 0)),
        ],
        out_specs=(pl.BlockSpec((block, channels), lambda i: (i, 0)),) * 2,
        compiler_params=pltpu.CompilerParams(vmem_limit_bytes=VMEM_BYTES),
        cost_estimate=pl.CostEstimate(
            flops=4 * rows * model * channels,
            bytes_accessed=2 * (rows * model + 2 * model * channels + 2 * rows * channels),
            transcendentals=rows * channels,
        ),
    )(tokens, gain.reshape(1, model), weights)


def scan_kernel(
    own_b, peer_b, own_g, peer_g, conv_ref, gates_ref, coef_ref, out_ref, pad, gel_ref, a0, u0, a1, u1
):
    half, width = own_b.shape
    length = 2 * half
    group = gates_ref.shape[1]
    rows = 256
    place = lax.axis_index("tp")
    pad[0:8, :] = jnp.zeros((8, width), jnp.float32)
    pad[8 + length : 16 + length, :] = jnp.zeros((8, width), jnp.float32)
    for source, base in ((own_b, place * half), (peer_b, (1 - place) * half)):
        at = pl.multiple_of(base, half)
        pad[pl.ds(8 + at, half), :] = source[...].astype(jnp.float32)

    gel_ref[0] = own_g[...]
    gel_ref[1] = peer_g[...]

    for part in range(width // group):
        cols = slice(part * group, (part + 1) * group)
        taps = conv_ref[:, cols].astype(jnp.float32)
        coef = coef_ref[:, cols]
        for start in range(0, length, rows):
            summed = taps[0:1] * pad[6 + start : 6 + start + rows, cols]
            for j in range(1, 4):
                summed = summed + taps[j : j + 1] * pad[6 + j + start : 6 + j + start + rows, cols]
            conv = summed.astype(jnp.bfloat16)
            wide = conv.astype(jnp.float32)
            for d, (a_ref, u_ref) in enumerate(((a0, u0), (a1, u1))):
                gate = jnp.dot(
                    conv,
                    gates_ref[part, :, 2 * d * group : 2 * (d + 1) * group],
                    preferred_element_type=jnp.float32,
                )
                rate = jax.nn.sigmoid(gate[:, :group])
                inflow = jax.nn.sigmoid(gate[:, group:])
                log_retain = rate * coef[d : d + 1]
                retain = jnp.exp(log_retain)
                left = one_minus_exp(2.0 * log_retain, retain * retain)
                a_ref[part, start : start + rows, :] = retain
                u_ref[part, start : start + rows, :] = jnp.sqrt(left) * inflow * wide

    steps = length // SEGMENTS

    def step(t, carry):
        out = []
        for (state, decayed), (a_ref, u_ref), at in (
            (carry[0], (a0, u0), t),
            (carry[1], (a1, u1), steps - 1 - t),
        ):
            where = pl.ds(at, SEGMENTS, stride=steps)
            nstate, ndecayed = [], []
            for c in range(n):
                retain = a_ref[c, where, :]
                h = retain * state[c] + u_ref[c, where, :]
                p = retain * decayed[c]
                u_ref[c, where, :] = h
                a_ref[c, where, :] = p
                nstate.append(h)
                ndecayed.append(p)
            out.append((tuple(nstate), tuple(ndecayed)))
        return tuple(out)

    n = width // group
    zero = tuple(jnp.zeros((SEGMENTS, group), jnp.float32) for c in range(n))
    one = tuple(jnp.ones((SEGMENTS, group), jnp.float32) for c in range(n))
    ended = lax.fori_loop(0, steps, step, ((zero, one), (zero, one)), unroll=8)
    per_half = SEGMENTS // 2
    for c in range(n):
        lanes = slice(c * group, (c + 1) * group)
        blank = jnp.zeros((1, group), jnp.float32)
        entry = [[None] * SEGMENTS, [None] * SEGMENTS]
        for d, order in ((0, range(SEGMENTS)), (1, range(SEGMENTS - 1, -1, -1))):
            carry = blank
            for s in order:
                entry[d][s] = carry
                carry = ended[d][0][c][s : s + 1] + ended[d][1][c][s : s + 1] * carry
        for s in range(SEGMENTS):
            span = slice(s * steps, (s + 1) * steps)
            side = s // per_half
            local = slice((s % per_half) * steps, (s % per_half + 1) * steps)
            which = jnp.where(place == side, 0, 1)
            forward = u0[c, span, :] + a0[c, span, :] * entry[0][s]
            backward = u1[c, span, :] + a1[c, span, :] * entry[1][s]
            gel = gel_ref[which, local, lanes].astype(jnp.float32)
            out_ref[which, local, lanes] = (gel * (forward + backward)).astype(jnp.bfloat16)


def gated_scan(own, peer, block, width, conv_weight, gates, coef):
    half = own[0].shape[0]
    length = 2 * half
    group = gates.shape[1]
    f32 = functools.partial(pltpu.VMEM, dtype=jnp.float32)
    rows_spec = pl.BlockSpec((half, width), lambda i: (0, block))
    return pl.pallas_call(
        scan_kernel,
        grid=(1,),
        out_shape=jax.ShapeDtypeStruct((2, half, width), jnp.bfloat16),
        in_specs=[
            rows_spec,
            rows_spec,
            rows_spec,
            rows_spec,
            pl.BlockSpec((4, width), lambda i: (0, block)),
            pl.BlockSpec((width // group, group, 4 * group), lambda i: (block, 0, 0)),
            pl.BlockSpec((2, width), lambda i: (0, block)),
        ],
        out_specs=pl.BlockSpec((2, half, width), lambda i: (0, 0, 0)),
        scratch_shapes=[f32((length + 16, width)), pltpu.VMEM((2, half, width), jnp.bfloat16)]
        + [f32((width // group, length, group)) for i in range(4)],
        compiler_params=pltpu.CompilerParams(vmem_limit_bytes=VMEM_BYTES),
        cost_estimate=pl.CostEstimate(
            flops=80 * length * group * width,
            bytes_accessed=6 * length * width,
            transcendentals=12 * length * width,
        ),
    )(own[0], peer[0], own[1], peer[1], conv_weight, gates, coef)


def mix_out_kernel(
    keep, ha, hb, ra, rb, own_ref, near_ref, far_ref, tokens_ref, post_ref, pre_ref, *rest
):
    total = rest[-1]
    span = near_ref.shape[0]
    core = lax.axis_index("fs") % 2
    width = ha.shape[2]
    total[...] = matmul_t(ha[0], own_ref[:, :width]) + matmul_t(hb[0], own_ref[:, width:])
    for part, at in ((near_ref, core * span), (far_ref, (1 - core) * span)):
        cols = pl.ds(pl.multiple_of(at, span), span)
        total[:, cols] += matmul_t(ra[0], part[:, :width]) + matmul_t(rb[0], part[:, width:])
    stream = tokens_ref[...].astype(jnp.float32)
    residual = (stream + normed(total[...], post_ref[...])).astype(jnp.bfloat16)
    if keep:
        rest[1][...] = residual
    rest[0][...] = normed(residual.astype(jnp.float32), pre_ref[...]).astype(jnp.bfloat16)


def mix_out(keep, hidden, came, out_own, near, far, tokens, post_gain, pre_gain):
    rows, model = tokens.shape
    width = hidden[0].shape[2]
    channels = out_own.shape[1]
    block = min(256, rows)
    mine, theirs = (0, 1) if keep else (1, 0)
    h_spec = pl.BlockSpec((1, block, width), lambda i: (mine, i, 0))
    r_spec = pl.BlockSpec((1, block, width), lambda i: (theirs, i, 0))
    row_spec = pl.BlockSpec((block, model), lambda i: (i, 0))
    gain_spec = pl.BlockSpec((1, model), lambda i: (0, 0))
    half_spec = pl.BlockSpec((model // 2, channels), lambda i: (0, 0))
    shape = jax.ShapeDtypeStruct((rows, model), jnp.bfloat16)
    count = 2 if keep else 1
    return pl.pallas_call(
        functools.partial(mix_out_kernel, keep),
        grid=(rows // block,),
        out_shape=(shape,) * count,
        in_specs=[
            h_spec,
            h_spec,
            r_spec,
            r_spec,
            pl.BlockSpec((model, channels), lambda i: (0, 0)),
            half_spec,
            half_spec,
            row_spec,
            gain_spec,
            gain_spec,
        ],
        out_specs=(row_spec,) * count,
        scratch_shapes=[pltpu.VMEM((block, model), jnp.float32)],
        compiler_params=pltpu.CompilerParams(vmem_limit_bytes=VMEM_BYTES),
        cost_estimate=pl.CostEstimate(
            flops=4 * rows * model * channels,
            bytes_accessed=2 * (3 * rows * model + 2 * model * channels),
            transcendentals=rows,
        ),
    )(
        *hidden,
        *came,
        out_own,
        near,
        far,
        tokens,
        post_gain.reshape(1, model),
        pre_gain.reshape(1, model),
    )


def expand_kernel(x_ref, gate_ref, up_ref, out_ref):
    gate = jnp.dot(x_ref[...], gate_ref[...], preferred_element_type=jnp.float32)
    up = jnp.dot(x_ref[...], up_ref[...], preferred_element_type=jnp.float32)
    out_ref[...] = (jax.nn.silu(gate) * up).astype(jnp.bfloat16)


def expand(x, weights):
    rows, model = x.shape
    units = weights.shape[1] // 2
    width = 256 if units % 256 == 0 else 128
    count = units // width
    return pl.pallas_call(
        expand_kernel,
        grid=(count,),
        out_shape=jax.ShapeDtypeStruct((rows, units), jnp.bfloat16),
        in_specs=[
            pl.BlockSpec((rows, model), lambda j: (0, 0)),
            pl.BlockSpec((model, width), lambda j: (0, j)),
            pl.BlockSpec((model, width), lambda j: (0, count + j)),
        ],
        out_specs=pl.BlockSpec((rows, width), lambda j: (0, j)),
        compiler_params=pltpu.CompilerParams(vmem_limit_bytes=VMEM_BYTES),
        cost_estimate=pl.CostEstimate(
            flops=4 * rows * model * units,
            bytes_accessed=2 * (rows * model + 2 * model * units + rows * units),
            transcendentals=rows * units,
        ),
    )(x, weights, weights)


def contract_kernel(x_ref, weight_ref, out_ref):
    out_ref[...] = matmul_t(x_ref[...], weight_ref[...]).astype(jnp.bfloat16)


def contract(x, weight_t):
    rows, units = x.shape
    model = weight_t.shape[0]
    width = min(256, model)
    return pl.pallas_call(
        contract_kernel,
        grid=(model // width,),
        out_shape=jax.ShapeDtypeStruct((rows, model), jnp.bfloat16),
        in_specs=[
            pl.BlockSpec((rows, units), lambda j: (0, 0)),
            pl.BlockSpec((width, units), lambda j: (j, 0)),
        ],
        out_specs=pl.BlockSpec((rows, width), lambda j: (0, j)),
        compiler_params=pltpu.CompilerParams(vmem_limit_bytes=VMEM_BYTES),
        cost_estimate=pl.CostEstimate(
            flops=2 * rows * model * units,
            bytes_accessed=2 * (rows * model + model * units + rows * units),
            transcendentals=0,
        ),
    )(x, weight_t)


def finish_kernel(pieces, size, *refs):
    own, back = refs[:pieces], refs[pieces : 2 * pieces]
    residual_ref, gain_ref, out_ref, total = refs[2 * pieces :]
    model = total.shape[1]
    shards = model // (pieces * size)
    for piece in range(pieces):
        summed = own[piece][...].astype(jnp.float32) + back[piece][...].astype(jnp.float32)
        for shard in range(shards):
            at = (shard * pieces + piece) * size
            total[:, at : at + size] = summed[:, shard * size : (shard + 1) * size]
    middle = residual_ref[...].astype(jnp.float32)
    out_ref[...] = (middle + normed(total[...], gain_ref[...])).astype(jnp.bfloat16)


def finish(own, back, size, residual, gain):
    rows, model = residual.shape
    pieces = len(own)
    block = min(128, rows)
    part_spec = pl.BlockSpec((block, model // pieces), lambda i: (i, 0))
    row_spec = pl.BlockSpec((block, model), lambda i: (i, 0))
    return pl.pallas_call(
        functools.partial(finish_kernel, pieces, size),
        grid=(rows // block,),
        out_shape=jax.ShapeDtypeStruct((rows, model), jnp.bfloat16),
        in_specs=[part_spec] * (2 * pieces) + [row_spec, pl.BlockSpec((1, model), lambda i: (0, 0))],
        out_specs=row_spec,
        scratch_shapes=[pltpu.VMEM((block, model), jnp.float32)],
        compiler_params=pltpu.CompilerParams(vmem_limit_bytes=VMEM_BYTES),
        cost_estimate=pl.CostEstimate(
            flops=8 * rows * model, bytes_accessed=8 * rows * model, transcendentals=rows
        ),
    )(*own, *back, residual, gain.reshape(1, model))


def paired_device(
    tokens,
    pre_mix_gain,
    post_mix_gain,
    pre_ffn_gain,
    post_ffn_gain,
    w_branch,
    w_gelu,
    conv_weight,
    w_rec,
    w_inp,
    decay,
    out_weight_t,
    w_gate,
    w_up,
    down_weight_t,
):
    channels = conv_weight.shape[1]
    core = lax.axis_index("fs") % 2
    fs_size = lax.axis_size("fs")
    gather = functools.partial(lax.all_gather, axis_name="fs", axis=0, tiled=True)
    other = swap(tokens)
    mix_all = gather(jnp.concatenate([w_branch, w_gelu], axis=1))
    out_own = gather(out_weight_t)
    up_all = gather(jnp.concatenate([w_gate, w_up], axis=1))
    size = down_weight_t.shape[0] // DOWN_PIECES
    down_all = [gather(down_weight_t[i * size : (i + 1) * size]) for i in range(DOWN_PIECES)]
    gates = jnp.concatenate([w_rec[0], w_inp[0], w_rec[1], w_inp[1]], axis=-1)
    coef = -8.0 * jax.nn.softplus(-decay)

    own = project(tokens, pre_mix_gain, mix_all)
    other, own, out_own = lax.optimization_barrier((other, own, out_own))
    span = out_own.shape[0] // 2
    partners = [(i, i + 1 - 2 * (i % 2)) for i in range(fs_size)]
    near = swap(lax.dynamic_slice_in_dim(out_own, core * span, span, 0))
    peer = project(other, pre_mix_gain, mix_all)
    width = min(256, channels)
    hidden, came = [], []
    for block in range(channels // width):
        hidden.append(gated_scan(own, peer, block, width, conv_weight, gates, coef))
        came.append(swap(hidden[-1]))
    far = lax.ppermute(near, "fs", partners)
    shared = (hidden, came, out_own, near, far)
    (away_mid,) = mix_out(False, *shared, other, post_mix_gain, pre_ffn_gain)
    away_hidden = expand(away_mid, up_all)
    back = []
    for piece in down_all:
        back.append(swap(contract(away_hidden, piece)))
    own_mid, residual = mix_out(True, *shared, tokens, post_mix_gain, pre_ffn_gain)
    own_hidden = expand(own_mid, up_all)
    kept = [contract(own_hidden, piece) for piece in down_all]
    return finish(kept, back, size, residual, post_ffn_gain)


def wide_device(
    tokens,
    pre_mix_gain,
    post_mix_gain,
    pre_ffn_gain,
    post_ffn_gain,
    w_branch,
    w_gelu,
    conv_weight,
    w_rec,
    w_inp,
    decay,
    out_weight_t,
    w_gate,
    w_up,
    down_weight_t,
):
    channels = conv_weight.shape[1]
    mix_shard = jnp.concatenate([w_branch, w_gelu, out_weight_t], axis=1)
    ffn_shard = jnp.concatenate([w_gate, w_up, down_weight_t], axis=1)
    stream = tokens.astype(jnp.float32)
    normed_in = normed(stream, pre_mix_gain).astype(jnp.bfloat16)
    mix_all = lax.all_gather(mix_shard, "fs", axis=0, tiled=True)
    whole = lax.all_gather(normed_in, "tp", axis=0, tiled=True)
    ffn_all = lax.all_gather(ffn_shard, "fs", axis=0, tiled=True)
    out_own = mix_all[:, 2 * channels :]
    hidden = mixer(whole, mix_all, conv_weight, w_rec, w_inp, decay)
    own_hidden = lax.all_to_all(hidden, "tp", split_axis=0, concat_axis=1, tiled=True)
    out_whole = lax.all_gather(out_own, "tp", axis=1, tiled=True)
    mixer_sum = matmul_t(own_hidden, out_whole)
    residual = (stream + normed(mixer_sum, post_mix_gain)).astype(jnp.bfloat16)
    middle = residual.astype(jnp.float32)
    normed_mid = normed(middle, pre_ffn_gain).astype(jnp.bfloat16)
    all_mid = lax.all_gather(normed_mid, "tp", axis=0, tiled=True)
    ffn_sum = lax.psum_scatter(
        ffn(all_mid, ffn_all), "tp", scatter_dimension=0, tiled=True
    ).astype(jnp.float32)
    return (middle + normed(ffn_sum, post_ffn_gain)).astype(jnp.bfloat16)


def solution(mesh):
    return jax.shard_map(
        paired_device if mesh.shape["tp"] == 2 else wide_device,
        mesh=mesh,
        in_specs=(
            P(("fs", "tp"), None),
            P(),
            P(),
            P(),
            P(),
            P("fs", "tp"),
            P("fs", "tp"),
            P(None, "tp"),
            P(None, "tp", None, None),
            P(None, "tp", None, None),
            P(None, "tp"),
            P("fs", "tp"),
            P("fs", "tp"),
            P("fs", "tp"),
            P("fs", "tp"),
        ),
        out_specs=P(("fs", "tp"), None),
        check_vma=False,
    )
```

```python
import functools

import jax
import jax.numpy as jnp
from jax import lax
from jax.experimental import pallas as pl
from jax.experimental.pallas import tpu as pltpu
from jax.sharding import PartitionSpec as P

EPS = 1e-06
SEGMENTS = 8
PIECES = 4
TOKEN_PIECES = 4
SCAN_TICKS = 8
MOST_VMEM = 67043328
VMEM_BYTES = 60 * 1024 * 1024


def normed(values, gain):
    factor = lax.rsqrt(jnp.mean(values * values, axis=-1, keepdims=True) + EPS)
    return values * factor * gain


def one_minus_exp(y, exp_y):
    series = 1.0 + y * (1.0 / 8.0)
    for order in (7, 6, 5, 4, 3, 2):
        series = 1.0 + y * (1.0 / order) * series
    return jnp.where(y > -0.5, -y * series, 1.0 - exp_y)


def mixer_kernel(
    x_ref, wb_ref, wg_ref, conv_ref, gates_ref, coef_ref, out_ref, pad, gel, a0, u0, a1, u1
):
    length, width = out_ref.shape
    group = gates_ref.shape[1]
    rows = 256
    pad[0:8, :] = jnp.zeros((8, width), jnp.float32)
    pad[8 + length : 16 + length, :] = jnp.zeros((8, width), jnp.float32)
    sources = ((x_ref, 0),)
    for source, base in sources:
        for start in range(0, source.shape[0], rows):
            piece = source[start : start + rows, :]
            branch = jnp.dot(piece, wb_ref[...], preferred_element_type=jnp.float32)
            gelu_in = jnp.dot(piece, wg_ref[...], preferred_element_type=jnp.float32)
            at = pl.multiple_of(base + start, rows)
            pad[pl.ds(8 + at, rows), :] = branch.astype(jnp.bfloat16).astype(jnp.float32)
            gel[pl.ds(at, rows), :] = jax.nn.gelu(
                gelu_in.astype(jnp.bfloat16).astype(jnp.float32)
            )

    for part in range(width // group):
        cols = slice(part * group, (part + 1) * group)
        taps = conv_ref[:, cols].astype(jnp.float32)
        coef = coef_ref[:, cols]
        for start in range(0, length, rows):
            summed = taps[0:1] * pad[6 + start : 6 + start + rows, cols]
            for j in range(1, 4):
                summed = summed + taps[j : j + 1] * pad[6 + j + start : 6 + j + start + rows, cols]
            conv = summed.astype(jnp.bfloat16)
            wide = conv.astype(jnp.float32)
            for d, (a_ref, u_ref) in enumerate(((a0, u0), (a1, u1))):
                gate = jnp.dot(
                    conv,
                    gates_ref[part, :, 2 * d * group : 2 * (d + 1) * group],
                    preferred_element_type=jnp.float32,
                )
                rate = jax.nn.sigmoid(gate[:, :group])
                inflow = jax.nn.sigmoid(gate[:, group:])
                log_retain = rate * coef[d : d + 1]
                retain = jnp.exp(log_retain)
                left = one_minus_exp(2.0 * log_retain, retain * retain)
                a_ref[part, start : start + rows, :] = retain
                u_ref[part, start : start + rows, :] = jnp.sqrt(left) * inflow * wide

    steps = length // SEGMENTS

    def step(t, carry):
        out = []
        for (state, decayed), (a_ref, u_ref), at in (
            (carry[0], (a0, u0), t),
            (carry[1], (a1, u1), steps - 1 - t),
        ):
            where = pl.ds(at, SEGMENTS, stride=steps)
            nstate, ndecayed = [], []
            for c in range(n):
                retain = a_ref[c, where, :]
                h = retain * state[c] + u_ref[c, where, :]
                p = retain * decayed[c]
                u_ref[c, where, :] = h
                a_ref[c, where, :] = p
                nstate.append(h)
                ndecayed.append(p)
            out.append((tuple(nstate), tuple(ndecayed)))
        return tuple(out)

    n = width // group
    zero = tuple(jnp.zeros((SEGMENTS, group), jnp.float32) for c in range(n))
    one = tuple(jnp.ones((SEGMENTS, group), jnp.float32) for c in range(n))
    ended = lax.fori_loop(0, steps, step, ((zero, one), (zero, one)), unroll=8)
    for c in range(n):
        lanes = slice(c * group, (c + 1) * group)
        blank = jnp.zeros((1, group), jnp.float32)
        entry = [[None] * SEGMENTS, [None] * SEGMENTS]
        for d, order in ((0, range(SEGMENTS)), (1, range(SEGMENTS - 1, -1, -1))):
            carry = blank
            for s in order:
                entry[d][s] = carry
                carry = ended[d][0][c][s : s + 1] + ended[d][1][c][s : s + 1] * carry
        for s in range(SEGMENTS):
            span = slice(s * steps, (s + 1) * steps)
            forward = u0[c, span, :] + a0[c, span, :] * entry[0][s]
            backward = u1[c, span, :] + a1[c, span, :] * entry[1][s]
            out_ref[span, lanes] = (gel[span, lanes] * (forward + backward)).astype(jnp.bfloat16)


def mixer(x, weights, conv_weight, w_rec, w_inp, decay):
    length, model = x.shape
    channels = conv_weight.shape[1]
    group = w_rec.shape[2]
    width = min(256, channels)
    count = channels // width
    gates = jnp.concatenate([w_rec[0], w_inp[0], w_rec[1], w_inp[1]], axis=-1)
    coef = -8.0 * jax.nn.softplus(-decay)
    f32 = functools.partial(pltpu.VMEM, dtype=jnp.float32)
    return pl.pallas_call(
        mixer_kernel,
        grid=(count,),
        out_shape=jax.ShapeDtypeStruct((length, channels), jnp.bfloat16),
        in_specs=[
            pl.BlockSpec((length, model), lambda j: (0, 0)),
            pl.BlockSpec((model, width), lambda j: (0, j)),
            pl.BlockSpec((model, width), lambda j: (0, count + j)),
            pl.BlockSpec((4, width), lambda j: (0, j)),
            pl.BlockSpec((width // group, group, 4 * group), lambda j: (j, 0, 0)),
            pl.BlockSpec((2, width), lambda j: (0, j)),
        ],
        out_specs=pl.BlockSpec((length, width), lambda j: (0, j)),
        scratch_shapes=[f32((length + 16, width)), f32((length, width))]
        + [f32((width // group, length, group)) for i in range(4)],
        compiler_params=pltpu.CompilerParams(vmem_limit_bytes=VMEM_BYTES),
        cost_estimate=pl.CostEstimate(
            flops=4 * length * model * channels + 16 * length * group * channels * 8,
            bytes_accessed=2 * (length * model + 2 * model * channels + length * channels),
            transcendentals=12 * length * channels,
        ),
    )(x, weights, weights, conv_weight, gates, coef)


def ffn_kernel(x_ref, gate_ref, up_ref, down_ref, out_ref, total):
    step = pl.program_id(0)
    gate = jnp.dot(x_ref[...], gate_ref[...], preferred_element_type=jnp.float32)
    up = jnp.dot(x_ref[...], up_ref[...], preferred_element_type=jnp.float32)
    hidden = (jax.nn.silu(gate) * up).astype(jnp.bfloat16)
    partial = lax.dot_general(
        hidden, down_ref[...], (((1,), (1,)), ((), ())), preferred_element_type=jnp.float32
    )

    @pl.when(step == 0)
    def _():
        total[...] = partial

    @pl.when(step > 0)
    def _():
        total[...] += partial

    @pl.when(step == pl.num_programs(0) - 1)
    def _():
        out_ref[...] = total[...].astype(jnp.bfloat16)


def ffn(x, weights):
    rows, model = x.shape
    units = weights.shape[1] // 3
    width = 256 if units % 256 == 0 else 128
    count = units // width
    return pl.pallas_call(
        ffn_kernel,
        grid=(count,),
        out_shape=jax.ShapeDtypeStruct((rows, model), jnp.bfloat16),
        in_specs=[
            pl.BlockSpec((rows, model), lambda j: (0, 0)),
            pl.BlockSpec((model, width), lambda j: (0, j)),
            pl.BlockSpec((model, width), lambda j: (0, count + j)),
            pl.BlockSpec((model, width), lambda j: (0, 2 * count + j)),
        ],
        out_specs=pl.BlockSpec((rows, model), lambda j: (0, 0)),
        scratch_shapes=[pltpu.VMEM((rows, model), jnp.float32)],
        compiler_params=pltpu.CompilerParams(vmem_limit_bytes=VMEM_BYTES),
        cost_estimate=pl.CostEstimate(
            flops=6 * rows * model * units,
            bytes_accessed=2 * (2 * rows * model + 3 * model * units),
            transcendentals=rows * units,
        ),
    )(x, weights, weights, weights)


def matmul_t(rows, weight_t):
    return lax.dot_general(
        rows, weight_t, (((1,), (1,)), ((), ())), preferred_element_type=jnp.float32
    )


def ring_chip(place, chips):
    half = chips // 2
    turned = place // half
    row = place * (1 - turned) + (chips - 1 - place) * turned
    return row * 2 + turned


def remote(src, dst, sent, landed, device):
    return pltpu.make_async_remote_copy(
        src_ref=src,
        dst_ref=dst,
        send_sem=sent,
        recv_sem=landed,
        device_id=device,
        device_id_type=pl.DeviceIdType.MESH,
    )


def branch_on(condition, body):
    if isinstance(condition, bool):
        if condition:
            body()
    else:
        pl.when(condition)(body)


def both(first, second):
    if isinstance(first, bool) and isinstance(second, bool):
        return first and second
    return jnp.logical_and(first, second)


def either(first, second):
    if isinstance(first, bool) and isinstance(second, bool):
        return first or second
    return jnp.logical_or(first, second)


def layer_kernel(
    size,
    tokens_ref,
    shards_ref,
    gains_ref,
    conv_ref,
    gates_ref,
    coef_ref,
    out_ref,
    full,
    far_out,
    other,
    xm,
    pad,
    gel,
    a0,
    u0,
    a1,
    u1,
    hid,
    got,
    total,
    hf,
    part,
    back,
    ring_send,
    ring_recv,
    near_send,
    near_recv,
    own_sem,
    tok_send,
    tok_recv,
    cross_send,
    cross_recv,
    share_send,
    share_recv,
    hid_send,
    hid_recv,
    back_send,
    back_recv,
):
    chips = size // 2
    reach = chips // 2
    stages, depth, cols = shards_ref.shape
    prow = depth // PIECES
    half, model = tokens_ref.shape
    blocks, width = conv_ref.shape[0], conv_ref.shape[2]
    channels = blocks * width
    group = gates_ref.shape[1]
    units = hf.shape[2]
    span = 2 * depth

    me = lax.axis_index("fs")
    core = me % 2
    turned = (me // 2) % 2
    row = me // 4
    place = row * (1 - turned) + (chips - 1 - row) * turned
    column = lax.axis_index("tp")

    def chip_at(offset):
        return ring_chip((place + chips + offset) % chips, chips)

    targets = ({"fs": chip_at(1) * 2 + core}, {"fs": chip_at(-1) * 2 + core})
    partner = {"fs": me + 1 - 2 * core}
    across = {"tp": 1 - column}

    barrier = pltpu.get_barrier_semaphore()
    for device in (*targets, partner, across):
        pl.semaphore_signal(barrier, inc=1, device_id=device, device_id_type=pl.DeviceIdType.MESH)
    pl.semaphore_wait(barrier, 4)

    def piece(g, chip, p):
        start = pl.multiple_of((chip * 2 + core) * depth + p * prow, prow)
        return full.at[g, pl.ds(start, prow), :]

    def shard_rows(g, chip, which):
        start = pl.multiple_of((chip * 2 + which) * depth, depth)
        return full.at[g, pl.ds(start, depth), :]

    def start_piece(g, p):
        src = shards_ref.at[g, pl.ds(pl.multiple_of(p * prow, prow), prow), :]
        dst = piece(g, me // 2, p)
        for way in range(2):
            remote(src, dst, ring_send.at[way, g, 0], ring_recv.at[way, g, 0, p], targets[way]).start()
        remote(src, dst, near_send.at[g, 0], near_recv.at[g, 0], partner).start()

    def pass_piece(g, s, p):
        for way in range(2):
            ref = piece(g, chip_at(-s if way == 0 else s), p)
            slot = 2 * s - 1 + way
            remote(
                ref, ref, ring_send.at[way, g, s], ring_recv.at[way, g, s - 1, p], targets[way]
            ).wait_recv()

            def forward():
                remote(
                    ref, ref, ring_send.at[way, g, s], ring_recv.at[way, g, s, p], targets[way]
                ).start()

            mine = p < PIECES // 2 if way == 0 else p >= PIECES // 2
            branch_on(either(s < reach - 1, mine), forward)
            remote(ref, ref, near_send.at[g, slot], near_recv.at[g, slot], partner).start()

    def last_piece(g, q):
        for way in range(2):
            p = q + way * (PIECES // 2)
            ref = piece(g, chip_at(reach), p)
            remote(
                ref,
                ref,
                ring_send.at[way, g, reach - 1],
                ring_recv.at[way, g, reach - 1, p],
                targets[way],
            ).wait_recv()
            remote(ref, ref, near_send.at[g, chips - 1], near_recv.at[g, chips - 1], partner).start()

    head = PIECES + PIECES // 2
    per_stage = head + (reach - 1) * PIECES

    def tick(e):
        g = e // per_stage
        k = e % per_stage
        branch_on(both(k < PIECES, g < stages), lambda: start_piece(g, k))
        branch_on(
            both(both(k >= PIECES, k < head), g > 0), lambda: last_piece(g - 1, k - PIECES)
        )
        branch_on(
            both(k >= head, g < stages),
            lambda: pass_piece(g, (k - head) // PIECES + 1, (k - head) % PIECES),
        )

    def ticks(first, last):
        @pl.loop(first, last)
        def _(e):
            tick(e)

    def near_wait(g, slot):
        ref = shard_rows(g, 0, 0)
        remote(ref, ref, near_send.at[g, slot], near_recv.at[g, slot], partner).wait_recv()

    token_rows = half // TOKEN_PIECES
    for i in range(TOKEN_PIECES):
        rows = pl.ds(i * token_rows, token_rows)
        remote(tokens_ref.at[rows, :], other.at[rows, :], tok_send.at[0], tok_recv.at[i], across).start()
    ticks(0, PIECES)
    own_copies = [
        pltpu.make_async_copy(shards_ref.at[g], shard_rows(g, me // 2, core), own_sem.at[g])
        for g in range(stages)
    ]
    for copy in own_copies:
        copy.start()

    chunk = 128

    def norm_rows(source, h, at):
        rows = pl.ds(at, chunk)
        values = source[rows, :].astype(jnp.float32)
        xm[h, rows, :] = normed(values, gains_ref[0:1, :]).astype(jnp.bfloat16)

    @pl.loop(0, half // chunk)
    def _(i):
        norm_rows(tokens_ref, 0, pl.multiple_of(i * chunk, chunk))

    length = 2 * half
    for b in range(blocks):
        pad[b, 0:8, :] = jnp.zeros((8, width), jnp.float32)
        pad[b, 8 + length : 16 + length, :] = jnp.zeros((8, width), jnp.float32)

    done0 = per_stage + head
    ticks(PIECES, done0)
    for copy in own_copies:
        copy.wait()

    @pl.loop(0, chips)
    def _(slot):
        near_wait(0, slot)

    @pl.loop(0, chips)
    def _(chip):
        src = shard_rows(0, chip, core).at[:, pl.ds(2 * channels, channels)]
        dst = far_out.at[pl.ds(pl.multiple_of((chip * 2 + core) * depth, depth), depth), :]
        remote(src, dst, cross_send.at[0], cross_recv.at[0], across).start()

    prows = 256

    @pl.loop(0, 2)
    def _(h):
        @pl.loop(0, half // prows)
        def _(i):
            at = pl.multiple_of(i * prows, prows)

            @pl.when(h == 1)
            def _():
                @pl.loop(0, prows // token_rows)
                def _(q):
                    n = i * (prows // token_rows) + q
                    rows = pl.ds(pl.multiple_of(n * token_rows, token_rows), token_rows)
                    remote(
                        tokens_ref.at[rows, :],
                        other.at[rows, :],
                        tok_send.at[0],
                        tok_recv.at[n],
                        across,
                    ).wait_recv()

                @pl.loop(0, prows // chunk)
                def _(q):
                    norm_rows(other, 1, pl.multiple_of(at + q * chunk, chunk))

            x = xm[h, pl.ds(at, prows), :]
            side = jnp.where(h == 0, column, 1 - column)
            base = pl.multiple_of(8 + side * half + at, 8)
            for b in range(blocks):
                lanes = slice(b * width, (b + 1) * width)
                branch = jnp.dot(x, full[0, :, lanes], preferred_element_type=jnp.float32)
                pad[b, pl.ds(base, prows), :] = branch.astype(jnp.bfloat16).astype(jnp.float32)
                lanes = slice(channels + b * width, channels + (b + 1) * width)
                gelu_in = jnp.dot(x, full[0, :, lanes], preferred_element_type=jnp.float32)
                gelu_in = gelu_in.astype(jnp.bfloat16).astype(jnp.float32)
                gel[h, b, pl.ds(at, prows), :] = jax.nn.gelu(gelu_in).astype(jnp.bfloat16)
            tick(done0 + h * 4 + i * 2)
            tick(done0 + h * 4 + i * 2 + 1)

    scan0 = done0 + 8
    parts = width // group
    steps = length // SEGMENTS
    crows = 256

    def hid_copy(b):
        return remote(hid.at[b], got.at[b], hid_send.at[b], hid_recv.at[b], across)

    @pl.loop(0, blocks)
    def _(b):
        at = scan0 + b * SCAN_TICKS
        count = 0
        for n in range(parts):
            lanes = slice(n * group, (n + 1) * group)
            taps = conv_ref[b, :, lanes].astype(jnp.float32)
            coef = coef_ref[b, :, lanes]
            for start in range(0, length, crows):
                summed = taps[0:1] * pad[b, 6 + start : 6 + start + crows, lanes]
                for j in range(1, 4):
                    first = 6 + j + start
                    summed = summed + taps[j : j + 1] * pad[b, first : first + crows, lanes]
                conv = summed.astype(jnp.bfloat16)
                wide = conv.astype(jnp.float32)
                for d, (a_ref, u_ref) in enumerate(((a0, u0), (a1, u1))):
                    gate = jnp.dot(
                        conv,
                        gates_ref[b * parts + n, :, 2 * d * group : 2 * (d + 1) * group],
                        preferred_element_type=jnp.float32,
                    )
                    rate = jax.nn.sigmoid(gate[:, :group])
                    inflow = jax.nn.sigmoid(gate[:, group:])
                    log_retain = rate * coef[d : d + 1]
                    retain = jnp.exp(log_retain)
                    left = one_minus_exp(2.0 * log_retain, retain * retain)
                    a_ref[n, start : start + crows, :] = retain
                    u_ref[n, start : start + crows, :] = jnp.sqrt(left) * inflow * wide
                if (start // crows) % 2 == 1 and count < SCAN_TICKS:
                    tick(at + count)
                    count += 1

        def step(t, carry):
            out = []
            for (state, decayed), (a_ref, u_ref), when in (
                (carry[0], (a0, u0), t),
                (carry[1], (a1, u1), steps - 1 - t),
            ):
                where = pl.ds(when, SEGMENTS, stride=steps)
                nstate, ndecayed = [], []
                for n in range(parts):
                    retain = a_ref[n, where, :]
                    h = retain * state[n] + u_ref[n, where, :]
                    p = retain * decayed[n]
                    u_ref[n, where, :] = h
                    a_ref[n, where, :] = p
                    nstate.append(h)
                    ndecayed.append(p)
                out.append((tuple(nstate), tuple(ndecayed)))
            return tuple(out)

        zero = tuple(jnp.zeros((SEGMENTS, group), jnp.float32) for n in range(parts))
        one = tuple(jnp.ones((SEGMENTS, group), jnp.float32) for n in range(parts))
        ended = ((zero, one), (zero, one))
        for run in range(2):
            low, high = run * steps // 2, (run + 1) * steps // 2
            ended = lax.fori_loop(low, high, step, ended, unroll=8)
            tick(at + count)
            count += 1
        per_half = SEGMENTS // 2
        for n in range(parts):
            lanes = slice(n * group, (n + 1) * group)
            blank = jnp.zeros((1, group), jnp.float32)
            entry = [[None] * SEGMENTS, [None] * SEGMENTS]
            for d, order in ((0, range(SEGMENTS)), (1, range(SEGMENTS - 1, -1, -1))):
                carry = blank
                for s in order:
                    entry[d][s] = carry
                    carry = ended[d][0][n][s : s + 1] + ended[d][1][n][s : s + 1] * carry
            for s in range(SEGMENTS):
                rows = slice(s * steps, (s + 1) * steps)
                local = slice((s % per_half) * steps, (s % per_half + 1) * steps)
                which = jnp.where(column == s // per_half, 0, 1)
                forward = u0[n, rows, :] + a0[n, rows, :] * entry[0][s]
                backward = u1[n, rows, :] + a1[n, rows, :] * entry[1][s]
                gate = gel[which, b, local, lanes].astype(jnp.float32)
                hid[b, which, local, lanes] = (gate * (forward + backward)).astype(jnp.bfloat16)
            tick(at + count)
            count += 1
        hid_copy(b).start()
        assert count == SCAN_TICKS

    out0 = scan0 + blocks * SCAN_TICKS

    ref = far_out.at[pl.ds(0, chips * depth), :]
    remote(ref, ref, cross_send.at[0], cross_recv.at[0], across).wait_recv()

    @pl.loop(0, chips)
    def _(chip):
        ref = far_out.at[pl.ds(pl.multiple_of((chip * 2 + core) * depth, depth), depth), :]
        remote(ref, ref, share_send.at[0], share_recv.at[0], partner).start()

    ocols = 256

    def mixed(h, use_own, use_far, e0):
        mine = jnp.concatenate([hid[b, h] for b in range(blocks)], axis=1)
        theirs = jnp.concatenate([got[b, 1 - h] for b in range(blocks)], axis=1)

        @pl.loop(0, model // ocols)
        def _(n):
            rows = pl.ds(pl.multiple_of(n * ocols, ocols), ocols)
            lanes = rows
            summed = 0.0
            if use_own:
                summed = matmul_t(mine, full[0, rows, 2 * channels : 3 * channels])
            else:
                summed = total[:, lanes]
            if use_far:
                summed = summed + matmul_t(theirs, far_out[rows, :])
            total[:, lanes] = summed
            if e0 is not None:

                @pl.when(n % 2 == 1)
                def _():
                    tick(e0 + n // 2)

    def settle(h, source):
        @pl.loop(0, half // chunk)
        def _(i):
            rows = pl.ds(pl.multiple_of(i * chunk, chunk), chunk)
            stream = source[rows, :].astype(jnp.float32)
            residual = stream + normed(total[rows, :], gains_ref[1:2, :])
            residual = residual.astype(jnp.bfloat16)
            if h == 0:
                out_ref[rows, :] = residual
            middle = normed(residual.astype(jnp.float32), gains_ref[2:3, :])
            xm[h, rows, :] = middle.astype(jnp.bfloat16)

    mixed(1, True, False, out0)
    ref = far_out.at[pl.ds(0, chips * depth), :]
    remote(ref, ref, share_send.at[0], share_recv.at[0], partner).wait_recv()
    for b in range(blocks):
        hid_copy(b).wait_recv()
    mixed(1, False, True, out0 + 4)
    settle(1, other)
    ffn0 = out0 + 8

    ucols = 256
    unit_chunks = units // 2 // ucols

    def expand(g, h, c):
        x = xm[h]
        lanes = pl.ds(pl.multiple_of(c * ucols, ucols), ucols)
        gate = jnp.dot(x, full[g, :, lanes], preferred_element_type=jnp.float32)
        lanes = pl.ds(pl.multiple_of(units // 2 + c * ucols, ucols), ucols)
        up = jnp.dot(x, full[g, :, lanes], preferred_element_type=jnp.float32)
        lanes = pl.ds(pl.multiple_of((g - 1) * (units // 2) + c * ucols, ucols), ucols)
        hf[h, :, lanes] = (jax.nn.silu(gate) * up).astype(jnp.bfloat16)

    first_done = 2 * per_stage + head
    second_done = 3 * per_stage + head
    ticks(ffn0, first_done) if ffn0 < first_done else None
    ffn1 = max(ffn0, first_done)

    @pl.loop(0, chips)
    def _(slot):
        near_wait(1, slot)

    @pl.loop(0, unit_chunks)
    def _(c):
        expand(1, 1, c)
        tick(ffn1 + c)

    ffn2 = ffn1 + unit_chunks
    ticks(ffn2, second_done)

    @pl.loop(0, chips)
    def _(slot):
        near_wait(2, slot)

    @pl.loop(0, unit_chunks)
    def _(c):
        expand(2, 1, c)
        tick(second_done + c)

    def feature_chip(slot):
        d = (slot + 1) // 2
        return chip_at(jnp.where(slot % 2 == 1, -d, d))

    def partial_of(h, chip):
        weight = full[stages - 1, pl.ds(pl.multiple_of(chip * span, span), span), :]
        return matmul_t(hf[h], weight)

    def back_copy(slot):
        chip = feature_chip(slot)
        return remote(part.at[chip], back.at[chip], back_send.at[slot], back_recv.at[slot], across)

    down0 = second_done + unit_chunks
    distance1 = (stages - 1) * per_stage + head + PIECES

    @pl.loop(0, chips)
    def _(slot):
        @pl.when(slot == 1)
        def _():
            ticks(down0, distance1)

        @pl.when(jnp.logical_and(slot % 2 == 1, jnp.logical_and(slot > 1, slot < chips - 1)))
        def _():
            @pl.loop(0, PIECES)
            def _(i):
                tick(distance1 + (slot // 2 - 1) * PIECES + i)

        @pl.when(slot == chips - 1)
        def _():
            ticks(stages * per_stage + PIECES, stages * per_stage + head)

        near_wait(stages - 1, slot)
        chip = feature_chip(slot)
        part[chip] = partial_of(1, chip).astype(jnp.bfloat16)
        back_copy(slot).start()

    mixed(0, True, True, None)
    settle(0, tokens_ref)

    @pl.loop(0, 2 * unit_chunks)
    def _(c):
        expand(1 + c // unit_chunks, 0, c % unit_chunks)

    @pl.loop(0, chips)
    def _(chip):
        lanes = pl.ds(pl.multiple_of(chip * span, span), span)
        total[:, lanes] = partial_of(0, chip).astype(jnp.bfloat16).astype(jnp.float32)

    @pl.loop(0, chips)
    def _(slot):
        back_copy(slot).wait_recv()

    @pl.loop(0, half // chunk)
    def _(i):
        rows = pl.ds(pl.multiple_of(i * chunk, chunk), chunk)
        came = jnp.concatenate([back[chip, rows, :] for chip in range(chips)], axis=1)
        summed = total[rows, :] + came.astype(jnp.float32)
        middle = out_ref[rows, :].astype(jnp.float32)
        out_ref[rows, :] = (middle + normed(summed, gains_ref[3:4, :])).astype(jnp.bfloat16)

    for g in range(stages):
        ref = shard_rows(g, 0, 0)
        for way in range(2):
            for s in range(reach):
                sent = ref if s < reach - 1 else full.at[g, pl.ds(0, depth // 2), :]
                remote(
                    sent, sent, ring_send.at[way, g, s], ring_recv.at[way, g, s, 0], targets[way]
                ).wait_send()
        for slot in range(chips):
            remote(ref, ref, near_send.at[g, slot], near_recv.at[g, slot], partner).wait_send()
    remote(tokens_ref, other, tok_send.at[0], tok_recv.at[0], across).wait_send()
    ref = far_out.at[pl.ds(0, chips * depth), :]
    remote(ref, ref, cross_send.at[0], cross_recv.at[0], across).wait_send()
    remote(ref, ref, share_send.at[0], share_recv.at[0], partner).wait_send()
    for b in range(blocks):
        hid_copy(b).wait_send()
    for slot in range(chips):
        back_copy(slot).wait_send()


def paired_device(
    tokens,
    pre_mix_gain,
    post_mix_gain,
    pre_ffn_gain,
    post_ffn_gain,
    w_branch,
    w_gelu,
    conv_weight,
    w_rec,
    w_inp,
    decay,
    out_weight_t,
    w_gate,
    w_up,
    down_weight_t,
):
    half, model = tokens.shape
    depth, channels = w_branch.shape
    units = w_gate.shape[1]
    size = lax.axis_size("fs")
    chips = size // 2
    group = w_rec.shape[2]
    width = min(256, channels)
    blocks = channels // width
    length = 2 * half
    cut = units // 2
    shards = jnp.stack(
        [
            jnp.concatenate([w_branch, w_gelu, out_weight_t], axis=1),
            jnp.concatenate([w_gate[:, :cut], w_up[:, :cut]], axis=1),
            jnp.concatenate([w_gate[:, cut:], w_up[:, cut:]], axis=1),
            down_weight_t,
        ]
    )
    gains = jnp.stack([pre_mix_gain, post_mix_gain, pre_ffn_gain, post_ffn_gain])
    conv = conv_weight.reshape(4, blocks, width).swapaxes(0, 1)
    gates = jnp.concatenate([w_rec[0], w_inp[0], w_rec[1], w_inp[1]], axis=-1)
    coef = (-8.0 * jax.nn.softplus(-decay)).reshape(2, blocks, width).swapaxes(0, 1)
    bf16 = functools.partial(pltpu.VMEM, dtype=jnp.bfloat16)
    f32 = functools.partial(pltpu.VMEM, dtype=jnp.float32)
    dma = pltpu.SemaphoreType.DMA
    stages = shards.shape[0]
    reach = chips // 2
    vmem = pl.BlockSpec(memory_space=pltpu.VMEM)
    return pl.pallas_call(
        functools.partial(layer_kernel, size),
        out_shape=jax.ShapeDtypeStruct((half, model), jnp.bfloat16),
        in_specs=[vmem] * 6,
        out_specs=vmem,
        scratch_shapes=[
            bf16((stages, model, shards.shape[2])),
            bf16((model, channels)),
            bf16((half, model)),
            bf16((2, half, model)),
            f32((blocks, length + 16, width)),
            bf16((2, blocks, half, width)),
        ]
        + [f32((width // group, length, group)) for i in range(4)]
        + [
            bf16((blocks, 2, half, width)),
            bf16((blocks, 2, half, width)),
            f32((half, model)),
            bf16((2, half, units)),
            bf16((chips, half, 2 * depth)),
            bf16((chips, half, 2 * depth)),
            dma((2, stages, reach)),
            dma((2, stages, reach, PIECES)),
            dma((stages, chips)),
            dma((stages, chips)),
            dma((stages,)),
            dma((1,)),
            dma((TOKEN_PIECES,)),
            dma((1,)),
            dma((1,)),
            dma((1,)),
            dma((1,)),
            dma((blocks,)),
            dma((blocks,)),
            dma((chips,)),
            dma((chips,)),
        ],
        compiler_params=pltpu.CompilerParams(
            collective_id=0, has_side_effects=True, vmem_limit_bytes=MOST_VMEM
        ),
        cost_estimate=pl.CostEstimate(
            flops=1 << 34, bytes_accessed=1 << 26, transcendentals=1 << 24
        ),
    )(tokens, shards, gains, conv, gates, coef)


def wide_device(
    tokens,
    pre_mix_gain,
    post_mix_gain,
    pre_ffn_gain,
    post_ffn_gain,
    w_branch,
    w_gelu,
    conv_weight,
    w_rec,
    w_inp,
    decay,
    out_weight_t,
    w_gate,
    w_up,
    down_weight_t,
):
    channels = conv_weight.shape[1]
    mix_shard = jnp.concatenate([w_branch, w_gelu, out_weight_t], axis=1)
    ffn_shard = jnp.concatenate([w_gate, w_up, down_weight_t], axis=1)
    stream = tokens.astype(jnp.float32)
    normed_in = normed(stream, pre_mix_gain).astype(jnp.bfloat16)
    mix_all = lax.all_gather(mix_shard, "fs", axis=0, tiled=True)
    whole = lax.all_gather(normed_in, "tp", axis=0, tiled=True)
    ffn_all = lax.all_gather(ffn_shard, "fs", axis=0, tiled=True)
    out_own = mix_all[:, 2 * channels :]
    hidden = mixer(whole, mix_all, conv_weight, w_rec, w_inp, decay)
    own_hidden = lax.all_to_all(hidden, "tp", split_axis=0, concat_axis=1, tiled=True)
    out_whole = lax.all_gather(out_own, "tp", axis=1, tiled=True)
    mixer_sum = matmul_t(own_hidden, out_whole)
    residual = (stream + normed(mixer_sum, post_mix_gain)).astype(jnp.bfloat16)
    middle = residual.astype(jnp.float32)
    normed_mid = normed(middle, pre_ffn_gain).astype(jnp.bfloat16)
    all_mid = lax.all_gather(normed_mid, "tp", axis=0, tiled=True)
    ffn_sum = lax.psum_scatter(
        ffn(all_mid, ffn_all), "tp", scatter_dimension=0, tiled=True
    ).astype(jnp.float32)
    return (middle + normed(ffn_sum, post_ffn_gain)).astype(jnp.bfloat16)


def solution(mesh):
    return jax.shard_map(
        paired_device if mesh.shape["tp"] == 2 else wide_device,
        mesh=mesh,
        in_specs=(
            P(("fs", "tp"), None),
            P(),
            P(),
            P(),
            P(),
            P("fs", "tp"),
            P("fs", "tp"),
            P(None, "tp"),
            P(None, "tp", None, None),
            P(None, "tp", None, None),
            P(None, "tp"),
            P("fs", "tp"),
            P("fs", "tp"),
            P("fs", "tp"),
            P("fs", "tp"),
        ),
        out_specs=P(("fs", "tp"), None),
        check_vma=False,
    )
```

```python
import functools

import jax
import jax.numpy as jnp
from jax import lax
from jax.experimental import pallas as pl
from jax.experimental.pallas import tpu as pltpu
from jax.sharding import PartitionSpec as P

EPS = 1e-06
SEGMENTS = 8
PIECES = 4
TOKEN_PIECES = 4
SCAN_TICKS = 9
MOST_VMEM = 67043328
VMEM_BYTES = 60 * 1024 * 1024


def normed(values, gain):
    factor = lax.rsqrt(jnp.mean(values * values, axis=-1, keepdims=True) + EPS)
    return values * factor * gain


def one_minus_exp(y, exp_y):
    series = 1.0 + y * (1.0 / 8.0)
    for order in (7, 6, 5, 4, 3, 2):
        series = 1.0 + y * (1.0 / order) * series
    return jnp.where(y > -0.5, -y * series, 1.0 - exp_y)


def mixer_kernel(
    x_ref, wb_ref, wg_ref, conv_ref, gates_ref, coef_ref, out_ref, pad, gel, a0, u0, a1, u1
):
    length, width = out_ref.shape
    group = gates_ref.shape[1]
    rows = 256
    pad[0:8, :] = jnp.zeros((8, width), jnp.float32)
    pad[8 + length : 16 + length, :] = jnp.zeros((8, width), jnp.float32)
    sources = ((x_ref, 0),)
    for source, base in sources:
        for start in range(0, source.shape[0], rows):
            piece = source[start : start + rows, :]
            branch = jnp.dot(piece, wb_ref[...], preferred_element_type=jnp.float32)
            gelu_in = jnp.dot(piece, wg_ref[...], preferred_element_type=jnp.float32)
            at = pl.multiple_of(base + start, rows)
            pad[pl.ds(8 + at, rows), :] = branch.astype(jnp.bfloat16).astype(jnp.float32)
            gel[pl.ds(at, rows), :] = jax.nn.gelu(
                gelu_in.astype(jnp.bfloat16).astype(jnp.float32)
            )

    for part in range(width // group):
        cols = slice(part * group, (part + 1) * group)
        taps = conv_ref[:, cols].astype(jnp.float32)
        coef = coef_ref[:, cols]
        for start in range(0, length, rows):
            summed = taps[0:1] * pad[6 + start : 6 + start + rows, cols]
            for j in range(1, 4):
                summed = summed + taps[j : j + 1] * pad[6 + j + start : 6 + j + start + rows, cols]
            conv = summed.astype(jnp.bfloat16)
            wide = conv.astype(jnp.float32)
            for d, (a_ref, u_ref) in enumerate(((a0, u0), (a1, u1))):
                gate = jnp.dot(
                    conv,
                    gates_ref[part, :, 2 * d * group : 2 * (d + 1) * group],
                    preferred_element_type=jnp.float32,
                )
                rate = jax.nn.sigmoid(gate[:, :group])
                inflow = jax.nn.sigmoid(gate[:, group:])
                log_retain = rate * coef[d : d + 1]
                retain = jnp.exp(log_retain)
                left = one_minus_exp(2.0 * log_retain, retain * retain)
                a_ref[part, start : start + rows, :] = retain
                u_ref[part, start : start + rows, :] = jnp.sqrt(left) * inflow * wide

    steps = length // SEGMENTS

    def step(t, carry):
        out = []
        for (state, decayed), (a_ref, u_ref), at in (
            (carry[0], (a0, u0), t),
            (carry[1], (a1, u1), steps - 1 - t),
        ):
            where = pl.ds(at, SEGMENTS, stride=steps)
            nstate, ndecayed = [], []
            for c in range(n):
                retain = a_ref[c, where, :]
                h = retain * state[c] + u_ref[c, where, :]
                p = retain * decayed[c]
                u_ref[c, where, :] = h
                a_ref[c, where, :] = p
                nstate.append(h)
                ndecayed.append(p)
            out.append((tuple(nstate), tuple(ndecayed)))
        return tuple(out)

    n = width // group
    zero = tuple(jnp.zeros((SEGMENTS, group), jnp.float32) for c in range(n))
    one = tuple(jnp.ones((SEGMENTS, group), jnp.float32) for c in range(n))
    ended = lax.fori_loop(0, steps, step, ((zero, one), (zero, one)), unroll=8)
    for c in range(n):
        lanes = slice(c * group, (c + 1) * group)
        blank = jnp.zeros((1, group), jnp.float32)
        entry = [[None] * SEGMENTS, [None] * SEGMENTS]
        for d, order in ((0, range(SEGMENTS)), (1, range(SEGMENTS - 1, -1, -1))):
            carry = blank
            for s in order:
                entry[d][s] = carry
                carry = ended[d][0][c][s : s + 1] + ended[d][1][c][s : s + 1] * carry
        for s in range(SEGMENTS):
            span = slice(s * steps, (s + 1) * steps)
            forward = u0[c, span, :] + a0[c, span, :] * entry[0][s]
            backward = u1[c, span, :] + a1[c, span, :] * entry[1][s]
            out_ref[span, lanes] = (gel[span, lanes] * (forward + backward)).astype(jnp.bfloat16)


def mixer(x, weights, conv_weight, w_rec, w_inp, decay):
    length, model = x.shape
    channels = conv_weight.shape[1]
    group = w_rec.shape[2]
    width = min(256, channels)
    count = channels // width
    gates = jnp.concatenate([w_rec[0], w_inp[0], w_rec[1], w_inp[1]], axis=-1)
    coef = -8.0 * jax.nn.softplus(-decay)
    f32 = functools.partial(pltpu.VMEM, dtype=jnp.float32)
    return pl.pallas_call(
        mixer_kernel,
        grid=(count,),
        out_shape=jax.ShapeDtypeStruct((length, channels), jnp.bfloat16),
        in_specs=[
            pl.BlockSpec((length, model), lambda j: (0, 0)),
            pl.BlockSpec((model, width), lambda j: (0, j)),
            pl.BlockSpec((model, width), lambda j: (0, count + j)),
            pl.BlockSpec((4, width), lambda j: (0, j)),
            pl.BlockSpec((width // group, group, 4 * group), lambda j: (j, 0, 0)),
            pl.BlockSpec((2, width), lambda j: (0, j)),
        ],
        out_specs=pl.BlockSpec((length, width), lambda j: (0, j)),
        scratch_shapes=[f32((length + 16, width)), f32((length, width))]
        + [f32((width // group, length, group)) for i in range(4)],
        compiler_params=pltpu.CompilerParams(vmem_limit_bytes=VMEM_BYTES),
        cost_estimate=pl.CostEstimate(
            flops=4 * length * model * channels + 16 * length * group * channels * 8,
            bytes_accessed=2 * (length * model + 2 * model * channels + length * channels),
            transcendentals=12 * length * channels,
        ),
    )(x, weights, weights, conv_weight, gates, coef)


def ffn_kernel(x_ref, gate_ref, up_ref, down_ref, out_ref, total):
    step = pl.program_id(0)
    gate = jnp.dot(x_ref[...], gate_ref[...], preferred_element_type=jnp.float32)
    up = jnp.dot(x_ref[...], up_ref[...], preferred_element_type=jnp.float32)
    hidden = (jax.nn.silu(gate) * up).astype(jnp.bfloat16)
    partial = lax.dot_general(
        hidden, down_ref[...], (((1,), (1,)), ((), ())), preferred_element_type=jnp.float32
    )

    @pl.when(step == 0)
    def _():
        total[...] = partial

    @pl.when(step > 0)
    def _():
        total[...] += partial

    @pl.when(step == pl.num_programs(0) - 1)
    def _():
        out_ref[...] = total[...].astype(jnp.bfloat16)


def ffn(x, weights):
    rows, model = x.shape
    units = weights.shape[1] // 3
    width = 256 if units % 256 == 0 else 128
    count = units // width
    return pl.pallas_call(
        ffn_kernel,
        grid=(count,),
        out_shape=jax.ShapeDtypeStruct((rows, model), jnp.bfloat16),
        in_specs=[
            pl.BlockSpec((rows, model), lambda j: (0, 0)),
            pl.BlockSpec((model, width), lambda j: (0, j)),
            pl.BlockSpec((model, width), lambda j: (0, count + j)),
            pl.BlockSpec((model, width), lambda j: (0, 2 * count + j)),
        ],
        out_specs=pl.BlockSpec((rows, model), lambda j: (0, 0)),
        scratch_shapes=[pltpu.VMEM((rows, model), jnp.float32)],
        compiler_params=pltpu.CompilerParams(vmem_limit_bytes=VMEM_BYTES),
        cost_estimate=pl.CostEstimate(
            flops=6 * rows * model * units,
            bytes_accessed=2 * (2 * rows * model + 3 * model * units),
            transcendentals=rows * units,
        ),
    )(x, weights, weights, weights)


def matmul_t(rows, weight_t):
    return lax.dot_general(
        rows, weight_t, (((1,), (1,)), ((), ())), preferred_element_type=jnp.float32
    )


def ring_chip(place, chips):
    half = chips // 2
    turned = place // half
    row = place * (1 - turned) + (chips - 1 - place) * turned
    return row * 2 + turned


def remote(src, dst, sent, landed, device):
    return pltpu.make_async_remote_copy(
        src_ref=src,
        dst_ref=dst,
        send_sem=sent,
        recv_sem=landed,
        device_id=device,
        device_id_type=pl.DeviceIdType.MESH,
    )


def branch_on(condition, body):
    if isinstance(condition, bool):
        if condition:
            body()
    else:
        pl.when(condition)(body)


def both(first, second):
    if isinstance(first, bool) and isinstance(second, bool):
        return first and second
    return jnp.logical_and(first, second)


def either(first, second):
    if isinstance(first, bool) and isinstance(second, bool):
        return first or second
    return jnp.logical_or(first, second)


def layer_kernel(
    size,
    tokens_ref,
    branch_ref,
    gelu_ref,
    outw_ref,
    gate_ref,
    up_ref,
    down_ref,
    gain0_ref,
    gain1_ref,
    gain2_ref,
    gain3_ref,
    taps_ref,
    rec_ref,
    inp_ref,
    decay_ref,
    out_ref,
    mine,
    gains,
    conv_ref,
    gates_ref,
    coef_ref,
    full,
    far_out,
    other,
    xm,
    pad,
    gel,
    a0,
    u0,
    a1,
    u1,
    hid,
    got,
    total,
    hf,
    part,
    back,
    ring_send,
    ring_recv,
    near_send,
    near_recv,
    own_sem,
    small_sem,
    mine_sem,
    out_sem,
    tok_send,
    tok_recv,
    cross_send,
    cross_recv,
    share_send,
    share_recv,
    hid_send,
    hid_recv,
    back_send,
    back_recv,
):
    chips = size // 2
    reach = chips // 2
    stages = full.shape[0]
    depth, channels = branch_ref.shape
    prow = depth // PIECES
    half, model = tokens_ref.shape
    blocks, width = pad.shape[0], pad.shape[2]
    group = gates_ref.shape[1]
    groups = gates_ref.shape[0]
    units = hf.shape[2]
    span = 2 * depth

    me = lax.axis_index("fs")
    core = me % 2
    turned = (me // 2) % 2
    row = me // 4
    place = row * (1 - turned) + (chips - 1 - row) * turned
    column = lax.axis_index("tp")

    def chip_at(offset):
        return ring_chip((place + chips + offset) % chips, chips)

    targets = ({"fs": chip_at(1) * 2 + core}, {"fs": chip_at(-1) * 2 + core})
    partner = {"fs": me + 1 - 2 * core}
    across = {"tp": 1 - column}

    cut = units // 2
    own_rows = pl.ds(pl.multiple_of(me * depth, depth), depth)

    def own_part(g, source, lanes, at, sem):
        place_at = full.at[g, own_rows, pl.ds(at, lanes.size)]
        return pltpu.make_async_copy(source.at[:, lanes], place_at, own_sem.at[sem])

    every = pl.ds(0, channels)
    low, high = pl.ds(0, cut), pl.ds(cut, cut)
    own_copies = [
        [own_part(0, source, every, i * channels, i) for i, source in enumerate((branch_ref, gelu_ref, outw_ref))],
        [own_part(1, gate_ref, low, 0, 3), own_part(1, up_ref, low, cut, 4)],
        [own_part(2, gate_ref, high, 0, 5), own_part(2, up_ref, high, cut, 6)],
        [own_part(3, down_ref, pl.ds(0, units), 0, 7)],
    ]
    for copy in own_copies[0]:
        copy.start()
    chunk = 128
    mine_copies = []
    for i in range(half // chunk):
        rows = pl.ds(i * chunk, chunk)
        mine_copies.append(
            pltpu.make_async_copy(tokens_ref.at[rows, :], mine.at[rows, :], mine_sem.at[i])
        )
    for i, copy in enumerate(mine_copies):
        copy.start()
    small = [(source, gains.at[i]) for i, source in enumerate((gain0_ref, gain1_ref, gain2_ref, gain3_ref))]
    small += [(taps_ref, conv_ref), (decay_ref, coef_ref)]
    for n in range(groups):
        for d in range(2):
            for i, source in enumerate((rec_ref, inp_ref)):
                lanes = pl.ds((2 * d + i) * group, group)
                small.append((source.at[d, n], gates_ref.at[n, :, lanes]))
    small = [
        pltpu.make_async_copy(source, place_at, small_sem.at[i])
        for i, (source, place_at) in enumerate(small)
    ]
    for copy in small:
        copy.start()
    for copies in own_copies[1:]:
        for copy in copies:
            copy.start()

    barrier = pltpu.get_barrier_semaphore()
    for device in (*targets, partner, across):
        pl.semaphore_signal(barrier, inc=1, device_id=device, device_id_type=pl.DeviceIdType.MESH)
    pl.semaphore_wait(barrier, 4)

    def piece(g, chip, p):
        start = pl.multiple_of((chip * 2 + core) * depth + p * prow, prow)
        return full.at[g, pl.ds(start, prow), :]

    def shard_rows(g, chip, which):
        start = pl.multiple_of((chip * 2 + which) * depth, depth)
        return full.at[g, pl.ds(start, depth), :]

    def start_piece(g, p):
        src = piece(g, me // 2, p)
        dst = src
        for way in range(2):
            remote(src, dst, ring_send.at[way, g, 0], ring_recv.at[way, g, 0, p], targets[way]).start()
        remote(src, dst, near_send.at[g, 0], near_recv.at[g, 0], partner).start()

    def pass_piece(g, s, p):
        for way in range(2):
            ref = piece(g, chip_at(-s if way == 0 else s), p)
            slot = 2 * s - 1 + way
            remote(
                ref, ref, ring_send.at[way, g, s], ring_recv.at[way, g, s - 1, p], targets[way]
            ).wait_recv()

            def forward():
                remote(
                    ref, ref, ring_send.at[way, g, s], ring_recv.at[way, g, s, p], targets[way]
                ).start()

            mine = p < PIECES // 2 if way == 0 else p >= PIECES // 2
            branch_on(either(s < reach - 1, mine), forward)
            remote(ref, ref, near_send.at[g, slot], near_recv.at[g, slot], partner).start()

    def last_piece(g, q):
        for way in range(2):
            p = q + way * (PIECES // 2)
            ref = piece(g, chip_at(reach), p)
            remote(
                ref,
                ref,
                ring_send.at[way, g, reach - 1],
                ring_recv.at[way, g, reach - 1, p],
                targets[way],
            ).wait_recv()
            remote(ref, ref, near_send.at[g, chips - 1], near_recv.at[g, chips - 1], partner).start()

    head = PIECES + PIECES // 2
    per_stage = head + (reach - 1) * PIECES

    def tick(e):
        g = e // per_stage
        k = e % per_stage
        branch_on(both(k < PIECES, g < stages), lambda: start_piece(g, k))
        branch_on(
            both(both(k >= PIECES, k < head), g > 0), lambda: last_piece(g - 1, k - PIECES)
        )
        branch_on(
            both(k >= head, g < stages),
            lambda: pass_piece(g, (k - head) // PIECES + 1, (k - head) % PIECES),
        )

    def ticks(first, last):
        @pl.loop(first, last)
        def _(e):
            tick(e)

    def near_wait(g, slot):
        ref = shard_rows(g, 0, 0)
        remote(ref, ref, near_send.at[g, slot], near_recv.at[g, slot], partner).wait_recv()

    token_rows = half // TOKEN_PIECES
    for i in range(TOKEN_PIECES):
        rows = pl.ds(i * token_rows, token_rows)
        remote(tokens_ref.at[rows, :], other.at[rows, :], tok_send.at[0], tok_recv.at[i], across).start()
    for copy in own_copies[0]:
        copy.wait()
    ticks(0, PIECES)
    for copy in (*small, *mine_copies):
        copy.wait()
    for copies in own_copies[1:]:
        for copy in copies:
            copy.wait()
    slow = coef_ref[...]
    coef_ref[...] = -8.0 * (jnp.maximum(-slow, 0.0) + jnp.log1p(jnp.exp(-jnp.abs(slow))))

    def norm_rows(source, h, at):
        rows = pl.ds(at, chunk)
        values = source[rows, :].astype(jnp.float32)
        xm[h, rows, :] = normed(values, gains[0]).astype(jnp.bfloat16)

    @pl.loop(0, half // chunk)
    def _(i):
        norm_rows(mine, 0, pl.multiple_of(i * chunk, chunk))

    length = 2 * half
    for b in range(blocks):
        pad[b, 0:8, :] = jnp.zeros((8, width), jnp.float32)
        pad[b, 8 + length : 16 + length, :] = jnp.zeros((8, width), jnp.float32)

    done0 = per_stage + head
    ticks(PIECES, done0)

    @pl.loop(0, chips)
    def _(slot):
        near_wait(0, slot)

    @pl.loop(0, chips)
    def _(chip):
        src = shard_rows(0, chip, core).at[:, pl.ds(2 * channels, channels)]
        dst = far_out.at[pl.ds(pl.multiple_of((chip * 2 + core) * depth, depth), depth), :]
        remote(src, dst, cross_send.at[0], cross_recv.at[0], across).start()

    prows = 256

    @pl.loop(0, 2)
    def _(h):
        @pl.loop(0, half // prows)
        def _(i):
            at = pl.multiple_of(i * prows, prows)

            @pl.when(h == 1)
            def _():
                @pl.loop(0, prows // token_rows)
                def _(q):
                    n = i * (prows // token_rows) + q
                    rows = pl.ds(pl.multiple_of(n * token_rows, token_rows), token_rows)
                    remote(
                        tokens_ref.at[rows, :],
                        other.at[rows, :],
                        tok_send.at[0],
                        tok_recv.at[n],
                        across,
                    ).wait_recv()

                @pl.loop(0, prows // chunk)
                def _(q):
                    norm_rows(other, 1, pl.multiple_of(at + q * chunk, chunk))

            x = xm[h, pl.ds(at, prows), :]
            side = jnp.where(h == 0, column, 1 - column)
            base = pl.multiple_of(8 + side * half + at, 8)
            for b in range(blocks):
                lanes = slice(b * width, (b + 1) * width)
                branch = jnp.dot(x, full[0, :, lanes], preferred_element_type=jnp.float32)
                pad[b, pl.ds(base, prows), :] = branch.astype(jnp.bfloat16).astype(jnp.float32)
                lanes = slice(channels + b * width, channels + (b + 1) * width)
                gelu_in = jnp.dot(x, full[0, :, lanes], preferred_element_type=jnp.float32)
                gelu_in = gelu_in.astype(jnp.bfloat16).astype(jnp.float32)
                gel[h, b, pl.ds(at, prows), :] = jax.nn.gelu(gelu_in).astype(jnp.bfloat16)

            @pl.when(h * (half // prows) + i < 2 * (half // prows) - 1)
            def _():
                ticks(done0 + h * 4 + i * 2, done0 + h * 4 + i * 2 + 2)

    scan0 = done0 + 2 * (2 * (half // prows) - 1)
    parts = width // group
    steps = length // SEGMENTS
    crows = 256

    def hid_copy(b, h):
        return remote(
            hid.at[b, h], got.at[b, h], hid_send.at[b, h], hid_recv.at[b, h], across
        )

    @pl.loop(0, blocks)
    def _(b):
        at = scan0 + b * SCAN_TICKS
        count = 0
        for n in range(parts):
            lanes = slice(n * group, (n + 1) * group)
            table = pl.ds(pl.multiple_of(b * width + n * group, group), group)
            taps = conv_ref[:, table].astype(jnp.float32)
            coef = coef_ref[:, table]
            for start in range(0, length, crows):
                summed = taps[0:1] * pad[b, 6 + start : 6 + start + crows, lanes]
                for j in range(1, 4):
                    first = 6 + j + start
                    summed = summed + taps[j : j + 1] * pad[b, first : first + crows, lanes]
                conv = summed.astype(jnp.bfloat16)
                wide = conv.astype(jnp.float32)
                for d, (a_ref, u_ref) in enumerate(((a0, u0), (a1, u1))):
                    gate = jnp.dot(
                        conv,
                        gates_ref[b * parts + n, :, 2 * d * group : 2 * (d + 1) * group],
                        preferred_element_type=jnp.float32,
                    )
                    rate = jax.nn.sigmoid(gate[:, :group])
                    inflow = jax.nn.sigmoid(gate[:, group:])
                    log_retain = rate * coef[d : d + 1]
                    retain = jnp.exp(log_retain)
                    left = one_minus_exp(2.0 * log_retain, retain * retain)
                    a_ref[n, start : start + crows, :] = retain
                    u_ref[n, start : start + crows, :] = jnp.sqrt(left) * inflow * wide
                if (start // crows) % 2 == 1 and count < SCAN_TICKS:
                    tick(at + count)
                    count += 1

        def step(t, carry):
            out = []
            for (state, decayed), (a_ref, u_ref), when in (
                (carry[0], (a0, u0), t),
                (carry[1], (a1, u1), steps - 1 - t),
            ):
                where = pl.ds(when, SEGMENTS, stride=steps)
                nstate, ndecayed = [], []
                for n in range(parts):
                    retain = a_ref[n, where, :]
                    h = retain * state[n] + u_ref[n, where, :]
                    p = retain * decayed[n]
                    u_ref[n, where, :] = h
                    a_ref[n, where, :] = p
                    nstate.append(h)
                    ndecayed.append(p)
                out.append((tuple(nstate), tuple(ndecayed)))
            return tuple(out)

        zero = tuple(jnp.zeros((SEGMENTS, group), jnp.float32) for n in range(parts))
        one = tuple(jnp.ones((SEGMENTS, group), jnp.float32) for n in range(parts))
        ended = ((zero, one), (zero, one))
        for run in range(2):
            low, high = run * steps // 2, (run + 1) * steps // 2
            ended = lax.fori_loop(low, high, step, ended, unroll=8)
            tick(at + count)
            count += 1
        per_half = SEGMENTS // 2
        for n in range(parts):
            lanes = slice(n * group, (n + 1) * group)
            blank = jnp.zeros((1, group), jnp.float32)
            entry = [[None] * SEGMENTS, [None] * SEGMENTS]
            for d, order in ((0, range(SEGMENTS)), (1, range(SEGMENTS - 1, -1, -1))):
                carry = blank
                for s in order:
                    entry[d][s] = carry
                    carry = ended[d][0][n][s : s + 1] + ended[d][1][n][s : s + 1] * carry
            for s in range(SEGMENTS):
                rows = slice(s * steps, (s + 1) * steps)
                local = slice((s % per_half) * steps, (s % per_half + 1) * steps)
                which = jnp.where(column == s // per_half, 0, 1)
                forward = u0[n, rows, :] + a0[n, rows, :] * entry[0][s]
                backward = u1[n, rows, :] + a1[n, rows, :] * entry[1][s]
                gate = gel[which, b, local, lanes].astype(jnp.float32)
                hid[b, which, local, lanes] = (gate * (forward + backward)).astype(jnp.bfloat16)
            tick(at + count)
            count += 1
        tick(at + count)
        count += 1
        assert count == SCAN_TICKS
        hid_copy(b, 0).start()

    for b in range(blocks):
        hid_copy(b, 1).start()
    out0 = scan0 + blocks * SCAN_TICKS

    ref = far_out.at[pl.ds(0, chips * depth), :]
    remote(ref, ref, cross_send.at[0], cross_recv.at[0], across).wait_recv()

    @pl.loop(0, chips)
    def _(chip):
        ref = far_out.at[pl.ds(pl.multiple_of((chip * 2 + core) * depth, depth), depth), :]
        remote(ref, ref, share_send.at[0], share_recv.at[0], partner).start()

    ocols = 256

    def mixed(h, own_blocks, far_blocks, fresh, e0=0, count=0):
        left = [hid[b, h] for b in own_blocks]
        left = jnp.concatenate(left, axis=1) if left else None
        right = [got[b, 1 - h] for b in far_blocks]
        right = jnp.concatenate(right, axis=1) if right else None
        parts_n = model // ocols

        @pl.loop(0, parts_n)
        def _(n):
            rows = pl.ds(pl.multiple_of(n * ocols, ocols), ocols)
            lanes = rows
            summed = None if fresh else total[:, lanes]
            if left is not None:
                first = 2 * channels + own_blocks[0] * width
                term = matmul_t(left, full[0, rows, first : first + len(own_blocks) * width])
                summed = term if summed is None else summed + term
            if right is not None:
                first = far_blocks[0] * width
                term = matmul_t(right, far_out[rows, first : first + len(far_blocks) * width])
                summed = term if summed is None else summed + term
            total[:, lanes] = summed
            if count:
                every_n = parts_n // count

                @pl.when(n % every_n == every_n - 1)
                def _():
                    tick(e0 + n // every_n)

    def settle(h, source):
        @pl.loop(0, half // chunk)
        def _(i):
            rows = pl.ds(pl.multiple_of(i * chunk, chunk), chunk)
            stream = source[rows, :].astype(jnp.float32)
            residual = stream + normed(total[rows, :], gains[1])
            residual = residual.astype(jnp.bfloat16)
            if h == 0:
                source[rows, :] = residual
            middle = normed(residual.astype(jnp.float32), gains[2])
            xm[h, rows, :] = middle.astype(jnp.bfloat16)

    all_blocks = tuple(range(blocks))
    mixed(1, all_blocks, (), True, out0, 2)
    ref = far_out.at[pl.ds(0, chips * depth), :]
    remote(ref, ref, share_send.at[0], share_recv.at[0], partner).wait_recv()
    ffn0 = out0 + 2
    for b in all_blocks:
        hid_copy(b, 0).wait_recv()
        mixed(1, (), (b,), False, ffn0, 2)
        ffn0 += 2
    settle(1, other)

    ucols = 256
    unit_chunks = units // 2 // ucols

    def expand(g, h, c):
        x = xm[h]
        lanes = pl.ds(pl.multiple_of(c * ucols, ucols), ucols)
        gate = jnp.dot(x, full[g, :, lanes], preferred_element_type=jnp.float32)
        lanes = pl.ds(pl.multiple_of(units // 2 + c * ucols, ucols), ucols)
        up = jnp.dot(x, full[g, :, lanes], preferred_element_type=jnp.float32)
        lanes = pl.ds(pl.multiple_of((g - 1) * (units // 2) + c * ucols, ucols), ucols)
        hf[h, :, lanes] = (jax.nn.silu(gate) * up).astype(jnp.bfloat16)

    first_done = 2 * per_stage + head
    second_done = 3 * per_stage + head
    ticks(min(ffn0, first_done), first_done)
    ffn1 = max(ffn0, first_done)

    @pl.loop(0, chips)
    def _(slot):
        near_wait(1, slot)

    @pl.loop(0, unit_chunks)
    def _(c):
        expand(1, 1, c)
        tick(ffn1 + c)

    ffn2 = ffn1 + unit_chunks
    ticks(min(ffn2, second_done), second_done)

    @pl.loop(0, chips)
    def _(slot):
        near_wait(2, slot)

    @pl.loop(0, unit_chunks)
    def _(c):
        expand(2, 1, c)
        tick(second_done + c)

    def feature_chip(slot):
        d = (slot + 1) // 2
        return chip_at(jnp.where(slot % 2 == 1, -d, d))

    def partial_of(h, chip):
        weight = full[stages - 1, pl.ds(pl.multiple_of(chip * span, span), span), :]
        return matmul_t(hf[h], weight)

    def back_copy(slot):
        chip = feature_chip(slot)
        return remote(part.at[chip], back.at[chip], back_send.at[slot], back_recv.at[slot], across)

    down0 = second_done + unit_chunks
    distance1 = (stages - 1) * per_stage + head + PIECES

    @pl.loop(0, chips)
    def _(slot):
        @pl.when(slot == 1)
        def _():
            ticks(down0, distance1)

        @pl.when(jnp.logical_and(slot % 2 == 1, jnp.logical_and(slot > 1, slot < chips - 1)))
        def _():
            @pl.loop(0, PIECES)
            def _(i):
                tick(distance1 + (slot // 2 - 1) * PIECES + i)

        @pl.when(slot == chips - 1)
        def _():
            ticks(stages * per_stage + PIECES, stages * per_stage + head)

        near_wait(stages - 1, slot)
        chip = feature_chip(slot)
        part[chip] = partial_of(1, chip).astype(jnp.bfloat16)
        back_copy(slot).start()

    for b in all_blocks:
        hid_copy(b, 1).wait_recv()
    mixed(0, all_blocks, all_blocks, True)
    settle(0, mine)

    @pl.loop(0, 2 * unit_chunks)
    def _(c):
        expand(1 + c // unit_chunks, 0, c % unit_chunks)

    @pl.loop(0, chips)
    def _(chip):
        lanes = pl.ds(pl.multiple_of(chip * span, span), span)
        total[:, lanes] = partial_of(0, chip).astype(jnp.bfloat16).astype(jnp.float32)

    @pl.loop(0, chips)
    def _(slot):
        back_copy(slot).wait_recv()

    @pl.loop(0, half // chunk)
    def _(i):
        rows = pl.ds(pl.multiple_of(i * chunk, chunk), chunk)
        came = jnp.concatenate([back[chip, rows, :] for chip in range(chips)], axis=1)
        summed = total[rows, :] + came.astype(jnp.float32)
        middle = mine[rows, :].astype(jnp.float32)
        mine[rows, :] = (middle + normed(summed, gains[3])).astype(jnp.bfloat16)
        pltpu.make_async_copy(mine.at[rows, :], out_ref.at[rows, :], out_sem.at[i]).start()

    for g in range(stages):
        ref = shard_rows(g, 0, 0)
        for way in range(2):
            for s in range(reach):
                sent = ref if s < reach - 1 else full.at[g, pl.ds(0, depth // 2), :]
                remote(
                    sent, sent, ring_send.at[way, g, s], ring_recv.at[way, g, s, 0], targets[way]
                ).wait_send()
        for slot in range(chips):
            remote(ref, ref, near_send.at[g, slot], near_recv.at[g, slot], partner).wait_send()
    remote(mine, other, tok_send.at[0], tok_recv.at[0], across).wait_send()
    ref = far_out.at[pl.ds(0, chips * depth), :]
    remote(ref, ref, cross_send.at[0], cross_recv.at[0], across).wait_send()
    remote(ref, ref, share_send.at[0], share_recv.at[0], partner).wait_send()
    for b in range(blocks):
        for h in range(2):
            hid_copy(b, h).wait_send()
    for i in range(half // chunk):
        rows = pl.ds(i * chunk, chunk)
        pltpu.make_async_copy(mine.at[rows, :], out_ref.at[rows, :], out_sem.at[i]).wait()
    for slot in range(chips):
        back_copy(slot).wait_send()


def paired_device(
    tokens,
    pre_mix_gain,
    post_mix_gain,
    pre_ffn_gain,
    post_ffn_gain,
    w_branch,
    w_gelu,
    conv_weight,
    w_rec,
    w_inp,
    decay,
    out_weight_t,
    w_gate,
    w_up,
    down_weight_t,
):
    half, model = tokens.shape
    depth, channels = w_branch.shape
    units = w_gate.shape[1]
    size = lax.axis_size("fs")
    chips = size // 2
    group = w_rec.shape[2]
    width = min(256, channels)
    blocks = channels // width
    length = 2 * half
    bf16 = functools.partial(pltpu.VMEM, dtype=jnp.bfloat16)
    f32 = functools.partial(pltpu.VMEM, dtype=jnp.float32)
    dma = pltpu.SemaphoreType.DMA
    stages = 4
    chunks = half // 128
    groups = channels // group
    reach = chips // 2
    hbm = pl.BlockSpec(memory_space=pl.ANY)
    gains = (pre_mix_gain, post_mix_gain, pre_ffn_gain, post_ffn_gain)
    return pl.pallas_call(
        functools.partial(layer_kernel, size),
        out_shape=jax.ShapeDtypeStruct((half, model), jnp.bfloat16),
        in_specs=[hbm] * 15,
        out_specs=hbm,
        scratch_shapes=[
            bf16((half, model)),
            f32((4, 1, model)),
            bf16(conv_weight.shape),
            bf16((groups, group, 4 * group)),
            f32(decay.shape),
            bf16((stages, model, 3 * channels)),
            bf16((model, channels)),
            bf16((half, model)),
            bf16((2, half, model)),
            f32((blocks, length + 16, width)),
            bf16((2, blocks, half, width)),
        ]
        + [f32((width // group, length, group)) for i in range(4)]
        + [
            bf16((blocks, 2, half, width)),
            bf16((blocks, 2, half, width)),
            f32((half, model)),
            bf16((2, half, units)),
            bf16((chips, half, 2 * depth)),
            bf16((chips, half, 2 * depth)),
            dma((2, stages, reach)),
            dma((2, stages, reach, PIECES)),
            dma((stages, chips)),
            dma((stages, chips)),
            dma((8,)),
            dma((6 + 4 * groups,)),
            dma((chunks,)),
            dma((chunks,)),
            dma((1,)),
            dma((TOKEN_PIECES,)),
            dma((1,)),
            dma((1,)),
            dma((1,)),
            dma((1,)),
            dma((blocks, 2)),
            dma((blocks, 2)),
            dma((chips,)),
            dma((chips,)),
        ],
        compiler_params=pltpu.CompilerParams(
            collective_id=0, has_side_effects=True, vmem_limit_bytes=MOST_VMEM
        ),
        cost_estimate=pl.CostEstimate(
            flops=1 << 34, bytes_accessed=1 << 26, transcendentals=1 << 24
        ),
    )(
        tokens,
        w_branch,
        w_gelu,
        out_weight_t,
        w_gate,
        w_up,
        down_weight_t,
        *(gain.reshape(1, model) for gain in gains),
        conv_weight,
        w_rec,
        w_inp,
        decay,
    )


def wide_device(
    tokens,
    pre_mix_gain,
    post_mix_gain,
    pre_ffn_gain,
    post_ffn_gain,
    w_branch,
    w_gelu,
    conv_weight,
    w_rec,
    w_inp,
    decay,
    out_weight_t,
    w_gate,
    w_up,
    down_weight_t,
):
    channels = conv_weight.shape[1]
    mix_shard = jnp.concatenate([w_branch, w_gelu, out_weight_t], axis=1)
    ffn_shard = jnp.concatenate([w_gate, w_up, down_weight_t], axis=1)
    stream = tokens.astype(jnp.float32)
    normed_in = normed(stream, pre_mix_gain).astype(jnp.bfloat16)
    mix_all = lax.all_gather(mix_shard, "fs", axis=0, tiled=True)
    whole = lax.all_gather(normed_in, "tp", axis=0, tiled=True)
    ffn_all = lax.all_gather(ffn_shard, "fs", axis=0, tiled=True)
    out_own = mix_all[:, 2 * channels :]
    hidden = mixer(whole, mix_all, conv_weight, w_rec, w_inp, decay)
    own_hidden = lax.all_to_all(hidden, "tp", split_axis=0, concat_axis=1, tiled=True)
    out_whole = lax.all_gather(out_own, "tp", axis=1, tiled=True)
    mixer_sum = matmul_t(own_hidden, out_whole)
    residual = (stream + normed(mixer_sum, post_mix_gain)).astype(jnp.bfloat16)
    middle = residual.astype(jnp.float32)
    normed_mid = normed(middle, pre_ffn_gain).astype(jnp.bfloat16)
    all_mid = lax.all_gather(normed_mid, "tp", axis=0, tiled=True)
    ffn_sum = lax.psum_scatter(
        ffn(all_mid, ffn_all), "tp", scatter_dimension=0, tiled=True
    ).astype(jnp.float32)
    return (middle + normed(ffn_sum, post_ffn_gain)).astype(jnp.bfloat16)


def solution(mesh):
    return jax.shard_map(
        paired_device if mesh.shape["tp"] == 2 else wide_device,
        mesh=mesh,
        in_specs=(
            P(("fs", "tp"), None),
            P(),
            P(),
            P(),
            P(),
            P("fs", "tp"),
            P("fs", "tp"),
            P(None, "tp"),
            P(None, "tp", None, None),
            P(None, "tp", None, None),
            P(None, "tp"),
            P("fs", "tp"),
            P("fs", "tp"),
            P("fs", "tp"),
            P("fs", "tp"),
        ),
        out_specs=P(("fs", "tp"), None),
        check_vma=False,
    )
```

```python
import functools

import jax
import jax.numpy as jnp
from jax import lax
from jax.experimental import pallas as pl
from jax.experimental.pallas import tpu as pltpu
from jax.sharding import PartitionSpec as P

EPS = 1e-06
SEGMENTS = 8
PIECES = 4
TOKEN_PIECES = 4
SCAN_TICKS = 6
PITCH_PAD = 8
MOST_VMEM = 67043328
VMEM_BYTES = 60 * 1024 * 1024


def normed(values, gain):
    factor = lax.rsqrt(jnp.mean(values * values, axis=-1, keepdims=True) + EPS)
    return values * factor * gain


def one_minus_exp(y, exp_y):
    series = 1.0 + y * (1.0 / 8.0)
    for order in (7, 6, 5, 4, 3, 2):
        series = 1.0 + y * (1.0 / order) * series
    return jnp.where(y > -0.5, -y * series, 1.0 - exp_y)


def mixer_kernel(
    x_ref, wb_ref, wg_ref, conv_ref, gates_ref, coef_ref, out_ref, pad, gel, a0, u0, a1, u1
):
    length, width = out_ref.shape
    group = gates_ref.shape[1]
    rows = 256
    pad[0:8, :] = jnp.zeros((8, width), jnp.float32)
    pad[8 + length : 16 + length, :] = jnp.zeros((8, width), jnp.float32)
    sources = ((x_ref, 0),)
    for source, base in sources:
        for start in range(0, source.shape[0], rows):
            piece = source[start : start + rows, :]
            branch = jnp.dot(piece, wb_ref[...], preferred_element_type=jnp.float32)
            gelu_in = jnp.dot(piece, wg_ref[...], preferred_element_type=jnp.float32)
            at = pl.multiple_of(base + start, rows)
            pad[pl.ds(8 + at, rows), :] = branch.astype(jnp.bfloat16).astype(jnp.float32)
            gel[pl.ds(at, rows), :] = jax.nn.gelu(
                gelu_in.astype(jnp.bfloat16).astype(jnp.float32)
            )

    for part in range(width // group):
        cols = slice(part * group, (part + 1) * group)
        taps = conv_ref[:, cols].astype(jnp.float32)
        coef = coef_ref[:, cols]
        for start in range(0, length, rows):
            summed = taps[0:1] * pad[6 + start : 6 + start + rows, cols]
            for j in range(1, 4):
                summed = summed + taps[j : j + 1] * pad[6 + j + start : 6 + j + start + rows, cols]
            conv = summed.astype(jnp.bfloat16)
            wide = conv.astype(jnp.float32)
            for d, (a_ref, u_ref) in enumerate(((a0, u0), (a1, u1))):
                gate = jnp.dot(
                    conv,
                    gates_ref[part, :, 2 * d * group : 2 * (d + 1) * group],
                    preferred_element_type=jnp.float32,
                )
                rate = jax.nn.sigmoid(gate[:, :group])
                inflow = jax.nn.sigmoid(gate[:, group:])
                log_retain = rate * coef[d : d + 1]
                retain = jnp.exp(log_retain)
                left = one_minus_exp(2.0 * log_retain, retain * retain)
                a_ref[part, start : start + rows, :] = retain
                u_ref[part, start : start + rows, :] = jnp.sqrt(left) * inflow * wide

    steps = length // SEGMENTS

    def step(t, carry):
        out = []
        for (state, decayed), (a_ref, u_ref), at in (
            (carry[0], (a0, u0), t),
            (carry[1], (a1, u1), steps - 1 - t),
        ):
            where = pl.ds(at, SEGMENTS, stride=steps)
            nstate, ndecayed = [], []
            for c in range(n):
                retain = a_ref[c, where, :]
                h = retain * state[c] + u_ref[c, where, :]
                p = retain * decayed[c]
                u_ref[c, where, :] = h
                a_ref[c, where, :] = p
                nstate.append(h)
                ndecayed.append(p)
            out.append((tuple(nstate), tuple(ndecayed)))
        return tuple(out)

    n = width // group
    zero = tuple(jnp.zeros((SEGMENTS, group), jnp.float32) for c in range(n))
    one = tuple(jnp.ones((SEGMENTS, group), jnp.float32) for c in range(n))
    ended = lax.fori_loop(0, steps, step, ((zero, one), (zero, one)), unroll=8)
    for c in range(n):
        lanes = slice(c * group, (c + 1) * group)
        blank = jnp.zeros((1, group), jnp.float32)
        entry = [[None] * SEGMENTS, [None] * SEGMENTS]
        for d, order in ((0, range(SEGMENTS)), (1, range(SEGMENTS - 1, -1, -1))):
            carry = blank
            for s in order:
                entry[d][s] = carry
                carry = ended[d][0][c][s : s + 1] + ended[d][1][c][s : s + 1] * carry
        for s in range(SEGMENTS):
            span = slice(s * steps, (s + 1) * steps)
            forward = u0[c, span, :] + a0[c, span, :] * entry[0][s]
            backward = u1[c, span, :] + a1[c, span, :] * entry[1][s]
            out_ref[span, lanes] = (gel[span, lanes] * (forward + backward)).astype(jnp.bfloat16)


def mixer(x, weights, conv_weight, w_rec, w_inp, decay):
    length, model = x.shape
    channels = conv_weight.shape[1]
    group = w_rec.shape[2]
    width = min(256, channels)
    count = channels // width
    gates = jnp.concatenate([w_rec[0], w_inp[0], w_rec[1], w_inp[1]], axis=-1)
    coef = -8.0 * jax.nn.softplus(-decay)
    f32 = functools.partial(pltpu.VMEM, dtype=jnp.float32)
    return pl.pallas_call(
        mixer_kernel,
        grid=(count,),
        out_shape=jax.ShapeDtypeStruct((length, channels), jnp.bfloat16),
        in_specs=[
            pl.BlockSpec((length, model), lambda j: (0, 0)),
            pl.BlockSpec((model, width), lambda j: (0, j)),
            pl.BlockSpec((model, width), lambda j: (0, count + j)),
            pl.BlockSpec((4, width), lambda j: (0, j)),
            pl.BlockSpec((width // group, group, 4 * group), lambda j: (j, 0, 0)),
            pl.BlockSpec((2, width), lambda j: (0, j)),
        ],
        out_specs=pl.BlockSpec((length, width), lambda j: (0, j)),
        scratch_shapes=[f32((length + 16, width)), f32((length, width))]
        + [f32((width // group, length, group)) for i in range(4)],
        compiler_params=pltpu.CompilerParams(vmem_limit_bytes=VMEM_BYTES),
        cost_estimate=pl.CostEstimate(
            flops=4 * length * model * channels + 16 * length * group * channels * 8,
            bytes_accessed=2 * (length * model + 2 * model * channels + length * channels),
            transcendentals=12 * length * channels,
        ),
    )(x, weights, weights, conv_weight, gates, coef)


def ffn_kernel(x_ref, gate_ref, up_ref, down_ref, out_ref, total):
    step = pl.program_id(0)
    gate = jnp.dot(x_ref[...], gate_ref[...], preferred_element_type=jnp.float32)
    up = jnp.dot(x_ref[...], up_ref[...], preferred_element_type=jnp.float32)
    hidden = (jax.nn.silu(gate) * up).astype(jnp.bfloat16)
    partial = lax.dot_general(
        hidden, down_ref[...], (((1,), (1,)), ((), ())), preferred_element_type=jnp.float32
    )

    @pl.when(step == 0)
    def _():
        total[...] = partial

    @pl.when(step > 0)
    def _():
        total[...] += partial

    @pl.when(step == pl.num_programs(0) - 1)
    def _():
        out_ref[...] = total[...].astype(jnp.bfloat16)


def ffn(x, weights):
    rows, model = x.shape
    units = weights.shape[1] // 3
    width = 256 if units % 256 == 0 else 128
    count = units // width
    return pl.pallas_call(
        ffn_kernel,
        grid=(count,),
        out_shape=jax.ShapeDtypeStruct((rows, model), jnp.bfloat16),
        in_specs=[
            pl.BlockSpec((rows, model), lambda j: (0, 0)),
            pl.BlockSpec((model, width), lambda j: (0, j)),
            pl.BlockSpec((model, width), lambda j: (0, count + j)),
            pl.BlockSpec((model, width), lambda j: (0, 2 * count + j)),
        ],
        out_specs=pl.BlockSpec((rows, model), lambda j: (0, 0)),
        scratch_shapes=[pltpu.VMEM((rows, model), jnp.float32)],
        compiler_params=pltpu.CompilerParams(vmem_limit_bytes=VMEM_BYTES),
        cost_estimate=pl.CostEstimate(
            flops=6 * rows * model * units,
            bytes_accessed=2 * (2 * rows * model + 3 * model * units),
            transcendentals=rows * units,
        ),
    )(x, weights, weights, weights)


def matmul_t(rows, weight_t):
    return lax.dot_general(
        rows, weight_t, (((1,), (1,)), ((), ())), preferred_element_type=jnp.float32
    )


def ring_chip(place, chips):
    half = chips // 2
    turned = place // half
    row = place * (1 - turned) + (chips - 1 - place) * turned
    return row * 2 + turned


def remote(src, dst, sent, landed, device):
    return pltpu.make_async_remote_copy(
        src_ref=src,
        dst_ref=dst,
        send_sem=sent,
        recv_sem=landed,
        device_id=device,
        device_id_type=pl.DeviceIdType.MESH,
    )


def branch_on(condition, body):
    if isinstance(condition, bool):
        if condition:
            body()
    else:
        pl.when(condition)(body)


def both(first, second):
    if isinstance(first, bool) and isinstance(second, bool):
        return first and second
    return jnp.logical_and(first, second)


def either(first, second):
    if isinstance(first, bool) and isinstance(second, bool):
        return first or second
    return jnp.logical_or(first, second)


def layer_kernel(
    size,
    tokens_ref,
    branch_ref,
    gelu_ref,
    outw_ref,
    gate_ref,
    up_ref,
    down_ref,
    gain0_ref,
    gain1_ref,
    gain2_ref,
    gain3_ref,
    taps_ref,
    rec_ref,
    inp_ref,
    decay_ref,
    out_ref,
    mine,
    gains,
    conv_ref,
    gates_ref,
    coef_ref,
    full,
    far_out,
    other,
    xm,
    pad,
    gel,
    a0,
    u0,
    a1,
    u1,
    hid,
    got,
    total,
    hf,
    part,
    back,
    ring_send,
    ring_recv,
    near_send,
    near_recv,
    own_sem,
    small_sem,
    mine_sem,
    out_sem,
    tok_send,
    tok_recv,
    cross_send,
    cross_recv,
    share_send,
    share_recv,
    hid_send,
    hid_recv,
    back_send,
    back_recv,
):
    chips = size // 2
    reach = chips // 2
    stages = full.shape[0]
    depth, channels = branch_ref.shape
    prow = depth // PIECES
    half, model = tokens_ref.shape
    blocks, width = pad.shape[0], pad.shape[2]
    group = gates_ref.shape[1]
    units = hf.shape[2]
    span = 2 * depth

    me = lax.axis_index("fs")
    core = me % 2
    turned = (me // 2) % 2
    row = me // 4
    place = row * (1 - turned) + (chips - 1 - row) * turned
    column = lax.axis_index("tp")

    def chip_at(offset):
        return ring_chip((place + chips + offset) % chips, chips)

    targets = ({"fs": chip_at(1) * 2 + core}, {"fs": chip_at(-1) * 2 + core})
    partner = {"fs": me + 1 - 2 * core}
    across = {"tp": 1 - column}

    cut = units // 2
    own_rows = pl.ds(pl.multiple_of(me * depth, depth), depth)

    def own_part(g, source, lanes, at, sem):
        place_at = full.at[g, own_rows, pl.ds(at, lanes.size)]
        return pltpu.make_async_copy(source.at[:, lanes], place_at, own_sem.at[sem])

    every = pl.ds(0, channels)
    low, high = pl.ds(0, cut), pl.ds(cut, cut)
    own_copies = [
        [own_part(0, source, every, i * channels, i) for i, source in enumerate((branch_ref, gelu_ref, outw_ref))],
        [own_part(1, gate_ref, low, 0, 3), own_part(1, up_ref, low, cut, 4)],
        [own_part(2, gate_ref, high, 0, 5), own_part(2, up_ref, high, cut, 6)],
        [own_part(3, down_ref, pl.ds(0, units), 0, 7)],
    ]
    for copy in own_copies[0]:
        copy.start()
    chunk = 128
    mine_copy = pltpu.make_async_copy(tokens_ref, mine, mine_sem.at[0])
    mine_copy.start()
    small = [(source, gains.at[i]) for i, source in enumerate((gain0_ref, gain1_ref, gain2_ref, gain3_ref))]
    small += [(taps_ref, conv_ref), (decay_ref, coef_ref)]
    for d in range(2):
        for i, source in enumerate((rec_ref, inp_ref)):
            lanes = pl.ds((2 * d + i) * group, group)
            small.append((source.at[d], gates_ref.at[:, :, lanes]))
    small = [
        pltpu.make_async_copy(source, place_at, small_sem.at[i])
        for i, (source, place_at) in enumerate(small)
    ]
    for copy in small:
        copy.start()
    for copies in own_copies[1:]:
        for copy in copies:
            copy.start()

    barrier = pltpu.get_barrier_semaphore()
    for device in (*targets, partner, across):
        pl.semaphore_signal(barrier, inc=1, device_id=device, device_id_type=pl.DeviceIdType.MESH)
    pl.semaphore_wait(barrier, 4)

    def piece(g, chip, p):
        start = pl.multiple_of((chip * 2 + core) * depth + p * prow, prow)
        return full.at[g, pl.ds(start, prow), :]

    def shard_rows(g, chip, which):
        start = pl.multiple_of((chip * 2 + which) * depth, depth)
        return full.at[g, pl.ds(start, depth), :]

    def start_piece(g, p):
        src = piece(g, me // 2, p)
        dst = src
        for way in range(2):
            remote(src, dst, ring_send.at[way, g], ring_recv.at[way, g, 0, p], targets[way]).start()
        remote(src, dst, near_send.at[g], near_recv.at[g, 0], partner).start()

    def pass_piece(g, s, p):
        for way in range(2):
            ref = piece(g, chip_at(-s if way == 0 else s), p)
            slot = 2 * s - 1 + way
            remote(
                ref, ref, ring_send.at[way, g], ring_recv.at[way, g, s - 1, p], targets[way]
            ).wait_recv()

            def forward():
                remote(
                    ref, ref, ring_send.at[way, g], ring_recv.at[way, g, s, p], targets[way]
                ).start()

            mine = p < PIECES // 2 if way == 0 else p >= PIECES // 2
            branch_on(either(s < reach - 1, mine), forward)
            remote(ref, ref, near_send.at[g], near_recv.at[g, slot], partner).start()

    def last_piece(g, q):
        for way in range(2):
            p = q + way * (PIECES // 2)
            ref = piece(g, chip_at(reach), p)
            remote(
                ref,
                ref,
                ring_send.at[way, g],
                ring_recv.at[way, g, reach - 1, p],
                targets[way],
            ).wait_recv()
            remote(ref, ref, near_send.at[g], near_recv.at[g, chips - 1], partner).start()

    head = PIECES + PIECES // 2
    per_stage = head + (reach - 1) * PIECES

    def tick(e):
        g = e // per_stage
        k = e % per_stage
        branch_on(both(k < PIECES, g < stages), lambda: start_piece(g, k))
        branch_on(
            both(both(k >= PIECES, k < head), g > 0), lambda: last_piece(g - 1, k - PIECES)
        )
        branch_on(
            both(k >= head, g < stages),
            lambda: pass_piece(g, (k - head) // PIECES + 1, (k - head) % PIECES),
        )

    def ticks(first, last):
        @pl.loop(first, last)
        def _(e):
            tick(e)

    def near_wait(g, slot):
        ref = shard_rows(g, 0, 0)
        remote(ref, ref, near_send.at[g], near_recv.at[g, slot], partner).wait_recv()

    token_rows = half // TOKEN_PIECES
    for i in range(TOKEN_PIECES):
        rows = pl.ds(i * token_rows, token_rows)
        remote(tokens_ref.at[rows, :], other.at[rows, :], tok_send.at[0], tok_recv.at[i], across).start()
    for copy in own_copies[0]:
        copy.wait()
    ticks(0, PIECES)
    for copy in (*small, mine_copy):
        copy.wait()
    for copies in own_copies[1:]:
        for copy in copies:
            copy.wait()
    slow = coef_ref[...]
    coef_ref[...] = -8.0 * (jnp.maximum(-slow, 0.0) + jnp.log1p(jnp.exp(-jnp.abs(slow))))

    def norm_rows(source, h, at):
        rows = pl.ds(at, chunk)
        values = source[rows, :].astype(jnp.float32)
        xm[h, rows, :] = normed(values, gains[0]).astype(jnp.bfloat16)

    @pl.loop(0, half // chunk)
    def _(i):
        norm_rows(mine, 0, pl.multiple_of(i * chunk, chunk))

    length = 2 * half
    for b in range(blocks):
        pad[b, 0:8, :] = jnp.zeros((8, width), jnp.float32)
        pad[b, 8 + length : 16 + length, :] = jnp.zeros((8, width), jnp.float32)

    done0 = per_stage + head
    ticks(PIECES, done0)

    @pl.loop(0, chips)
    def _(slot):
        near_wait(0, slot)

    @pl.loop(0, chips)
    def _(chip):
        src = shard_rows(0, chip, core).at[:, pl.ds(2 * channels, channels)]
        dst = far_out.at[pl.ds(pl.multiple_of((chip * 2 + core) * depth, depth), depth), :]
        remote(src, dst, cross_send.at[0], cross_recv.at[0], across).start()

    prows = 256

    @pl.loop(0, 2)
    def _(h):
        @pl.loop(0, half // prows)
        def _(i):
            at = pl.multiple_of(i * prows, prows)

            @pl.when(h == 1)
            def _():
                @pl.loop(0, prows // token_rows)
                def _(q):
                    n = i * (prows // token_rows) + q
                    rows = pl.ds(pl.multiple_of(n * token_rows, token_rows), token_rows)
                    remote(
                        tokens_ref.at[rows, :],
                        other.at[rows, :],
                        tok_send.at[0],
                        tok_recv.at[n],
                        across,
                    ).wait_recv()

                @pl.loop(0, prows // chunk)
                def _(q):
                    norm_rows(other, 1, pl.multiple_of(at + q * chunk, chunk))

            x = xm[h, pl.ds(at, prows), :]
            side = jnp.where(h == 0, column, 1 - column)
            base = pl.multiple_of(8 + side * half + at, 8)
            for b in range(blocks):
                lanes = slice(b * width, (b + 1) * width)
                branch = jnp.dot(x, full[0, :, lanes], preferred_element_type=jnp.float32)
                pad[b, pl.ds(base, prows), :] = branch.astype(jnp.bfloat16).astype(jnp.float32)
                lanes = slice(channels + b * width, channels + (b + 1) * width)
                gelu_in = jnp.dot(x, full[0, :, lanes], preferred_element_type=jnp.float32)
                gelu_in = gelu_in.astype(jnp.bfloat16).astype(jnp.float32)
                gel[h, b, pl.ds(at, prows), :] = jax.nn.gelu(gelu_in).astype(jnp.bfloat16)

            @pl.when(h * (half // prows) + i < 2 * (half // prows) - 1)
            def _():
                ticks(done0 + h * 4 + i * 2, done0 + h * 4 + i * 2 + 2)

    scan0 = done0 + 2 * (2 * (half // prows) - 1)
    parts = width // group
    steps = length // SEGMENTS
    pitch = steps + PITCH_PAD
    crows = 256

    def hid_copy(b, h):
        return remote(
            hid.at[b, h], got.at[b, h], hid_send.at[0], hid_recv.at[b, h], across
        )

    @pl.loop(0, blocks)
    def _(b):
        at = scan0 + b * SCAN_TICKS
        count = 0
        for n in range(parts):
            lanes = slice(n * group, (n + 1) * group)
            table = pl.ds(pl.multiple_of(b * width + n * group, group), group)
            taps = conv_ref[:, table].astype(jnp.float32)
            coef = coef_ref[:, table]
            for start in range(0, length, crows):
                summed = taps[0:1] * pad[b, 6 + start : 6 + start + crows, lanes]
                for j in range(1, 4):
                    first = 6 + j + start
                    summed = summed + taps[j : j + 1] * pad[b, first : first + crows, lanes]
                conv = summed.astype(jnp.bfloat16)
                wide = conv.astype(jnp.float32)
                for d, (a_ref, u_ref) in enumerate(((a0, u0), (a1, u1))):
                    gate = jnp.dot(
                        conv,
                        gates_ref[b * parts + n, :, 2 * d * group : 2 * (d + 1) * group],
                        preferred_element_type=jnp.float32,
                    )
                    rate = jax.nn.sigmoid(gate[:, :group])
                    inflow = jax.nn.sigmoid(gate[:, group:])
                    log_retain = rate * coef[d : d + 1]
                    retain = jnp.exp(log_retain)
                    left = one_minus_exp(2.0 * log_retain, retain * retain)
                    feed = jnp.sqrt(left) * inflow * wide
                    for q in range(crows // steps):
                        first = (start // steps + q) * pitch
                        a_ref[n, first : first + steps, :] = retain[q * steps : (q + 1) * steps]
                        u_ref[n, first : first + steps, :] = feed[q * steps : (q + 1) * steps]
                if (start // crows) % 2 == 1:
                    tick(at + count)
                    count += 1

        def step(t, carry):
            out = []
            for (state, decayed), (a_ref, u_ref), when in (
                (carry[0], (a0, u0), t),
                (carry[1], (a1, u1), steps - 1 - t),
            ):
                where = pl.ds(when, SEGMENTS, stride=pitch)
                nstate, ndecayed = [], []
                for n in range(parts):
                    retain = a_ref[n, where, :]
                    h = retain * state[n] + u_ref[n, where, :]
                    p = retain * decayed[n]
                    u_ref[n, where, :] = h
                    a_ref[n, where, :] = p
                    nstate.append(h)
                    ndecayed.append(p)
                out.append((tuple(nstate), tuple(ndecayed)))
            return tuple(out)

        zero = tuple(jnp.zeros((SEGMENTS, group), jnp.float32) for n in range(parts))
        one = tuple(jnp.ones((SEGMENTS, group), jnp.float32) for n in range(parts))
        ended = ((zero, one), (zero, one))
        for run in range(2):
            first, last = run * steps // 2, (run + 1) * steps // 2
            ended = lax.fori_loop(first, last, step, ended, unroll=8)
            if run == 0:
                tick(at + count)
                count += 1
        per_half = SEGMENTS // 2
        for n in range(parts):
            lanes = slice(n * group, (n + 1) * group)
            blank = jnp.zeros((1, group), jnp.float32)
            entry = [[None] * SEGMENTS, [None] * SEGMENTS]
            for d, order in ((0, range(SEGMENTS)), (1, range(SEGMENTS - 1, -1, -1))):
                carry = blank
                for s in order:
                    entry[d][s] = carry
                    carry = ended[d][0][n][s : s + 1] + ended[d][1][n][s : s + 1] * carry
            for s in range(SEGMENTS):
                rows = slice(s * pitch, s * pitch + steps)
                local = slice((s % per_half) * steps, (s % per_half + 1) * steps)
                which = jnp.where(column == s // per_half, 0, 1)
                forward = u0[n, rows, :] + a0[n, rows, :] * entry[0][s]
                backward = u1[n, rows, :] + a1[n, rows, :] * entry[1][s]
                gate = gel[which, b, local, lanes].astype(jnp.float32)
                hid[b, which, local, lanes] = (gate * (forward + backward)).astype(jnp.bfloat16)
        tick(at + count)
        count += 1
        assert count == SCAN_TICKS
        hid_copy(b, 0).start()

    for b in range(blocks):
        hid_copy(b, 1).start()
    out0 = scan0 + blocks * SCAN_TICKS

    ocols = 256

    def mixed(h, own_blocks, far_blocks, fresh, e0=0, count=0):
        left = [hid[b, h] for b in own_blocks]
        left = jnp.concatenate(left, axis=1) if left else None
        right = [got[b, 1 - h] for b in far_blocks]
        right = jnp.concatenate(right, axis=1) if right else None
        parts_n = model // ocols

        @pl.loop(0, parts_n)
        def _(n):
            rows = pl.ds(pl.multiple_of(n * ocols, ocols), ocols)
            lanes = rows
            summed = None if fresh else total[:, lanes]
            if left is not None:
                first = 2 * channels + own_blocks[0] * width
                term = matmul_t(left, full[0, rows, first : first + len(own_blocks) * width])
                summed = term if summed is None else summed + term
            if right is not None:
                first = far_blocks[0] * width
                term = matmul_t(right, far_out[rows, first : first + len(far_blocks) * width])
                summed = term if summed is None else summed + term
            total[:, lanes] = summed
            if count:
                every_n = parts_n // count

                @pl.when(n % every_n == every_n - 1)
                def _():
                    tick(e0 + n // every_n)

    def settle(h, source):
        @pl.loop(0, half // chunk)
        def _(i):
            rows = pl.ds(pl.multiple_of(i * chunk, chunk), chunk)
            stream = source[rows, :].astype(jnp.float32)
            residual = stream + normed(total[rows, :], gains[1])
            residual = residual.astype(jnp.bfloat16)
            if h == 0:
                source[rows, :] = residual
            middle = normed(residual.astype(jnp.float32), gains[2])
            xm[h, rows, :] = middle.astype(jnp.bfloat16)

    all_blocks = tuple(range(blocks))
    mixed(1, all_blocks, (), True, out0, 2)
    ticks(out0 + 2, out0 + 4)

    ref = far_out.at[pl.ds(0, chips * depth), :]
    remote(ref, ref, cross_send.at[0], cross_recv.at[0], across).wait_recv()

    @pl.loop(0, chips)
    def _(chip):
        ref = far_out.at[pl.ds(pl.multiple_of((chip * 2 + core) * depth, depth), depth), :]
        remote(ref, ref, share_send.at[0], share_recv.at[0], partner).start()

    ffn0 = out0 + 4
    for b in all_blocks:
        ticks(ffn0, ffn0 + b + 1)
        hid_copy(b, 0).wait_recv()
        if b == 0:
            ref = far_out.at[pl.ds(0, chips * depth), :]
            remote(ref, ref, share_send.at[0], share_recv.at[0], partner).wait_recv()
        mixed(1, (), (b,), False, ffn0 + b + 1, 1)
        ffn0 += b + 2
    settle(1, other)

    ucols = 256
    unit_chunks = units // 2 // ucols

    def expand(g, h, c):
        x = xm[h]
        lanes = pl.ds(pl.multiple_of(c * ucols, ucols), ucols)
        gate = jnp.dot(x, full[g, :, lanes], preferred_element_type=jnp.float32)
        lanes = pl.ds(pl.multiple_of(units // 2 + c * ucols, ucols), ucols)
        up = jnp.dot(x, full[g, :, lanes], preferred_element_type=jnp.float32)
        lanes = pl.ds(pl.multiple_of((g - 1) * (units // 2) + c * ucols, ucols), ucols)
        hf[h, :, lanes] = (jax.nn.silu(gate) * up).astype(jnp.bfloat16)

    first_done = 2 * per_stage + head
    second_done = 3 * per_stage + head
    ticks(min(ffn0, first_done), first_done)
    ffn1 = max(ffn0, first_done)

    @pl.loop(0, chips)
    def _(slot):
        near_wait(1, slot)

    @pl.loop(0, unit_chunks)
    def _(c):
        expand(1, 1, c)
        tick(ffn1 + c)

    def feature_chip(slot):
        d = (slot + 1) // 2
        return chip_at(jnp.where(slot % 2 == 1, -d, d))

    def expand_part(g, h, c, slots, fresh, last):
        rows = [pl.ds(pl.multiple_of(feature_chip(slot) * span, span), span) for slot in slots]
        x = jnp.concatenate([xm[h, :, at] for at in rows], axis=1)
        summed = []
        for side in range(2):
            lanes = pl.ds(pl.multiple_of(side * cut + c * ucols, ucols), ucols)
            w = jnp.concatenate([full[g, at, lanes] for at in rows], axis=0)
            term = jnp.dot(x, w, preferred_element_type=jnp.float32)
            if not fresh:
                term = total[:, lanes] + term
            if last:
                summed.append(term)
            else:
                total[:, lanes] = term
        if last:
            lanes = pl.ds(pl.multiple_of((g - 1) * cut + c * ucols, ucols), ucols)
            hf[h, :, lanes] = (jax.nn.silu(summed[0]) * summed[1]).astype(jnp.bfloat16)

    ffn2 = ffn1 + unit_chunks
    before = second_done - PIECES // 2
    ticks(min(ffn2, before), before)
    parts_b = (tuple(range(chips - 3)), (chips - 3, chips - 2), (chips - 1,))
    for n, slots in enumerate(parts_b):
        if n == len(parts_b) - 1:
            ticks(before, second_done)
        for slot in slots:
            near_wait(2, slot)

        @pl.loop(0, unit_chunks)
        def _(c):
            expand_part(2, 1, c, slots, n == 0, n == len(parts_b) - 1)

    def partial_of(h, chip):
        weight = full[stages - 1, pl.ds(pl.multiple_of(chip * span, span), span), :]
        return matmul_t(hf[h], weight)

    def back_copy(slot):
        chip = feature_chip(slot)
        return remote(part.at[chip], back.at[chip], back_send.at[0], back_recv.at[slot], across)

    down0 = second_done
    distance1 = (stages - 1) * per_stage + head + PIECES

    @pl.loop(0, chips)
    def _(slot):
        @pl.when(slot == 1)
        def _():
            ticks(down0, distance1)

        @pl.when(jnp.logical_and(slot % 2 == 1, jnp.logical_and(slot > 1, slot < chips - 1)))
        def _():
            @pl.loop(0, PIECES)
            def _(i):
                tick(distance1 + (slot // 2 - 1) * PIECES + i)

        @pl.when(slot == chips - 1)
        def _():
            ticks(stages * per_stage + PIECES, stages * per_stage + head)

        near_wait(stages - 1, slot)
        chip = feature_chip(slot)
        part[chip] = partial_of(1, chip).astype(jnp.bfloat16)
        back_copy(slot).start()

    for b in all_blocks:
        hid_copy(b, 1).wait_recv()
    mixed(0, all_blocks, all_blocks, True)
    settle(0, mine)

    @pl.loop(0, 2 * unit_chunks)
    def _(c):
        expand(1 + c // unit_chunks, 0, c % unit_chunks)

    @pl.loop(0, chips)
    def _(chip):
        lanes = pl.ds(pl.multiple_of(chip * span, span), span)
        total[:, lanes] = partial_of(0, chip).astype(jnp.bfloat16).astype(jnp.float32)

    @pl.loop(0, chips)
    def _(slot):
        back_copy(slot).wait_recv()

    @pl.loop(0, half // chunk)
    def _(i):
        rows = pl.ds(pl.multiple_of(i * chunk, chunk), chunk)
        came = jnp.concatenate([back[chip, rows, :] for chip in range(chips)], axis=1)
        summed = total[rows, :] + came.astype(jnp.float32)
        middle = mine[rows, :].astype(jnp.float32)
        mine[rows, :] = (middle + normed(summed, gains[3])).astype(jnp.bfloat16)
        pltpu.make_async_copy(mine.at[rows, :], out_ref.at[rows, :], out_sem.at[0]).start()

    for g in range(stages):
        rows = full.at[g, pl.ds(0, (reach - 1) * depth + depth // 2), :]
        for way in range(2):
            remote(
                rows, rows, ring_send.at[way, g], ring_recv.at[way, g, 0, 0], targets[way]
            ).wait_send()
        rows = full.at[g, pl.ds(0, chips * depth), :]
        remote(rows, rows, near_send.at[g], near_recv.at[g, 0], partner).wait_send()
    remote(mine, other, tok_send.at[0], tok_recv.at[0], across).wait_send()
    ref = far_out.at[pl.ds(0, chips * depth), :]
    remote(ref, ref, cross_send.at[0], cross_recv.at[0], across).wait_send()
    remote(ref, ref, share_send.at[0], share_recv.at[0], partner).wait_send()
    remote(hid, got, hid_send.at[0], hid_recv.at[0, 0], across).wait_send()
    remote(part, back, back_send.at[0], back_recv.at[0], across).wait_send()
    pltpu.make_async_copy(mine, out_ref, out_sem.at[0]).wait()


def paired_device(
    tokens,
    pre_mix_gain,
    post_mix_gain,
    pre_ffn_gain,
    post_ffn_gain,
    w_branch,
    w_gelu,
    conv_weight,
    w_rec,
    w_inp,
    decay,
    out_weight_t,
    w_gate,
    w_up,
    down_weight_t,
):
    half, model = tokens.shape
    depth, channels = w_branch.shape
    units = w_gate.shape[1]
    size = lax.axis_size("fs")
    chips = size // 2
    group = w_rec.shape[2]
    width = min(256, channels)
    blocks = channels // width
    length = 2 * half
    bf16 = functools.partial(pltpu.VMEM, dtype=jnp.bfloat16)
    f32 = functools.partial(pltpu.VMEM, dtype=jnp.float32)
    dma = pltpu.SemaphoreType.DMA
    stages = 4
    groups = channels // group
    reach = chips // 2
    hbm = pl.BlockSpec(memory_space=pl.ANY)
    gains = (pre_mix_gain, post_mix_gain, pre_ffn_gain, post_ffn_gain)
    return pl.pallas_call(
        functools.partial(layer_kernel, size),
        out_shape=jax.ShapeDtypeStruct((half, model), jnp.bfloat16),
        in_specs=[hbm] * 15,
        out_specs=hbm,
        scratch_shapes=[
            bf16((half, model)),
            f32((4, 1, model)),
            bf16(conv_weight.shape),
            bf16((groups, group, 4 * group)),
            f32(decay.shape),
            bf16((stages, model, 3 * channels)),
            bf16((model, channels)),
            bf16((half, model)),
            bf16((2, half, model)),
            f32((blocks, length + 16, width)),
            bf16((2, blocks, half, width)),
        ]
        + [f32((width // group, length + SEGMENTS * PITCH_PAD, group)) for i in range(4)]
        + [
            bf16((blocks, 2, half, width)),
            bf16((blocks, 2, half, width)),
            f32((half, model)),
            bf16((2, half, units)),
            bf16((chips, half, 2 * depth)),
            bf16((chips, half, 2 * depth)),
            dma((2, stages)),
            dma((2, stages, reach, PIECES)),
            dma((stages,)),
            dma((stages, chips)),
            dma((8,)),
            dma((10,)),
            dma((1,)),
            dma((1,)),
            dma((1,)),
            dma((TOKEN_PIECES,)),
            dma((1,)),
            dma((1,)),
            dma((1,)),
            dma((1,)),
            dma((1,)),
            dma((blocks, 2)),
            dma((1,)),
            dma((chips,)),
        ],
        compiler_params=pltpu.CompilerParams(
            collective_id=0, has_side_effects=True, vmem_limit_bytes=MOST_VMEM
        ),
        cost_estimate=pl.CostEstimate(
            flops=1 << 34, bytes_accessed=1 << 26, transcendentals=1 << 24
        ),
    )(
        tokens,
        w_branch,
        w_gelu,
        out_weight_t,
        w_gate,
        w_up,
        down_weight_t,
        *(gain.reshape(1, model) for gain in gains),
        conv_weight,
        w_rec,
        w_inp,
        decay,
    )


def wide_device(
    tokens,
    pre_mix_gain,
    post_mix_gain,
    pre_ffn_gain,
    post_ffn_gain,
    w_branch,
    w_gelu,
    conv_weight,
    w_rec,
    w_inp,
    decay,
    out_weight_t,
    w_gate,
    w_up,
    down_weight_t,
):
    channels = conv_weight.shape[1]
    mix_shard = jnp.concatenate([w_branch, w_gelu, out_weight_t], axis=1)
    ffn_shard = jnp.concatenate([w_gate, w_up, down_weight_t], axis=1)
    stream = tokens.astype(jnp.float32)
    normed_in = normed(stream, pre_mix_gain).astype(jnp.bfloat16)
    mix_all = lax.all_gather(mix_shard, "fs", axis=0, tiled=True)
    whole = lax.all_gather(normed_in, "tp", axis=0, tiled=True)
    ffn_all = lax.all_gather(ffn_shard, "fs", axis=0, tiled=True)
    out_own = mix_all[:, 2 * channels :]
    hidden = mixer(whole, mix_all, conv_weight, w_rec, w_inp, decay)
    own_hidden = lax.all_to_all(hidden, "tp", split_axis=0, concat_axis=1, tiled=True)
    out_whole = lax.all_gather(out_own, "tp", axis=1, tiled=True)
    mixer_sum = matmul_t(own_hidden, out_whole)
    residual = (stream + normed(mixer_sum, post_mix_gain)).astype(jnp.bfloat16)
    middle = residual.astype(jnp.float32)
    normed_mid = normed(middle, pre_ffn_gain).astype(jnp.bfloat16)
    all_mid = lax.all_gather(normed_mid, "tp", axis=0, tiled=True)
    ffn_sum = lax.psum_scatter(
        ffn(all_mid, ffn_all), "tp", scatter_dimension=0, tiled=True
    ).astype(jnp.float32)
    return (middle + normed(ffn_sum, post_ffn_gain)).astype(jnp.bfloat16)


def solution(mesh):
    return jax.shard_map(
        paired_device if mesh.shape["tp"] == 2 else wide_device,
        mesh=mesh,
        in_specs=(
            P(("fs", "tp"), None),
            P(),
            P(),
            P(),
            P(),
            P("fs", "tp"),
            P("fs", "tp"),
            P(None, "tp"),
            P(None, "tp", None, None),
            P(None, "tp", None, None),
            P(None, "tp"),
            P("fs", "tp"),
            P("fs", "tp"),
            P("fs", "tp"),
            P("fs", "tp"),
        ),
        out_specs=P(("fs", "tp"), None),
        check_vma=False,
    )
```

```python
import functools

import jax
import jax.numpy as jnp
from jax import lax
from jax.experimental import pallas as pl
from jax.experimental.pallas import tpu as pltpu
from jax.sharding import PartitionSpec as P

EPS = 1e-06
SEGMENTS = 8
PIECES = 4
TOKEN_PIECES = 4
SCAN_TICKS = 6
PITCH_PAD = 8
MOST_VMEM = 67043328
VMEM_BYTES = 60 * 1024 * 1024


def normed(values, gain):
    factor = lax.rsqrt(jnp.mean(values * values, axis=-1, keepdims=True) + EPS)
    return values * factor * gain


def one_minus_exp(y, exp_y):
    series = 1.0 + y * (1.0 / 8.0)
    for order in (7, 6, 5, 4, 3, 2):
        series = 1.0 + y * (1.0 / order) * series
    return jnp.where(y > -0.5, -y * series, 1.0 - exp_y)


def mixer_kernel(
    x_ref, wb_ref, wg_ref, conv_ref, gates_ref, coef_ref, out_ref, pad, gel, a0, u0, a1, u1
):
    length, width = out_ref.shape
    group = gates_ref.shape[1]
    rows = 256
    pad[0:8, :] = jnp.zeros((8, width), jnp.float32)
    pad[8 + length : 16 + length, :] = jnp.zeros((8, width), jnp.float32)
    sources = ((x_ref, 0),)
    for source, base in sources:
        for start in range(0, source.shape[0], rows):
            piece = source[start : start + rows, :]
            branch = jnp.dot(piece, wb_ref[...], preferred_element_type=jnp.float32)
            gelu_in = jnp.dot(piece, wg_ref[...], preferred_element_type=jnp.float32)
            at = pl.multiple_of(base + start, rows)
            pad[pl.ds(8 + at, rows), :] = branch.astype(jnp.bfloat16).astype(jnp.float32)
            gel[pl.ds(at, rows), :] = jax.nn.gelu(
                gelu_in.astype(jnp.bfloat16).astype(jnp.float32)
            )

    for part in range(width // group):
        cols = slice(part * group, (part + 1) * group)
        taps = conv_ref[:, cols].astype(jnp.float32)
        coef = coef_ref[:, cols]
        for start in range(0, length, rows):
            summed = taps[0:1] * pad[6 + start : 6 + start + rows, cols]
            for j in range(1, 4):
                summed = summed + taps[j : j + 1] * pad[6 + j + start : 6 + j + start + rows, cols]
            conv = summed.astype(jnp.bfloat16)
            wide = conv.astype(jnp.float32)
            for d, (a_ref, u_ref) in enumerate(((a0, u0), (a1, u1))):
                gate = jnp.dot(
                    conv,
                    gates_ref[part, :, 2 * d * group : 2 * (d + 1) * group],
                    preferred_element_type=jnp.float32,
                )
                rate = jax.nn.sigmoid(gate[:, :group])
                inflow = jax.nn.sigmoid(gate[:, group:])
                log_retain = rate * coef[d : d + 1]
                retain = jnp.exp(log_retain)
                left = one_minus_exp(2.0 * log_retain, retain * retain)
                a_ref[part, start : start + rows, :] = retain
                u_ref[part, start : start + rows, :] = jnp.sqrt(left) * inflow * wide

    steps = length // SEGMENTS

    def step(t, carry):
        out = []
        for (state, decayed), (a_ref, u_ref), at in (
            (carry[0], (a0, u0), t),
            (carry[1], (a1, u1), steps - 1 - t),
        ):
            where = pl.ds(at, SEGMENTS, stride=steps)
            nstate, ndecayed = [], []
            for c in range(n):
                retain = a_ref[c, where, :]
                h = retain * state[c] + u_ref[c, where, :]
                p = retain * decayed[c]
                u_ref[c, where, :] = h
                a_ref[c, where, :] = p
                nstate.append(h)
                ndecayed.append(p)
            out.append((tuple(nstate), tuple(ndecayed)))
        return tuple(out)

    n = width // group
    zero = tuple(jnp.zeros((SEGMENTS, group), jnp.float32) for c in range(n))
    one = tuple(jnp.ones((SEGMENTS, group), jnp.float32) for c in range(n))
    ended = lax.fori_loop(0, steps, step, ((zero, one), (zero, one)), unroll=8)
    for c in range(n):
        lanes = slice(c * group, (c + 1) * group)
        blank = jnp.zeros((1, group), jnp.float32)
        entry = [[None] * SEGMENTS, [None] * SEGMENTS]
        for d, order in ((0, range(SEGMENTS)), (1, range(SEGMENTS - 1, -1, -1))):
            carry = blank
            for s in order:
                entry[d][s] = carry
                carry = ended[d][0][c][s : s + 1] + ended[d][1][c][s : s + 1] * carry
        for s in range(SEGMENTS):
            span = slice(s * steps, (s + 1) * steps)
            forward = u0[c, span, :] + a0[c, span, :] * entry[0][s]
            backward = u1[c, span, :] + a1[c, span, :] * entry[1][s]
            out_ref[span, lanes] = (gel[span, lanes] * (forward + backward)).astype(jnp.bfloat16)


def mixer(x, weights, conv_weight, w_rec, w_inp, decay):
    length, model = x.shape
    channels = conv_weight.shape[1]
    group = w_rec.shape[2]
    width = min(256, channels)
    count = channels // width
    gates = jnp.concatenate([w_rec[0], w_inp[0], w_rec[1], w_inp[1]], axis=-1)
    coef = -8.0 * jax.nn.softplus(-decay)
    f32 = functools.partial(pltpu.VMEM, dtype=jnp.float32)
    return pl.pallas_call(
        mixer_kernel,
        grid=(count,),
        out_shape=jax.ShapeDtypeStruct((length, channels), jnp.bfloat16),
        in_specs=[
            pl.BlockSpec((length, model), lambda j: (0, 0)),
            pl.BlockSpec((model, width), lambda j: (0, j)),
            pl.BlockSpec((model, width), lambda j: (0, count + j)),
            pl.BlockSpec((4, width), lambda j: (0, j)),
            pl.BlockSpec((width // group, group, 4 * group), lambda j: (j, 0, 0)),
            pl.BlockSpec((2, width), lambda j: (0, j)),
        ],
        out_specs=pl.BlockSpec((length, width), lambda j: (0, j)),
        scratch_shapes=[f32((length + 16, width)), f32((length, width))]
        + [f32((width // group, length, group)) for i in range(4)],
        compiler_params=pltpu.CompilerParams(vmem_limit_bytes=VMEM_BYTES),
        cost_estimate=pl.CostEstimate(
            flops=4 * length * model * channels + 16 * length * group * channels * 8,
            bytes_accessed=2 * (length * model + 2 * model * channels + length * channels),
            transcendentals=12 * length * channels,
        ),
    )(x, weights, weights, conv_weight, gates, coef)


def ffn_kernel(x_ref, gate_ref, up_ref, down_ref, out_ref, total):
    step = pl.program_id(0)
    gate = jnp.dot(x_ref[...], gate_ref[...], preferred_element_type=jnp.float32)
    up = jnp.dot(x_ref[...], up_ref[...], preferred_element_type=jnp.float32)
    hidden = (jax.nn.silu(gate) * up).astype(jnp.bfloat16)
    partial = lax.dot_general(
        hidden, down_ref[...], (((1,), (1,)), ((), ())), preferred_element_type=jnp.float32
    )

    @pl.when(step == 0)
    def _():
        total[...] = partial

    @pl.when(step > 0)
    def _():
        total[...] += partial

    @pl.when(step == pl.num_programs(0) - 1)
    def _():
        out_ref[...] = total[...].astype(jnp.bfloat16)


def ffn(x, weights):
    rows, model = x.shape
    units = weights.shape[1] // 3
    width = 256 if units % 256 == 0 else 128
    count = units // width
    return pl.pallas_call(
        ffn_kernel,
        grid=(count,),
        out_shape=jax.ShapeDtypeStruct((rows, model), jnp.bfloat16),
        in_specs=[
            pl.BlockSpec((rows, model), lambda j: (0, 0)),
            pl.BlockSpec((model, width), lambda j: (0, j)),
            pl.BlockSpec((model, width), lambda j: (0, count + j)),
            pl.BlockSpec((model, width), lambda j: (0, 2 * count + j)),
        ],
        out_specs=pl.BlockSpec((rows, model), lambda j: (0, 0)),
        scratch_shapes=[pltpu.VMEM((rows, model), jnp.float32)],
        compiler_params=pltpu.CompilerParams(vmem_limit_bytes=VMEM_BYTES),
        cost_estimate=pl.CostEstimate(
            flops=6 * rows * model * units,
            bytes_accessed=2 * (2 * rows * model + 3 * model * units),
            transcendentals=rows * units,
        ),
    )(x, weights, weights, weights)


def matmul_t(rows, weight_t):
    return lax.dot_general(
        rows, weight_t, (((1,), (1,)), ((), ())), preferred_element_type=jnp.float32
    )


def ring_chip(place, chips):
    half = chips // 2
    turned = place // half
    row = place * (1 - turned) + (chips - 1 - place) * turned
    return row * 2 + turned


def remote(src, dst, sent, landed, device):
    return pltpu.make_async_remote_copy(
        src_ref=src,
        dst_ref=dst,
        send_sem=sent,
        recv_sem=landed,
        device_id=device,
        device_id_type=pl.DeviceIdType.MESH,
    )


def branch_on(condition, body):
    if isinstance(condition, bool):
        if condition:
            body()
    else:
        pl.when(condition)(body)


def both(first, second):
    if isinstance(first, bool) and isinstance(second, bool):
        return first and second
    return jnp.logical_and(first, second)


def either(first, second):
    if isinstance(first, bool) and isinstance(second, bool):
        return first or second
    return jnp.logical_or(first, second)


def layer_kernel(
    size,
    tokens_ref,
    branch_ref,
    gelu_ref,
    outw_ref,
    gate_ref,
    up_ref,
    down_ref,
    gain0_ref,
    gain1_ref,
    gain2_ref,
    gain3_ref,
    taps_ref,
    rec_ref,
    inp_ref,
    decay_ref,
    out_ref,
    mine,
    gains,
    conv_ref,
    gates_ref,
    coef_ref,
    full,
    far_out,
    other,
    xm,
    pad,
    gel,
    a0,
    u0,
    a1,
    u1,
    hid,
    got,
    total,
    squares,
    hf,
    part,
    back,
    ring_send,
    ring_recv,
    near_send,
    near_recv,
    own_sem,
    small_sem,
    mine_sem,
    out_sem,
    tok_send,
    tok_recv,
    cross_send,
    cross_recv,
    share_send,
    share_recv,
    hid_send,
    hid_recv,
    back_send,
    back_recv,
):
    chips = size // 2
    reach = chips // 2
    stages = full.shape[0]
    depth, channels = branch_ref.shape
    prow = depth // PIECES
    half, model = tokens_ref.shape
    blocks, width = pad.shape[0], pad.shape[2]
    group = gates_ref.shape[1]
    units = hf.shape[2]
    span = 2 * depth

    me = lax.axis_index("fs")
    core = me % 2
    turned = (me // 2) % 2
    row = me // 4
    place = row * (1 - turned) + (chips - 1 - row) * turned
    column = lax.axis_index("tp")

    def chip_at(offset):
        return ring_chip((place + chips + offset) % chips, chips)

    targets = ({"fs": chip_at(1) * 2 + core}, {"fs": chip_at(-1) * 2 + core})
    partner = {"fs": me + 1 - 2 * core}
    across = {"tp": 1 - column}

    cut = units // 2
    own_rows = pl.ds(pl.multiple_of(me * depth, depth), depth)

    def own_part(g, source, lanes, at, sem):
        place_at = full.at[g, own_rows, pl.ds(at, lanes.size)]
        return pltpu.make_async_copy(source.at[:, lanes], place_at, own_sem.at[sem])

    every = pl.ds(0, channels)
    low, high = pl.ds(0, cut), pl.ds(cut, cut)
    own_copies = [
        [own_part(0, source, every, i * channels, i) for i, source in enumerate((branch_ref, gelu_ref, outw_ref))],
        [own_part(1, gate_ref, low, 0, 3), own_part(1, up_ref, low, cut, 4)],
        [own_part(2, gate_ref, high, 0, 5), own_part(2, up_ref, high, cut, 6)],
        [own_part(3, down_ref, pl.ds(0, units), 0, 7)],
    ]
    for copy in own_copies[0]:
        copy.start()
    chunk = 128
    mine_copy = pltpu.make_async_copy(tokens_ref, mine, mine_sem.at[0])
    mine_copy.start()
    small = [(source, gains.at[i]) for i, source in enumerate((gain0_ref, gain1_ref, gain2_ref, gain3_ref))]
    small += [(taps_ref, conv_ref), (decay_ref, coef_ref)]
    for d in range(2):
        for i, source in enumerate((rec_ref, inp_ref)):
            lanes = pl.ds((2 * d + i) * group, group)
            small.append((source.at[d], gates_ref.at[:, :, lanes]))
    small = [
        pltpu.make_async_copy(source, place_at, small_sem.at[i])
        for i, (source, place_at) in enumerate(small)
    ]
    for copy in small:
        copy.start()
    for copies in own_copies[1:]:
        for copy in copies:
            copy.start()

    barrier = pltpu.get_barrier_semaphore()
    for device in (*targets, partner, across):
        pl.semaphore_signal(barrier, inc=1, device_id=device, device_id_type=pl.DeviceIdType.MESH)
    pl.semaphore_wait(barrier, 4)

    def piece(g, chip, p):
        start = pl.multiple_of((chip * 2 + core) * depth + p * prow, prow)
        return full.at[g, pl.ds(start, prow), :]

    def shard_rows(g, chip, which):
        start = pl.multiple_of((chip * 2 + which) * depth, depth)
        return full.at[g, pl.ds(start, depth), :]

    def start_piece(g, p):
        src = piece(g, me // 2, p)
        dst = src
        for way in range(2):
            remote(src, dst, ring_send.at[way, g], ring_recv.at[g, 0, p], targets[way]).start()
        remote(src, dst, near_send.at[g], near_recv.at[g, 0], partner).start()

    def landed(g, s, p):
        rows = full.at[g, pl.ds(0, 2 * prow), :]
        remote(rows, rows, ring_send.at[0, g], ring_recv.at[g, s, p], targets[0]).wait_recv()

    def pass_piece(g, s, p):
        landed(g, s - 1, p)
        for way in range(2):
            ref = piece(g, chip_at(-s if way == 0 else s), p)
            slot = 2 * s - 1 + way
            low_half = way * (PIECES // 2)

            def forward():
                index = jnp.where(s < reach - 1, p, p - low_half)
                remote(
                    ref, ref, ring_send.at[way, g], ring_recv.at[g, s, index], targets[way]
                ).start()

            mine = p < PIECES // 2 if way == 0 else p >= PIECES // 2
            branch_on(either(s < reach - 1, mine), forward)
            remote(ref, ref, near_send.at[g], near_recv.at[g, slot], partner).start()

    def last_piece(g, q):
        landed(g, reach - 1, q)
        for way in range(2):
            ref = piece(g, chip_at(reach), q + way * (PIECES // 2))
            remote(ref, ref, near_send.at[g], near_recv.at[g, chips - 1], partner).start()

    head = PIECES + PIECES // 2
    per_stage = head + (reach - 1) * PIECES

    def tick(e):
        g = e // per_stage
        k = e % per_stage
        branch_on(both(k < PIECES, g < stages), lambda: start_piece(g, k))
        branch_on(
            both(both(k >= PIECES, k < head), g > 0), lambda: last_piece(g - 1, k - PIECES)
        )
        branch_on(
            both(k >= head, g < stages),
            lambda: pass_piece(g, (k - head) // PIECES + 1, (k - head) % PIECES),
        )

    def ticks(first, last):
        @pl.loop(first, last)
        def _(e):
            tick(e)

    def near_wait(g, slot):
        ref = shard_rows(g, 0, 0)
        remote(ref, ref, near_send.at[g], near_recv.at[g, slot], partner).wait_recv()

    token_rows = half // TOKEN_PIECES
    for i in range(TOKEN_PIECES):
        rows = pl.ds(i * token_rows, token_rows)
        remote(tokens_ref.at[rows, :], other.at[rows, :], tok_send.at[0], tok_recv.at[i], across).start()
    for copy in own_copies[0]:
        copy.wait()
    ticks(0, PIECES)
    for copy in (*small, mine_copy):
        copy.wait()
    for copies in own_copies[1:]:
        for copy in copies:
            copy.wait()
    slow = coef_ref[...]
    coef_ref[...] = -8.0 * (jnp.maximum(-slow, 0.0) + jnp.log1p(jnp.exp(-jnp.abs(slow))))

    def norm_rows(source, h, at):
        rows = pl.ds(at, chunk)
        values = source[rows, :].astype(jnp.float32)
        xm[h, rows, :] = normed(values, gains[0]).astype(jnp.bfloat16)

    @pl.loop(0, half // chunk)
    def _(i):
        norm_rows(mine, 0, pl.multiple_of(i * chunk, chunk))

    length = 2 * half
    for b in range(blocks):
        pad[b, 0:8, :] = jnp.zeros((8, width), jnp.float32)
        pad[b, 8 + length : 16 + length, :] = jnp.zeros((8, width), jnp.float32)

    done0 = per_stage + head
    ticks(PIECES, done0)

    @pl.loop(0, chips)
    def _(slot):
        near_wait(0, slot)

    @pl.loop(0, chips)
    def _(chip):
        src = shard_rows(0, chip, core).at[:, pl.ds(2 * channels, channels)]
        dst = far_out.at[pl.ds(pl.multiple_of((chip * 2 + core) * depth, depth), depth), :]
        remote(src, dst, cross_send.at[0], cross_recv.at[0], across).start()

    prows = 256
    scan0 = done0 + 2 * (2 * (half // prows) - 1) + 1

    @pl.loop(0, 2)
    def _(h):
        @pl.loop(0, half // prows)
        def _(i):
            at = pl.multiple_of(i * prows, prows)

            @pl.when(h == 1)
            def _():
                @pl.loop(0, prows // token_rows)
                def _(q):
                    n = i * (prows // token_rows) + q
                    rows = pl.ds(pl.multiple_of(n * token_rows, token_rows), token_rows)
                    remote(
                        tokens_ref.at[rows, :],
                        other.at[rows, :],
                        tok_send.at[0],
                        tok_recv.at[n],
                        across,
                    ).wait_recv()

                @pl.loop(0, prows // chunk)
                def _(q):
                    norm_rows(other, 1, pl.multiple_of(at + q * chunk, chunk))

                @pl.when(i == half // prows - 1)
                def _():
                    tick(scan0 - 1)

            x = xm[h, pl.ds(at, prows), :]
            side = jnp.where(h == 0, column, 1 - column)
            base = pl.multiple_of(8 + side * half + at, 8)
            for b in range(blocks):
                lanes = slice(b * width, (b + 1) * width)
                branch = jnp.dot(x, full[0, :, lanes], preferred_element_type=jnp.float32)
                pad[b, pl.ds(base, prows), :] = branch.astype(jnp.bfloat16).astype(jnp.float32)
                lanes = slice(channels + b * width, channels + (b + 1) * width)
                gelu_in = jnp.dot(x, full[0, :, lanes], preferred_element_type=jnp.float32)
                gelu_in = gelu_in.astype(jnp.bfloat16).astype(jnp.float32)
                gel[h, b, pl.ds(at, prows), :] = jax.nn.gelu(gelu_in).astype(jnp.bfloat16)

            @pl.when(h * (half // prows) + i < 2 * (half // prows) - 1)
            def _():
                ticks(done0 + h * 4 + i * 2, done0 + h * 4 + i * 2 + 2)

    parts = width // group
    steps = length // SEGMENTS
    pitch = steps + PITCH_PAD
    crows = 256

    def hid_copy(b, h):
        return remote(
            hid.at[b, h], got.at[b, h], hid_send.at[0], hid_recv.at[b, h], across
        )

    @pl.loop(0, blocks)
    def _(b):
        at = scan0 + b * SCAN_TICKS
        count = 0
        for n in range(parts):
            lanes = slice(n * group, (n + 1) * group)
            table = pl.ds(pl.multiple_of(b * width + n * group, group), group)
            taps = conv_ref[:, table].astype(jnp.float32)
            coef = coef_ref[:, table]
            for start in range(0, length, crows):
                summed = taps[0:1] * pad[b, 6 + start : 6 + start + crows, lanes]
                for j in range(1, 4):
                    first = 6 + j + start
                    summed = summed + taps[j : j + 1] * pad[b, first : first + crows, lanes]
                conv = summed.astype(jnp.bfloat16)
                wide = conv.astype(jnp.float32)
                for d, (a_ref, u_ref) in enumerate(((a0, u0), (a1, u1))):
                    gate = jnp.dot(
                        conv,
                        gates_ref[b * parts + n, :, 2 * d * group : 2 * (d + 1) * group],
                        preferred_element_type=jnp.float32,
                    )
                    rate = jax.nn.sigmoid(gate[:, :group])
                    inflow = jax.nn.sigmoid(gate[:, group:])
                    log_retain = rate * coef[d : d + 1]
                    retain = jnp.exp(log_retain)
                    left = one_minus_exp(2.0 * log_retain, retain * retain)
                    feed = jnp.sqrt(left) * inflow * wide
                    for q in range(crows // steps):
                        first = (start // steps + q) * pitch
                        a_ref[n, first : first + steps, :] = retain[q * steps : (q + 1) * steps]
                        u_ref[n, first : first + steps, :] = feed[q * steps : (q + 1) * steps]
                if (start // crows) % 2 == 1:
                    tick(at + count)
                    count += 1

        def step(t, carry):
            out = []
            for (state, decayed), (a_ref, u_ref), when in (
                (carry[0], (a0, u0), t),
                (carry[1], (a1, u1), steps - 1 - t),
            ):
                where = pl.ds(when, SEGMENTS, stride=pitch)
                nstate, ndecayed = [], []
                for n in range(parts):
                    retain = a_ref[n, where, :]
                    h = retain * state[n] + u_ref[n, where, :]
                    p = retain * decayed[n]
                    u_ref[n, where, :] = h
                    a_ref[n, where, :] = p
                    nstate.append(h)
                    ndecayed.append(p)
                out.append((tuple(nstate), tuple(ndecayed)))
            return tuple(out)

        zero = tuple(jnp.zeros((SEGMENTS, group), jnp.float32) for n in range(parts))
        one = tuple(jnp.ones((SEGMENTS, group), jnp.float32) for n in range(parts))
        ended = ((zero, one), (zero, one))
        for run in range(2):
            first, last = run * steps // 2, (run + 1) * steps // 2
            ended = lax.fori_loop(first, last, step, ended, unroll=8)
            if run == 0:
                tick(at + count)
                count += 1
        per_half = SEGMENTS // 2
        for n in range(parts):
            lanes = slice(n * group, (n + 1) * group)
            blank = jnp.zeros((1, group), jnp.float32)
            entry = [[None] * SEGMENTS, [None] * SEGMENTS]
            for d, order in ((0, range(SEGMENTS)), (1, range(SEGMENTS - 1, -1, -1))):
                carry = blank
                for s in order:
                    entry[d][s] = carry
                    carry = ended[d][0][n][s : s + 1] + ended[d][1][n][s : s + 1] * carry
            for s in range(SEGMENTS):
                rows = slice(s * pitch, s * pitch + steps)
                local = slice((s % per_half) * steps, (s % per_half + 1) * steps)
                which = jnp.where(column == s // per_half, 0, 1)
                forward = u0[n, rows, :] + a0[n, rows, :] * entry[0][s]
                backward = u1[n, rows, :] + a1[n, rows, :] * entry[1][s]
                gate = gel[which, b, local, lanes].astype(jnp.float32)
                hid[b, which, local, lanes] = (gate * (forward + backward)).astype(jnp.bfloat16)
        tick(at + count)
        count += 1
        assert count == SCAN_TICKS
        hid_copy(b, 0).start()

    for b in range(blocks):
        hid_copy(b, 1).start()
    out0 = scan0 + blocks * SCAN_TICKS

    ocols = 256

    def mixed(h, own_blocks, far_blocks, fresh, e0=0, count=0):
        left = [hid[b, h] for b in own_blocks]
        left = jnp.concatenate(left, axis=1) if left else None
        right = [got[b, 1 - h] for b in far_blocks]
        right = jnp.concatenate(right, axis=1) if right else None
        parts_n = model // ocols

        @pl.loop(0, parts_n)
        def _(n):
            rows = pl.ds(pl.multiple_of(n * ocols, ocols), ocols)
            lanes = rows
            summed = None if fresh else total[:, lanes]
            if left is not None:
                first = 2 * channels + own_blocks[0] * width
                term = matmul_t(left, full[0, rows, first : first + len(own_blocks) * width])
                summed = term if summed is None else summed + term
            if right is not None:
                first = far_blocks[0] * width
                term = matmul_t(right, far_out[rows, first : first + len(far_blocks) * width])
                summed = term if summed is None else summed + term
            total[:, lanes] = summed
            if count:
                every_n = parts_n // count

                @pl.when(n % every_n == every_n - 1)
                def _():
                    tick(e0 + n // every_n)

    def settle(h, source):
        @pl.loop(0, half // chunk)
        def _(i):
            rows = pl.ds(pl.multiple_of(i * chunk, chunk), chunk)
            stream = source[rows, :].astype(jnp.float32)
            residual = stream + normed(total[rows, :], gains[1])
            residual = residual.astype(jnp.bfloat16)
            if h == 0:
                source[rows, :] = residual
            middle = normed(residual.astype(jnp.float32), gains[2])
            xm[h, rows, :] = middle.astype(jnp.bfloat16)

    all_blocks = tuple(range(blocks))
    mixed(1, all_blocks, (), True, out0, 2)
    tick(out0 + 2)

    ref = far_out.at[pl.ds(0, chips * depth), :]
    remote(ref, ref, cross_send.at[0], cross_recv.at[0], across).wait_recv()

    @pl.loop(0, chips)
    def _(chip):
        ref = far_out.at[pl.ds(pl.multiple_of((chip * 2 + core) * depth, depth), depth), :]
        remote(ref, ref, share_send.at[0], share_recv.at[0], partner).start()

    ffn0 = out0 + 3
    for b in all_blocks:
        ticks(ffn0, ffn0 + 2)
        hid_copy(b, 0).wait_recv()
        if b == 0:
            ref = far_out.at[pl.ds(0, chips * depth), :]
            remote(ref, ref, share_send.at[0], share_recv.at[0], partner).wait_recv()
        mixed(1, (), (b,), False, ffn0 + 2, 1)
        ffn0 += 3
    settle(1, other)
    tick(ffn0)
    ffn0 += 1

    ucols = 256
    unit_chunks = units // 2 // ucols

    def expand(g, h, c):
        x = xm[h]
        lanes = pl.ds(pl.multiple_of(c * ucols, ucols), ucols)
        gate = jnp.dot(x, full[g, :, lanes], preferred_element_type=jnp.float32)
        lanes = pl.ds(pl.multiple_of(units // 2 + c * ucols, ucols), ucols)
        up = jnp.dot(x, full[g, :, lanes], preferred_element_type=jnp.float32)
        lanes = pl.ds(pl.multiple_of((g - 1) * (units // 2) + c * ucols, ucols), ucols)
        hf[h, :, lanes] = (jax.nn.silu(gate) * up).astype(jnp.bfloat16)

    first_done = 2 * per_stage + head
    second_done = 3 * per_stage + head
    ticks(min(ffn0, first_done), first_done)
    ffn1 = max(ffn0, first_done)

    @pl.loop(0, chips)
    def _(slot):
        near_wait(1, slot)

    @pl.loop(0, unit_chunks)
    def _(c):
        expand(1, 1, c)

        @pl.when(c == 1)
        def _():
            tick(ffn1)

    def feature_chip(slot):
        d = (slot + 1) // 2
        return chip_at(jnp.where(slot % 2 == 1, -d, d))

    def expand_part(g, h, c, slots, fresh, last):
        rows = [pl.ds(pl.multiple_of(feature_chip(slot) * span, span), span) for slot in slots]
        x = jnp.concatenate([xm[h, :, at] for at in rows], axis=1)
        summed = []
        for side in range(2):
            lanes = pl.ds(pl.multiple_of(side * cut + c * ucols, ucols), ucols)
            w = jnp.concatenate([full[g, at, lanes] for at in rows], axis=0)
            term = jnp.dot(x, w, preferred_element_type=jnp.float32)
            if not fresh:
                term = total[:, lanes] + term
            if last:
                summed.append(term)
            else:
                total[:, lanes] = term
        if last:
            lanes = pl.ds(pl.multiple_of((g - 1) * cut + c * ucols, ucols), ucols)
            hf[h, :, lanes] = (jax.nn.silu(summed[0]) * summed[1]).astype(jnp.bfloat16)

    ffn2 = ffn1 + 1
    before = second_done - PIECES // 2
    ticks(min(ffn2, before), before)
    parts_b = (tuple(range(chips - 3)), (chips - 3, chips - 2), (chips - 1,))
    for n, slots in enumerate(parts_b):
        if n == len(parts_b) - 1:
            ticks(before, second_done)
        for slot in slots:
            near_wait(2, slot)

        @pl.loop(0, unit_chunks)
        def _(c):
            expand_part(2, 1, c, slots, n == 0, n == len(parts_b) - 1)

    def partial_of(h, chip):
        weight = full[stages - 1, pl.ds(pl.multiple_of(chip * span, span), span), :]
        return matmul_t(hf[h], weight)

    def back_copy(slot):
        chip = feature_chip(slot)
        return remote(part.at[chip], back.at[chip], back_send.at[0], back_recv.at[slot], across)

    distance1 = (stages - 1) * per_stage + head

    def send_back(slot):
        near_wait(stages - 1, slot)
        chip = feature_chip(slot)
        part[chip] = partial_of(1, chip).astype(jnp.bfloat16)
        back_copy(slot).start()

    def send_pair(d):
        @pl.loop(2 * d - 1, 2 * d + 1)
        def _(slot):
            send_back(slot)

    send_back(0)
    for b in all_blocks:
        hid_copy(b, 1).wait_recv()
    mixed(0, all_blocks, (), True, distance1, PIECES)
    send_pair(1)
    mixed(0, (), all_blocks, False, distance1 + PIECES, 2)
    settle(0, mine)
    tick(distance1 + PIECES + 2)

    @pl.loop(0, unit_chunks)
    def _(c):
        expand(1, 0, c)

        @pl.when(c == 1)
        def _():
            tick(distance1 + PIECES + 3)

    send_pair(2)

    @pl.loop(0, unit_chunks)
    def _(c):
        expand(2, 0, c)
        tick(distance1 + 2 * PIECES + c)

    ticks(distance1 + 2 * PIECES + unit_chunks, distance1 + 3 * PIECES)
    send_pair(3)
    ticks(stages * per_stage + PIECES, stages * per_stage + head)
    send_back(chips - 1)

    @pl.loop(0, chips)
    def _(chip):
        lanes = pl.ds(pl.multiple_of(chip * span, span), span)
        total[:, lanes] = partial_of(0, chip).astype(jnp.bfloat16).astype(jnp.float32)

    squares[...] = jnp.zeros_like(squares)

    @pl.loop(0, chips)
    def _(slot):
        back_copy(slot).wait_recv()
        chip = feature_chip(slot)
        lanes = pl.ds(pl.multiple_of(chip * span, span), span)

        @pl.loop(0, half // chunk)
        def _(i):
            rows = pl.ds(pl.multiple_of(i * chunk, chunk), chunk)
            summed = total[rows, lanes] + back[chip, rows, :].astype(jnp.float32)
            total[rows, lanes] = summed
            square = summed * summed
            folded = square[:, :128]
            for at in range(128, span, 128):
                folded = folded + square[:, at : at + 128]
            squares[rows, :] += folded

    @pl.loop(0, half // chunk)
    def _(i):
        rows = pl.ds(pl.multiple_of(i * chunk, chunk), chunk)
        mean = jnp.sum(squares[rows, :], axis=-1, keepdims=True) * (1.0 / model)
        scaled = total[rows, :] * lax.rsqrt(mean + EPS) * gains[3]
        middle = mine[rows, :].astype(jnp.float32)
        mine[rows, :] = (middle + scaled).astype(jnp.bfloat16)
        pltpu.make_async_copy(mine.at[rows, :], out_ref.at[rows, :], out_sem.at[0]).start()

    for g in range(stages):
        rows = full.at[g, pl.ds(0, (reach - 1) * depth + depth // 2), :]
        for way in range(2):
            remote(
                rows, rows, ring_send.at[way, g], ring_recv.at[g, 0, 0], targets[way]
            ).wait_send()
        rows = full.at[g, pl.ds(0, chips * depth), :]
        remote(rows, rows, near_send.at[g], near_recv.at[g, 0], partner).wait_send()
    remote(mine, other, tok_send.at[0], tok_recv.at[0], across).wait_send()
    ref = far_out.at[pl.ds(0, chips * depth), :]
    remote(ref, ref, cross_send.at[0], cross_recv.at[0], across).wait_send()
    remote(ref, ref, share_send.at[0], share_recv.at[0], partner).wait_send()
    remote(hid, got, hid_send.at[0], hid_recv.at[0, 0], across).wait_send()
    remote(part, back, back_send.at[0], back_recv.at[0], across).wait_send()
    pltpu.make_async_copy(mine, out_ref, out_sem.at[0]).wait()


def paired_device(
    tokens,
    pre_mix_gain,
    post_mix_gain,
    pre_ffn_gain,
    post_ffn_gain,
    w_branch,
    w_gelu,
    conv_weight,
    w_rec,
    w_inp,
    decay,
    out_weight_t,
    w_gate,
    w_up,
    down_weight_t,
):
    half, model = tokens.shape
    depth, channels = w_branch.shape
    units = w_gate.shape[1]
    size = lax.axis_size("fs")
    chips = size // 2
    group = w_rec.shape[2]
    width = min(256, channels)
    blocks = channels // width
    length = 2 * half
    bf16 = functools.partial(pltpu.VMEM, dtype=jnp.bfloat16)
    f32 = functools.partial(pltpu.VMEM, dtype=jnp.float32)
    dma = pltpu.SemaphoreType.DMA
    stages = 4
    groups = channels // group
    reach = chips // 2
    hbm = pl.BlockSpec(memory_space=pl.ANY)
    gains = (pre_mix_gain, post_mix_gain, pre_ffn_gain, post_ffn_gain)
    return pl.pallas_call(
        functools.partial(layer_kernel, size),
        out_shape=jax.ShapeDtypeStruct((half, model), jnp.bfloat16),
        in_specs=[hbm] * 15,
        out_specs=hbm,
        scratch_shapes=[
            bf16((half, model)),
            f32((4, 1, model)),
            bf16(conv_weight.shape),
            bf16((groups, group, 4 * group)),
            f32(decay.shape),
            bf16((stages, model, 3 * channels)),
            bf16((model, channels)),
            bf16((half, model)),
            bf16((2, half, model)),
            f32((blocks, length + 16, width)),
            bf16((2, blocks, half, width)),
        ]
        + [f32((width // group, length + SEGMENTS * PITCH_PAD, group)) for i in range(4)]
        + [
            bf16((blocks, 2, half, width)),
            bf16((blocks, 2, half, width)),
            f32((half, model)),
            f32((half, 128)),
            bf16((2, half, units)),
            bf16((chips, half, 2 * depth)),
            bf16((chips, half, 2 * depth)),
            dma((2, stages)),
            dma((stages, reach, PIECES)),
            dma((stages,)),
            dma((stages, chips)),
            dma((8,)),
            dma((10,)),
            dma((1,)),
            dma((1,)),
            dma((1,)),
            dma((TOKEN_PIECES,)),
            dma((1,)),
            dma((1,)),
            dma((1,)),
            dma((1,)),
            dma((1,)),
            dma((blocks, 2)),
            dma((1,)),
            dma((chips,)),
        ],
        compiler_params=pltpu.CompilerParams(
            collective_id=0, has_side_effects=True, vmem_limit_bytes=MOST_VMEM
        ),
        cost_estimate=pl.CostEstimate(
            flops=1 << 34, bytes_accessed=1 << 26, transcendentals=1 << 24
        ),
    )(
        tokens,
        w_branch,
        w_gelu,
        out_weight_t,
        w_gate,
        w_up,
        down_weight_t,
        *(gain.reshape(1, model) for gain in gains),
        conv_weight,
        w_rec,
        w_inp,
        decay,
    )


def wide_device(
    tokens,
    pre_mix_gain,
    post_mix_gain,
    pre_ffn_gain,
    post_ffn_gain,
    w_branch,
    w_gelu,
    conv_weight,
    w_rec,
    w_inp,
    decay,
    out_weight_t,
    w_gate,
    w_up,
    down_weight_t,
):
    channels = conv_weight.shape[1]
    mix_shard = jnp.concatenate([w_branch, w_gelu, out_weight_t], axis=1)
    ffn_shard = jnp.concatenate([w_gate, w_up, down_weight_t], axis=1)
    stream = tokens.astype(jnp.float32)
    normed_in = normed(stream, pre_mix_gain).astype(jnp.bfloat16)
    mix_all = lax.all_gather(mix_shard, "fs", axis=0, tiled=True)
    whole = lax.all_gather(normed_in, "tp", axis=0, tiled=True)
    ffn_all = lax.all_gather(ffn_shard, "fs", axis=0, tiled=True)
    out_own = mix_all[:, 2 * channels :]
    hidden = mixer(whole, mix_all, conv_weight, w_rec, w_inp, decay)
    own_hidden = lax.all_to_all(hidden, "tp", split_axis=0, concat_axis=1, tiled=True)
    out_whole = lax.all_gather(out_own, "tp", axis=1, tiled=True)
    mixer_sum = matmul_t(own_hidden, out_whole)
    residual = (stream + normed(mixer_sum, post_mix_gain)).astype(jnp.bfloat16)
    middle = residual.astype(jnp.float32)
    normed_mid = normed(middle, pre_ffn_gain).astype(jnp.bfloat16)
    all_mid = lax.all_gather(normed_mid, "tp", axis=0, tiled=True)
    ffn_sum = lax.psum_scatter(
        ffn(all_mid, ffn_all), "tp", scatter_dimension=0, tiled=True
    ).astype(jnp.float32)
    return (middle + normed(ffn_sum, post_ffn_gain)).astype(jnp.bfloat16)


def solution(mesh):
    return jax.shard_map(
        paired_device if mesh.shape["tp"] == 2 else wide_device,
        mesh=mesh,
        in_specs=(
            P(("fs", "tp"), None),
            P(),
            P(),
            P(),
            P(),
            P("fs", "tp"),
            P("fs", "tp"),
            P(None, "tp"),
            P(None, "tp", None, None),
            P(None, "tp", None, None),
            P(None, "tp"),
            P("fs", "tp"),
            P("fs", "tp"),
            P("fs", "tp"),
            P("fs", "tp"),
        ),
        out_specs=P(("fs", "tp"), None),
        check_vma=False,
    )
```

```python
import functools

import jax
import jax.numpy as jnp
from jax import lax
from jax.experimental import pallas as pl
from jax.experimental.pallas import tpu as pltpu
from jax.sharding import PartitionSpec as P

EPS = 1e-06
SEGMENTS = 8
PIECES = 4
TOKEN_PIECES = 4
SCAN_TICKS = 6
PITCH_PAD = 8
MOST_VMEM = 67043328
VMEM_BYTES = 60 * 1024 * 1024


def normed(values, gain):
    factor = lax.rsqrt(jnp.mean(values * values, axis=-1, keepdims=True) + EPS)
    return values * factor * gain


def one_minus_exp(y, exp_y):
    series = 1.0 + y * (1.0 / 8.0)
    for order in (7, 6, 5, 4, 3, 2):
        series = 1.0 + y * (1.0 / order) * series
    return jnp.where(y > -0.5, -y * series, 1.0 - exp_y)


def mixer_kernel(
    x_ref, wb_ref, wg_ref, conv_ref, gates_ref, coef_ref, out_ref, pad, gel, a0, u0, a1, u1
):
    length, width = out_ref.shape
    group = gates_ref.shape[1]
    rows = 256
    pad[0:8, :] = jnp.zeros((8, width), jnp.float32)
    pad[8 + length : 16 + length, :] = jnp.zeros((8, width), jnp.float32)
    sources = ((x_ref, 0),)
    for source, base in sources:
        for start in range(0, source.shape[0], rows):
            piece = source[start : start + rows, :]
            branch = jnp.dot(piece, wb_ref[...], preferred_element_type=jnp.float32)
            gelu_in = jnp.dot(piece, wg_ref[...], preferred_element_type=jnp.float32)
            at = pl.multiple_of(base + start, rows)
            pad[pl.ds(8 + at, rows), :] = branch.astype(jnp.bfloat16).astype(jnp.float32)
            gel[pl.ds(at, rows), :] = jax.nn.gelu(
                gelu_in.astype(jnp.bfloat16).astype(jnp.float32)
            )

    for part in range(width // group):
        cols = slice(part * group, (part + 1) * group)
        taps = conv_ref[:, cols].astype(jnp.float32)
        coef = coef_ref[:, cols]
        for start in range(0, length, rows):
            summed = taps[0:1] * pad[6 + start : 6 + start + rows, cols]
            for j in range(1, 4):
                summed = summed + taps[j : j + 1] * pad[6 + j + start : 6 + j + start + rows, cols]
            conv = summed.astype(jnp.bfloat16)
            wide = conv.astype(jnp.float32)
            for d, (a_ref, u_ref) in enumerate(((a0, u0), (a1, u1))):
                gate = jnp.dot(
                    conv,
                    gates_ref[part, :, 2 * d * group : 2 * (d + 1) * group],
                    preferred_element_type=jnp.float32,
                )
                rate = jax.nn.sigmoid(gate[:, :group])
                inflow = jax.nn.sigmoid(gate[:, group:])
                log_retain = rate * coef[d : d + 1]
                retain = jnp.exp(log_retain)
                left = one_minus_exp(2.0 * log_retain, retain * retain)
                a_ref[part, start : start + rows, :] = retain
                u_ref[part, start : start + rows, :] = jnp.sqrt(left) * inflow * wide

    steps = length // SEGMENTS

    def step(t, carry):
        out = []
        for (state, decayed), (a_ref, u_ref), at in (
            (carry[0], (a0, u0), t),
            (carry[1], (a1, u1), steps - 1 - t),
        ):
            where = pl.ds(at, SEGMENTS, stride=steps)
            nstate, ndecayed = [], []
            for c in range(n):
                retain = a_ref[c, where, :]
                h = retain * state[c] + u_ref[c, where, :]
                p = retain * decayed[c]
                u_ref[c, where, :] = h
                a_ref[c, where, :] = p
                nstate.append(h)
                ndecayed.append(p)
            out.append((tuple(nstate), tuple(ndecayed)))
        return tuple(out)

    n = width // group
    zero = tuple(jnp.zeros((SEGMENTS, group), jnp.float32) for c in range(n))
    one = tuple(jnp.ones((SEGMENTS, group), jnp.float32) for c in range(n))
    ended = lax.fori_loop(0, steps, step, ((zero, one), (zero, one)), unroll=8)
    for c in range(n):
        lanes = slice(c * group, (c + 1) * group)
        blank = jnp.zeros((1, group), jnp.float32)
        entry = [[None] * SEGMENTS, [None] * SEGMENTS]
        for d, order in ((0, range(SEGMENTS)), (1, range(SEGMENTS - 1, -1, -1))):
            carry = blank
            for s in order:
                entry[d][s] = carry
                carry = ended[d][0][c][s : s + 1] + ended[d][1][c][s : s + 1] * carry
        for s in range(SEGMENTS):
            span = slice(s * steps, (s + 1) * steps)
            forward = u0[c, span, :] + a0[c, span, :] * entry[0][s]
            backward = u1[c, span, :] + a1[c, span, :] * entry[1][s]
            out_ref[span, lanes] = (gel[span, lanes] * (forward + backward)).astype(jnp.bfloat16)


def mixer(x, weights, conv_weight, w_rec, w_inp, decay):
    length, model = x.shape
    channels = conv_weight.shape[1]
    group = w_rec.shape[2]
    width = min(256, channels)
    count = channels // width
    gates = jnp.concatenate([w_rec[0], w_inp[0], w_rec[1], w_inp[1]], axis=-1)
    coef = -8.0 * jax.nn.softplus(-decay)
    f32 = functools.partial(pltpu.VMEM, dtype=jnp.float32)
    return pl.pallas_call(
        mixer_kernel,
        grid=(count,),
        out_shape=jax.ShapeDtypeStruct((length, channels), jnp.bfloat16),
        in_specs=[
            pl.BlockSpec((length, model), lambda j: (0, 0)),
            pl.BlockSpec((model, width), lambda j: (0, j)),
            pl.BlockSpec((model, width), lambda j: (0, count + j)),
            pl.BlockSpec((4, width), lambda j: (0, j)),
            pl.BlockSpec((width // group, group, 4 * group), lambda j: (j, 0, 0)),
            pl.BlockSpec((2, width), lambda j: (0, j)),
        ],
        out_specs=pl.BlockSpec((length, width), lambda j: (0, j)),
        scratch_shapes=[f32((length + 16, width)), f32((length, width))]
        + [f32((width // group, length, group)) for i in range(4)],
        compiler_params=pltpu.CompilerParams(vmem_limit_bytes=VMEM_BYTES),
        cost_estimate=pl.CostEstimate(
            flops=4 * length * model * channels + 16 * length * group * channels * 8,
            bytes_accessed=2 * (length * model + 2 * model * channels + length * channels),
            transcendentals=12 * length * channels,
        ),
    )(x, weights, weights, conv_weight, gates, coef)


def ffn_kernel(x_ref, gate_ref, up_ref, down_ref, out_ref, total):
    step = pl.program_id(0)
    gate = jnp.dot(x_ref[...], gate_ref[...], preferred_element_type=jnp.float32)
    up = jnp.dot(x_ref[...], up_ref[...], preferred_element_type=jnp.float32)
    hidden = (jax.nn.silu(gate) * up).astype(jnp.bfloat16)
    partial = lax.dot_general(
        hidden, down_ref[...], (((1,), (1,)), ((), ())), preferred_element_type=jnp.float32
    )

    @pl.when(step == 0)
    def _():
        total[...] = partial

    @pl.when(step > 0)
    def _():
        total[...] += partial

    @pl.when(step == pl.num_programs(0) - 1)
    def _():
        out_ref[...] = total[...].astype(jnp.bfloat16)


def ffn(x, weights):
    rows, model = x.shape
    units = weights.shape[1] // 3
    width = 256 if units % 256 == 0 else 128
    count = units // width
    return pl.pallas_call(
        ffn_kernel,
        grid=(count,),
        out_shape=jax.ShapeDtypeStruct((rows, model), jnp.bfloat16),
        in_specs=[
            pl.BlockSpec((rows, model), lambda j: (0, 0)),
            pl.BlockSpec((model, width), lambda j: (0, j)),
            pl.BlockSpec((model, width), lambda j: (0, count + j)),
            pl.BlockSpec((model, width), lambda j: (0, 2 * count + j)),
        ],
        out_specs=pl.BlockSpec((rows, model), lambda j: (0, 0)),
        scratch_shapes=[pltpu.VMEM((rows, model), jnp.float32)],
        compiler_params=pltpu.CompilerParams(vmem_limit_bytes=VMEM_BYTES),
        cost_estimate=pl.CostEstimate(
            flops=6 * rows * model * units,
            bytes_accessed=2 * (2 * rows * model + 3 * model * units),
            transcendentals=rows * units,
        ),
    )(x, weights, weights, weights)


def matmul_t(rows, weight_t):
    return lax.dot_general(
        rows, weight_t, (((1,), (1,)), ((), ())), preferred_element_type=jnp.float32
    )


def ring_chip(place, chips):
    half = chips // 2
    turned = place // half
    row = place * (1 - turned) + (chips - 1 - place) * turned
    return row * 2 + turned


def remote(src, dst, sent, landed, device):
    return pltpu.make_async_remote_copy(
        src_ref=src,
        dst_ref=dst,
        send_sem=sent,
        recv_sem=landed,
        device_id=device,
        device_id_type=pl.DeviceIdType.MESH,
    )


def branch_on(condition, body):
    if isinstance(condition, bool):
        if condition:
            body()
    else:
        pl.when(condition)(body)


def both(first, second):
    if isinstance(first, bool) and isinstance(second, bool):
        return first and second
    return jnp.logical_and(first, second)


def either(first, second):
    if isinstance(first, bool) and isinstance(second, bool):
        return first or second
    return jnp.logical_or(first, second)


def layer_kernel(
    size,
    tokens_ref,
    branch_ref,
    gelu_ref,
    outw_ref,
    gate_ref,
    up_ref,
    down_ref,
    gain0_ref,
    gain1_ref,
    gain2_ref,
    gain3_ref,
    taps_ref,
    rec_ref,
    inp_ref,
    decay_ref,
    out_ref,
    mine,
    gains,
    conv_ref,
    gates_ref,
    coef_ref,
    full,
    far_out,
    other,
    xm,
    pad,
    gel,
    a0,
    u0,
    a1,
    u1,
    hid,
    got,
    total,
    squares,
    hf,
    part,
    back,
    ring_send,
    ring_recv,
    near_send,
    near_recv,
    own_sem,
    small_sem,
    mine_sem,
    out_sem,
    tok_send,
    tok_recv,
    cross_send,
    cross_recv,
    share_send,
    share_recv,
    hid_send,
    hid_recv,
    back_send,
    back_recv,
):
    chips = size // 2
    reach = chips // 2
    stages = full.shape[0]
    depth, channels = branch_ref.shape
    prow = depth // PIECES
    half, model = tokens_ref.shape
    blocks, width = pad.shape[0], pad.shape[2]
    group = gates_ref.shape[1]
    units = hf.shape[2]
    span = 2 * depth

    me = lax.axis_index("fs")
    core = me % 2
    turned = (me // 2) % 2
    row = me // 4
    place = row * (1 - turned) + (chips - 1 - row) * turned
    column = lax.axis_index("tp")

    def chip_at(offset):
        return ring_chip((place + chips + offset) % chips, chips)

    targets = ({"fs": chip_at(1) * 2 + core}, {"fs": chip_at(-1) * 2 + core})
    partner = {"fs": me + 1 - 2 * core}
    across = {"tp": 1 - column}

    cut = units // 2
    own_rows = pl.ds(pl.multiple_of(me * depth, depth), depth)

    def own_part(g, source, lanes, at, sem):
        place_at = full.at[g, own_rows, pl.ds(at, lanes.size)]
        return pltpu.make_async_copy(source.at[:, lanes], place_at, own_sem.at[sem])

    every = pl.ds(0, channels)
    ucols = 256
    unit_chunks = cut // ucols
    unit_pairs = 2 * unit_chunks

    def unit_parts(first, sem):
        found = []
        for c in range(unit_chunks):
            for side, source in enumerate((gate_ref, up_ref)):
                at = (2 * c + side) * ucols
                found.append((source, pl.ds(first + c * ucols, ucols), at, sem + len(found)))
        return found

    own_copies = [
        [own_part(0, source, every, i * channels, i) for i, source in enumerate((branch_ref, gelu_ref, outw_ref))],
        [own_part(1, *pair) for pair in unit_parts(0, 3)],
        [own_part(2, *pair) for pair in unit_parts(cut, 3 + unit_pairs)],
        [own_part(3, down_ref, pl.ds(0, units), 0, 3 + 2 * unit_pairs)],
    ]
    for copy in own_copies[0]:
        copy.start()
    chunk = 128
    mine_copy = pltpu.make_async_copy(tokens_ref, mine, mine_sem.at[0])
    mine_copy.start()
    small = [(source, gains.at[i]) for i, source in enumerate((gain0_ref, gain1_ref, gain2_ref, gain3_ref))]
    small += [(taps_ref, conv_ref), (decay_ref, coef_ref)]
    for d in range(2):
        for i, source in enumerate((rec_ref, inp_ref)):
            lanes = pl.ds((2 * d + i) * group, group)
            small.append((source.at[d], gates_ref.at[:, :, lanes]))
    small = [
        pltpu.make_async_copy(source, place_at, small_sem.at[i])
        for i, (source, place_at) in enumerate(small)
    ]
    for copy in small:
        copy.start()
    for copies in own_copies[1:]:
        for copy in copies:
            copy.start()

    barrier = pltpu.get_barrier_semaphore()
    for device in (*targets, partner, across):
        pl.semaphore_signal(barrier, inc=1, device_id=device, device_id_type=pl.DeviceIdType.MESH)
    pl.semaphore_wait(barrier, 4)

    def piece(g, chip, p):
        start = pl.multiple_of((chip * 2 + core) * depth + p * prow, prow)
        return full.at[g, pl.ds(start, prow), :]

    def shard_rows(g, chip, which):
        start = pl.multiple_of((chip * 2 + which) * depth, depth)
        return full.at[g, pl.ds(start, depth), :]

    def start_piece(g, p):
        src = piece(g, me // 2, p)
        dst = src
        for way in range(2):
            remote(src, dst, ring_send.at[way, g], ring_recv.at[g, 0, p], targets[way]).start()
        remote(src, dst, near_send.at[g], near_recv.at[g, 0], partner).start()

    def landed(g, s, p):
        rows = full.at[g, pl.ds(0, 2 * prow), :]
        remote(rows, rows, ring_send.at[0, g], ring_recv.at[g, s, p], targets[0]).wait_recv()

    def pass_piece(g, s, p):
        landed(g, s - 1, p)
        for way in range(2):
            ref = piece(g, chip_at(-s if way == 0 else s), p)
            slot = 2 * s - 1 + way

            def forward():
                index = jnp.where(s < reach - 1, p, p // 2)
                remote(
                    ref, ref, ring_send.at[way, g], ring_recv.at[g, s, index], targets[way]
                ).start()

            mine = p % 2 == way
            branch_on(either(s < reach - 1, mine), forward)
            remote(ref, ref, near_send.at[g], near_recv.at[g, slot], partner).start()

    def last_piece(g, q):
        landed(g, reach - 1, q)
        for way in range(2):
            ref = piece(g, chip_at(reach), 2 * q + way)
            remote(ref, ref, near_send.at[g], near_recv.at[g, chips - 1], partner).start()

    head = PIECES + PIECES // 2
    per_stage = head + (reach - 1) * PIECES

    def tick(e):
        g = e // per_stage
        k = e % per_stage
        branch_on(both(k < PIECES, g < stages), lambda: start_piece(g, k))
        branch_on(
            both(both(k >= PIECES, k < head), g > 0), lambda: last_piece(g - 1, k - PIECES)
        )
        branch_on(
            both(k >= head, g < stages),
            lambda: pass_piece(g, (k - head) // PIECES + 1, (k - head) % PIECES),
        )

    def ticks(first, last):
        @pl.loop(first, last)
        def _(e):
            tick(e)

    def near_wait(g, slot):
        ref = shard_rows(g, 0, 0)
        remote(ref, ref, near_send.at[g], near_recv.at[g, slot], partner).wait_recv()

    token_rows = half // TOKEN_PIECES
    for i in range(TOKEN_PIECES):
        rows = pl.ds(i * token_rows, token_rows)
        remote(tokens_ref.at[rows, :], other.at[rows, :], tok_send.at[0], tok_recv.at[i], across).start()
    for copy in own_copies[0]:
        copy.wait()
    ticks(0, PIECES)
    for copy in (*small, mine_copy):
        copy.wait()
    for copies in own_copies[1:]:
        for copy in copies:
            copy.wait()
    slow = coef_ref[...]
    coef_ref[...] = -8.0 * (jnp.maximum(-slow, 0.0) + jnp.log1p(jnp.exp(-jnp.abs(slow))))

    def norm_rows(source, h, at):
        rows = pl.ds(at, chunk)
        values = source[rows, :].astype(jnp.float32)
        xm[h, rows, :] = normed(values, gains[0]).astype(jnp.bfloat16)

    @pl.loop(0, half // chunk)
    def _(i):
        norm_rows(mine, 0, pl.multiple_of(i * chunk, chunk))

    length = 2 * half
    for b in range(blocks):
        pad[b, 0:8, :] = jnp.zeros((8, width), jnp.float32)
        pad[b, 8 + length : 16 + length, :] = jnp.zeros((8, width), jnp.float32)

    done0 = per_stage + head
    ticks(PIECES, done0)

    @pl.loop(0, chips)
    def _(slot):
        near_wait(0, slot)

    @pl.loop(0, chips)
    def _(chip):
        src = shard_rows(0, chip, core).at[:, pl.ds(2 * channels, channels)]
        dst = far_out.at[pl.ds(pl.multiple_of((chip * 2 + core) * depth, depth), depth), :]
        remote(src, dst, cross_send.at[0], cross_recv.at[0], across).start()

    prows = 256
    scan0 = done0 + 2 * (2 * (half // prows) - 1) + 1

    @pl.loop(0, 2)
    def _(h):
        @pl.loop(0, half // prows)
        def _(i):
            at = pl.multiple_of(i * prows, prows)

            @pl.when(h == 1)
            def _():
                @pl.loop(0, prows // token_rows)
                def _(q):
                    n = i * (prows // token_rows) + q
                    rows = pl.ds(pl.multiple_of(n * token_rows, token_rows), token_rows)
                    remote(
                        tokens_ref.at[rows, :],
                        other.at[rows, :],
                        tok_send.at[0],
                        tok_recv.at[n],
                        across,
                    ).wait_recv()

                @pl.loop(0, prows // chunk)
                def _(q):
                    norm_rows(other, 1, pl.multiple_of(at + q * chunk, chunk))

                @pl.when(i == half // prows - 1)
                def _():
                    tick(scan0 - 1)

            x = xm[h, pl.ds(at, prows), :]
            side = jnp.where(h == 0, column, 1 - column)
            base = pl.multiple_of(8 + side * half + at, 8)
            for b in range(blocks):
                lanes = slice(b * width, (b + 1) * width)
                branch = jnp.dot(x, full[0, :, lanes], preferred_element_type=jnp.float32)
                pad[b, pl.ds(base, prows), :] = branch.astype(jnp.bfloat16).astype(jnp.float32)
                lanes = slice(channels + b * width, channels + (b + 1) * width)
                gelu_in = jnp.dot(x, full[0, :, lanes], preferred_element_type=jnp.float32)
                gelu_in = gelu_in.astype(jnp.bfloat16).astype(jnp.float32)
                gel[h, b, pl.ds(at, prows), :] = jax.nn.gelu(gelu_in).astype(jnp.bfloat16)

            @pl.when(h * (half // prows) + i < 2 * (half // prows) - 1)
            def _():
                ticks(done0 + h * 4 + i * 2, done0 + h * 4 + i * 2 + 2)

    parts = width // group
    steps = length // SEGMENTS
    pitch = steps + PITCH_PAD
    crows = 256

    quarter = half // 2

    def hid_copies(b, h):
        copies = []
        for r in range(2):
            rows = pl.ds(r * quarter, quarter)
            copies.append(
                remote(
                    hid.at[b, h, rows, :],
                    got.at[b, h, rows, :],
                    hid_send.at[0],
                    hid_recv.at[b, h, r],
                    across,
                )
            )
        return copies

    @pl.loop(0, blocks)
    def _(b):
        at = scan0 + b * SCAN_TICKS
        count = 0
        for n in range(parts):
            lanes = slice(n * group, (n + 1) * group)
            table = pl.ds(pl.multiple_of(b * width + n * group, group), group)
            taps = conv_ref[:, table].astype(jnp.float32)
            coef = coef_ref[:, table]
            for start in range(0, length, crows):
                summed = taps[0:1] * pad[b, 6 + start : 6 + start + crows, lanes]
                for j in range(1, 4):
                    first = 6 + j + start
                    summed = summed + taps[j : j + 1] * pad[b, first : first + crows, lanes]
                conv = summed.astype(jnp.bfloat16)
                wide = conv.astype(jnp.float32)
                for d, (a_ref, u_ref) in enumerate(((a0, u0), (a1, u1))):
                    gate = jnp.dot(
                        conv,
                        gates_ref[b * parts + n, :, 2 * d * group : 2 * (d + 1) * group],
                        preferred_element_type=jnp.float32,
                    )
                    rate = jax.nn.sigmoid(gate[:, :group])
                    inflow = jax.nn.sigmoid(gate[:, group:])
                    log_retain = rate * coef[d : d + 1]
                    retain = jnp.exp(log_retain)
                    left = one_minus_exp(2.0 * log_retain, retain * retain)
                    feed = jnp.sqrt(left) * inflow * wide
                    for q in range(crows // steps):
                        first = (start // steps + q) * pitch
                        a_ref[n, first : first + steps, :] = retain[q * steps : (q + 1) * steps]
                        u_ref[n, first : first + steps, :] = feed[q * steps : (q + 1) * steps]
                if (start // crows) % 2 == 1:
                    tick(at + count)
                    count += 1

        def step(t, carry):
            out = []
            for (state, decayed), (a_ref, u_ref), when in (
                (carry[0], (a0, u0), t),
                (carry[1], (a1, u1), steps - 1 - t),
            ):
                where = pl.ds(when, SEGMENTS, stride=pitch)
                nstate, ndecayed = [], []
                for n in range(parts):
                    retain = a_ref[n, where, :]
                    h = retain * state[n] + u_ref[n, where, :]
                    p = retain * decayed[n]
                    u_ref[n, where, :] = h
                    a_ref[n, where, :] = p
                    nstate.append(h)
                    ndecayed.append(p)
                out.append((tuple(nstate), tuple(ndecayed)))
            return tuple(out)

        zero = tuple(jnp.zeros((SEGMENTS, group), jnp.float32) for n in range(parts))
        one = tuple(jnp.ones((SEGMENTS, group), jnp.float32) for n in range(parts))
        ended = ((zero, one), (zero, one))
        for run in range(2):
            first, last = run * steps // 2, (run + 1) * steps // 2
            ended = lax.fori_loop(first, last, step, ended, unroll=8)
            if run == 0:
                tick(at + count)
                count += 1
        per_half = SEGMENTS // 2
        for n in range(parts):
            lanes = slice(n * group, (n + 1) * group)
            blank = jnp.zeros((1, group), jnp.float32)
            entry = [[None] * SEGMENTS, [None] * SEGMENTS]
            for d, order in ((0, range(SEGMENTS)), (1, range(SEGMENTS - 1, -1, -1))):
                carry = blank
                for s in order:
                    entry[d][s] = carry
                    carry = ended[d][0][n][s : s + 1] + ended[d][1][n][s : s + 1] * carry
            for s in range(SEGMENTS):
                rows = slice(s * pitch, s * pitch + steps)
                local = slice((s % per_half) * steps, (s % per_half + 1) * steps)
                which = jnp.where(column == s // per_half, 0, 1)
                forward = u0[n, rows, :] + a0[n, rows, :] * entry[0][s]
                backward = u1[n, rows, :] + a1[n, rows, :] * entry[1][s]
                gate = gel[which, b, local, lanes].astype(jnp.float32)
                hid[b, which, local, lanes] = (gate * (forward + backward)).astype(jnp.bfloat16)
        tick(at + count)
        count += 1
        assert count == SCAN_TICKS
        for copy in hid_copies(b, 0):
            copy.start()

    for b in range(blocks):
        for copy in hid_copies(b, 1):
            copy.start()
    out0 = scan0 + blocks * SCAN_TICKS


    whole = slice(0, half)

    def mixed(h, own_blocks, far_blocks, fresh, e0=0, count=0, tall=whole, ocols=512):
        left = [hid[b, h, tall] for b in own_blocks]
        left = jnp.concatenate(left, axis=1) if left else None
        right = [got[b, 1 - h, tall] for b in far_blocks]
        right = jnp.concatenate(right, axis=1) if right else None
        parts_n = model // ocols

        @pl.loop(0, parts_n)
        def _(n):
            rows = pl.ds(pl.multiple_of(n * ocols, ocols), ocols)
            lanes = rows
            summed = None if fresh else total[tall, lanes]
            if left is not None:
                first = 2 * channels + own_blocks[0] * width
                term = matmul_t(left, full[0, rows, first : first + len(own_blocks) * width])
                summed = term if summed is None else summed + term
            if right is not None:
                first = far_blocks[0] * width
                term = matmul_t(right, far_out[rows, first : first + len(far_blocks) * width])
                summed = term if summed is None else summed + term
            total[tall, lanes] = summed
            if count:
                every_n = parts_n // count

                @pl.when(n % every_n == every_n - 1)
                def _():
                    tick(e0 + n // every_n)

    def settle(h, source, tall=whole):
        @pl.loop(tall.start // chunk, tall.stop // chunk)
        def _(i):
            rows = pl.ds(pl.multiple_of(i * chunk, chunk), chunk)
            stream = source[rows, :].astype(jnp.float32)
            residual = stream + normed(total[rows, :], gains[1])
            residual = residual.astype(jnp.bfloat16)
            if h == 0:
                source[rows, :] = residual
            middle = normed(residual.astype(jnp.float32), gains[2])
            xm[h, rows, :] = middle.astype(jnp.bfloat16)

    all_blocks = tuple(range(blocks))
    mixed(1, all_blocks, (), True, out0, 2)
    tick(out0 + 2)

    ref = far_out.at[pl.ds(0, chips * depth), :]
    remote(ref, ref, cross_send.at[0], cross_recv.at[0], across).wait_recv()

    @pl.loop(0, chips)
    def _(chip):
        ref = far_out.at[pl.ds(pl.multiple_of((chip * 2 + core) * depth, depth), depth), :]
        remote(ref, ref, share_send.at[0], share_recv.at[0], partner).start()

    ffn0 = out0 + 3
    for b in all_blocks[:-1]:
        ticks(ffn0, ffn0 + 2)
        for copy in hid_copies(b, 0):
            copy.wait_recv()
        if b == 0:
            ref = far_out.at[pl.ds(0, chips * depth), :]
            remote(ref, ref, share_send.at[0], share_recv.at[0], partner).wait_recv()
        mixed(1, (), (b,), False, ffn0 + 2, 1)
        ffn0 += 3
    for r, copy in enumerate(hid_copies(blocks - 1, 0)):
        tall = slice(r * quarter, (r + 1) * quarter)
        copy.wait_recv()
        if r == 1:
            tick(ffn0)
            ffn0 += 1
        mixed(1, (), (blocks - 1,), False, tall=tall, ocols=model // 2)
        if r == 0:
            tick(ffn0)
            ffn0 += 1
        settle(1, other, tall)

    def activate(g, h, c, product):
        lanes = pl.ds(pl.multiple_of((g - 1) * cut + c * ucols, ucols), ucols)
        hidden = jax.nn.silu(product[:, :ucols]) * product[:, ucols:]
        hf[h, :, lanes] = hidden.astype(jnp.bfloat16)

    def expand(g, h, c):
        lanes = pl.ds(pl.multiple_of(2 * c * ucols, 2 * ucols), 2 * ucols)
        activate(g, h, c, jnp.dot(xm[h], full[g, :, lanes], preferred_element_type=jnp.float32))

    first_done = 2 * per_stage + head
    second_done = 3 * per_stage + head
    ticks(min(ffn0, first_done), first_done)
    ffn1 = max(ffn0, first_done)

    @pl.loop(0, chips)
    def _(slot):
        near_wait(1, slot)

    def feature_chip(slot):
        d = (slot + 1) // 2
        return chip_at(jnp.where(slot % 2 == 1, -d, d))

    def expand_part(g, h, c, slots, fresh, last):
        rows = [pl.ds(pl.multiple_of(feature_chip(slot) * span, span), span) for slot in slots]
        x = jnp.concatenate([xm[h, :, at] for at in rows], axis=1)
        lanes = pl.ds(pl.multiple_of(2 * c * ucols, 2 * ucols), 2 * ucols)
        w = jnp.concatenate([full[g, at, lanes] for at in rows], axis=0)
        term = jnp.dot(x, w, preferred_element_type=jnp.float32)
        if not fresh:
            term = total[:, lanes] + term
        if last:
            activate(g, h, c, term)
        else:
            total[:, lanes] = term

    ffn2 = ffn1 + 2
    before = second_done - PIECES // 2
    parts_b = (tuple(range(chips - 3)), (chips - 3, chips - 2), (chips - 1,))

    @pl.loop(0, unit_chunks)
    def _(c):
        expand(1, 1, c)

        @pl.when(c < 2)
        def _():
            tick(ffn1 + c)

    for slot in parts_b[0]:
        near_wait(2, slot)

    @pl.loop(0, unit_chunks)
    def _(c):
        expand_part(2, 1, c, parts_b[0], True, False)

        @pl.when(c == 0)
        def _():
            tick(ffn2)

        @pl.when(c == 1)
        def _():
            ticks(ffn2 + 1, before)

        @pl.when(c == 2)
        def _():
            tick(before)

    for n in (1, 2):
        if n == 2:
            tick(before + 1)
        for slot in parts_b[n]:
            near_wait(2, slot)
        for c in range(unit_chunks):
            expand_part(2, 1, c, parts_b[n], False, n == 2)

    def partial_of(h, chip):
        weight = full[stages - 1, pl.ds(pl.multiple_of(chip * span, span), span), :]
        return matmul_t(hf[h], weight)

    def back_copy(slot):
        chip = feature_chip(slot)
        return remote(part.at[chip], back.at[chip], back_send.at[0], back_recv.at[slot], across)

    distance1 = (stages - 1) * per_stage + head

    def send_back(slot):
        near_wait(stages - 1, slot)
        chip = feature_chip(slot)
        part[chip] = partial_of(1, chip).astype(jnp.bfloat16)
        back_copy(slot).start()

    def send_pair(d):
        @pl.loop(2 * d - 1, 2 * d + 1)
        def _(slot):
            send_back(slot)

    send_back(0)
    for b in all_blocks:
        for copy in hid_copies(b, 1):
            copy.wait_recv()
    mixed(0, all_blocks, (), True, distance1, PIECES)
    send_pair(1)
    mixed(0, (), all_blocks, False, distance1 + PIECES, 2)
    settle(0, mine)
    tick(distance1 + PIECES + 2)

    @pl.loop(0, unit_chunks)
    def _(c):
        expand(1, 0, c)

        @pl.when(c == 1)
        def _():
            tick(distance1 + PIECES + 3)

    send_pair(2)

    @pl.loop(0, unit_chunks)
    def _(c):
        expand(2, 0, c)
        tick(distance1 + 2 * PIECES + c)

    ticks(distance1 + 2 * PIECES + unit_chunks, distance1 + 3 * PIECES)
    send_pair(3)
    ticks(stages * per_stage + PIECES, stages * per_stage + head)
    send_back(chips - 1)

    @pl.loop(0, chips)
    def _(chip):
        lanes = pl.ds(pl.multiple_of(chip * span, span), span)
        total[:, lanes] = partial_of(0, chip).astype(jnp.bfloat16).astype(jnp.float32)

    squares[...] = jnp.zeros_like(squares)

    @pl.loop(0, chips)
    def _(slot):
        back_copy(slot).wait_recv()
        chip = feature_chip(slot)
        lanes = pl.ds(pl.multiple_of(chip * span, span), span)

        @pl.loop(0, half // chunk)
        def _(i):
            rows = pl.ds(pl.multiple_of(i * chunk, chunk), chunk)
            summed = total[rows, lanes] + back[chip, rows, :].astype(jnp.float32)
            total[rows, lanes] = summed
            square = summed * summed
            folded = square[:, :128]
            for at in range(128, span, 128):
                folded = folded + square[:, at : at + 128]
            squares[rows, :] += folded

    @pl.loop(0, half // chunk)
    def _(i):
        rows = pl.ds(pl.multiple_of(i * chunk, chunk), chunk)
        mean = jnp.sum(squares[rows, :], axis=-1, keepdims=True) * (1.0 / model)
        scaled = total[rows, :] * lax.rsqrt(mean + EPS) * gains[3]
        middle = mine[rows, :].astype(jnp.float32)
        mine[rows, :] = (middle + scaled).astype(jnp.bfloat16)
        pltpu.make_async_copy(mine.at[rows, :], out_ref.at[rows, :], out_sem.at[0]).start()

    for g in range(stages):
        rows = full.at[g, pl.ds(0, (reach - 1) * depth + depth // 2), :]
        for way in range(2):
            remote(
                rows, rows, ring_send.at[way, g], ring_recv.at[g, 0, 0], targets[way]
            ).wait_send()
        rows = full.at[g, pl.ds(0, chips * depth), :]
        remote(rows, rows, near_send.at[g], near_recv.at[g, 0], partner).wait_send()
    remote(mine, other, tok_send.at[0], tok_recv.at[0], across).wait_send()
    ref = far_out.at[pl.ds(0, chips * depth), :]
    remote(ref, ref, cross_send.at[0], cross_recv.at[0], across).wait_send()
    remote(ref, ref, share_send.at[0], share_recv.at[0], partner).wait_send()
    remote(hid, got, hid_send.at[0], hid_recv.at[0, 0, 0], across).wait_send()
    remote(part, back, back_send.at[0], back_recv.at[0], across).wait_send()
    pltpu.make_async_copy(mine, out_ref, out_sem.at[0]).wait()


def paired_device(
    tokens,
    pre_mix_gain,
    post_mix_gain,
    pre_ffn_gain,
    post_ffn_gain,
    w_branch,
    w_gelu,
    conv_weight,
    w_rec,
    w_inp,
    decay,
    out_weight_t,
    w_gate,
    w_up,
    down_weight_t,
):
    half, model = tokens.shape
    depth, channels = w_branch.shape
    units = w_gate.shape[1]
    size = lax.axis_size("fs")
    chips = size // 2
    group = w_rec.shape[2]
    width = min(256, channels)
    blocks = channels // width
    length = 2 * half
    bf16 = functools.partial(pltpu.VMEM, dtype=jnp.bfloat16)
    f32 = functools.partial(pltpu.VMEM, dtype=jnp.float32)
    dma = pltpu.SemaphoreType.DMA
    stages = 4
    groups = channels // group
    reach = chips // 2
    hbm = pl.BlockSpec(memory_space=pl.ANY)
    gains = (pre_mix_gain, post_mix_gain, pre_ffn_gain, post_ffn_gain)
    return pl.pallas_call(
        functools.partial(layer_kernel, size),
        out_shape=jax.ShapeDtypeStruct((half, model), jnp.bfloat16),
        in_specs=[hbm] * 15,
        out_specs=hbm,
        scratch_shapes=[
            bf16((half, model)),
            f32((4, 1, model)),
            bf16(conv_weight.shape),
            bf16((groups, group, 4 * group)),
            f32(decay.shape),
            bf16((stages, model, 3 * channels)),
            bf16((model, channels)),
            bf16((half, model)),
            bf16((2, half, model)),
            f32((blocks, length + 16, width)),
            bf16((2, blocks, half, width)),
        ]
        + [f32((width // group, length + SEGMENTS * PITCH_PAD, group)) for i in range(4)]
        + [
            bf16((blocks, 2, half, width)),
            bf16((blocks, 2, half, width)),
            f32((half, model)),
            f32((half, 128)),
            bf16((2, half, units)),
            bf16((chips, half, 2 * depth)),
            bf16((chips, half, 2 * depth)),
            dma((2, stages)),
            dma((stages, reach, PIECES)),
            dma((stages,)),
            dma((stages, chips)),
            dma((4 + 4 * (units // 2 // 256),)),
            dma((10,)),
            dma((1,)),
            dma((1,)),
            dma((1,)),
            dma((TOKEN_PIECES,)),
            dma((1,)),
            dma((1,)),
            dma((1,)),
            dma((1,)),
            dma((1,)),
            dma((blocks, 2, 2)),
            dma((1,)),
            dma((chips,)),
        ],
        compiler_params=pltpu.CompilerParams(
            collective_id=0, has_side_effects=True, vmem_limit_bytes=MOST_VMEM
        ),
        cost_estimate=pl.CostEstimate(
            flops=1 << 34, bytes_accessed=1 << 26, transcendentals=1 << 24
        ),
    )(
        tokens,
        w_branch,
        w_gelu,
        out_weight_t,
        w_gate,
        w_up,
        down_weight_t,
        *(gain.reshape(1, model) for gain in gains),
        conv_weight,
        w_rec,
        w_inp,
        decay,
    )


def wide_device(
    tokens,
    pre_mix_gain,
    post_mix_gain,
    pre_ffn_gain,
    post_ffn_gain,
    w_branch,
    w_gelu,
    conv_weight,
    w_rec,
    w_inp,
    decay,
    out_weight_t,
    w_gate,
    w_up,
    down_weight_t,
):
    channels = conv_weight.shape[1]
    mix_shard = jnp.concatenate([w_branch, w_gelu, out_weight_t], axis=1)
    ffn_shard = jnp.concatenate([w_gate, w_up, down_weight_t], axis=1)
    stream = tokens.astype(jnp.float32)
    normed_in = normed(stream, pre_mix_gain).astype(jnp.bfloat16)
    mix_all = lax.all_gather(mix_shard, "fs", axis=0, tiled=True)
    whole = lax.all_gather(normed_in, "tp", axis=0, tiled=True)
    ffn_all = lax.all_gather(ffn_shard, "fs", axis=0, tiled=True)
    out_own = mix_all[:, 2 * channels :]
    hidden = mixer(whole, mix_all, conv_weight, w_rec, w_inp, decay)
    own_hidden = lax.all_to_all(hidden, "tp", split_axis=0, concat_axis=1, tiled=True)
    out_whole = lax.all_gather(out_own, "tp", axis=1, tiled=True)
    mixer_sum = matmul_t(own_hidden, out_whole)
    residual = (stream + normed(mixer_sum, post_mix_gain)).astype(jnp.bfloat16)
    middle = residual.astype(jnp.float32)
    normed_mid = normed(middle, pre_ffn_gain).astype(jnp.bfloat16)
    all_mid = lax.all_gather(normed_mid, "tp", axis=0, tiled=True)
    ffn_sum = lax.psum_scatter(
        ffn(all_mid, ffn_all), "tp", scatter_dimension=0, tiled=True
    ).astype(jnp.float32)
    return (middle + normed(ffn_sum, post_ffn_gain)).astype(jnp.bfloat16)


def solution(mesh):
    return jax.shard_map(
        paired_device if mesh.shape["tp"] == 2 else wide_device,
        mesh=mesh,
        in_specs=(
            P(("fs", "tp"), None),
            P(),
            P(),
            P(),
            P(),
            P("fs", "tp"),
            P("fs", "tp"),
            P(None, "tp"),
            P(None, "tp", None, None),
            P(None, "tp", None, None),
            P(None, "tp"),
            P("fs", "tp"),
            P("fs", "tp"),
            P("fs", "tp"),
            P("fs", "tp"),
        ),
        out_specs=P(("fs", "tp"), None),
        check_vma=False,
    )
```

```python
import functools

import jax
import jax.numpy as jnp
from jax import lax
from jax.experimental import pallas as pl
from jax.experimental.pallas import tpu as pltpu
from jax.sharding import PartitionSpec as P

EPS = 1e-06
SEGMENTS = 8
PIECES = 4
TOKEN_PIECES = 4
SCAN_TICKS = 6
PITCH_PAD = 8
MOST_VMEM = 67043328
VMEM_BYTES = 60 * 1024 * 1024


def normed(values, gain):
    factor = lax.rsqrt(jnp.mean(values * values, axis=-1, keepdims=True) + EPS)
    return values * factor * gain


def one_minus_exp(y, exp_y):
    series = 1.0 + y * (1.0 / 8.0)
    for order in (7, 6, 5, 4, 3, 2):
        series = 1.0 + y * (1.0 / order) * series
    return jnp.where(y > -0.5, -y * series, 1.0 - exp_y)


def mixer_kernel(
    x_ref, wb_ref, wg_ref, conv_ref, gates_ref, coef_ref, out_ref, pad, gel, a0, u0, a1, u1
):
    length, width = out_ref.shape
    group = gates_ref.shape[1]
    rows = 256
    pad[0:8, :] = jnp.zeros((8, width), jnp.float32)
    pad[8 + length : 16 + length, :] = jnp.zeros((8, width), jnp.float32)
    sources = ((x_ref, 0),)
    for source, base in sources:
        for start in range(0, source.shape[0], rows):
            piece = source[start : start + rows, :]
            branch = jnp.dot(piece, wb_ref[...], preferred_element_type=jnp.float32)
            gelu_in = jnp.dot(piece, wg_ref[...], preferred_element_type=jnp.float32)
            at = pl.multiple_of(base + start, rows)
            pad[pl.ds(8 + at, rows), :] = branch.astype(jnp.bfloat16).astype(jnp.float32)
            gel[pl.ds(at, rows), :] = jax.nn.gelu(
                gelu_in.astype(jnp.bfloat16).astype(jnp.float32)
            )

    for part in range(width // group):
        cols = slice(part * group, (part + 1) * group)
        taps = conv_ref[:, cols].astype(jnp.float32)
        coef = coef_ref[:, cols]
        for start in range(0, length, rows):
            summed = taps[0:1] * pad[6 + start : 6 + start + rows, cols]
            for j in range(1, 4):
                summed = summed + taps[j : j + 1] * pad[6 + j + start : 6 + j + start + rows, cols]
            conv = summed.astype(jnp.bfloat16)
            wide = conv.astype(jnp.float32)
            for d, (a_ref, u_ref) in enumerate(((a0, u0), (a1, u1))):
                gate = jnp.dot(
                    conv,
                    gates_ref[part, :, 2 * d * group : 2 * (d + 1) * group],
                    preferred_element_type=jnp.float32,
                )
                rate = jax.nn.sigmoid(gate[:, :group])
                inflow = jax.nn.sigmoid(gate[:, group:])
                log_retain = rate * coef[d : d + 1]
                retain = jnp.exp(log_retain)
                left = one_minus_exp(2.0 * log_retain, retain * retain)
                a_ref[part, start : start + rows, :] = retain
                u_ref[part, start : start + rows, :] = jnp.sqrt(left) * inflow * wide

    steps = length // SEGMENTS

    def step(t, carry):
        out = []
        for (state, decayed), (a_ref, u_ref), at in (
            (carry[0], (a0, u0), t),
            (carry[1], (a1, u1), steps - 1 - t),
        ):
            where = pl.ds(at, SEGMENTS, stride=steps)
            nstate, ndecayed = [], []
            for c in range(n):
                retain = a_ref[c, where, :]
                h = retain * state[c] + u_ref[c, where, :]
                p = retain * decayed[c]
                u_ref[c, where, :] = h
                a_ref[c, where, :] = p
                nstate.append(h)
                ndecayed.append(p)
            out.append((tuple(nstate), tuple(ndecayed)))
        return tuple(out)

    n = width // group
    zero = tuple(jnp.zeros((SEGMENTS, group), jnp.float32) for c in range(n))
    one = tuple(jnp.ones((SEGMENTS, group), jnp.float32) for c in range(n))
    ended = lax.fori_loop(0, steps, step, ((zero, one), (zero, one)), unroll=8)
    for c in range(n):
        lanes = slice(c * group, (c + 1) * group)
        blank = jnp.zeros((1, group), jnp.float32)
        entry = [[None] * SEGMENTS, [None] * SEGMENTS]
        for d, order in ((0, range(SEGMENTS)), (1, range(SEGMENTS - 1, -1, -1))):
            carry = blank
            for s in order:
                entry[d][s] = carry
                carry = ended[d][0][c][s : s + 1] + ended[d][1][c][s : s + 1] * carry
        for s in range(SEGMENTS):
            span = slice(s * steps, (s + 1) * steps)
            forward = u0[c, span, :] + a0[c, span, :] * entry[0][s]
            backward = u1[c, span, :] + a1[c, span, :] * entry[1][s]
            out_ref[span, lanes] = (gel[span, lanes] * (forward + backward)).astype(jnp.bfloat16)


def mixer(x, weights, conv_weight, w_rec, w_inp, decay):
    length, model = x.shape
    channels = conv_weight.shape[1]
    group = w_rec.shape[2]
    width = min(256, channels)
    count = channels // width
    gates = jnp.concatenate([w_rec[0], w_inp[0], w_rec[1], w_inp[1]], axis=-1)
    coef = -8.0 * jax.nn.softplus(-decay)
    f32 = functools.partial(pltpu.VMEM, dtype=jnp.float32)
    return pl.pallas_call(
        mixer_kernel,
        grid=(count,),
        out_shape=jax.ShapeDtypeStruct((length, channels), jnp.bfloat16),
        in_specs=[
            pl.BlockSpec((length, model), lambda j: (0, 0)),
            pl.BlockSpec((model, width), lambda j: (0, j)),
            pl.BlockSpec((model, width), lambda j: (0, count + j)),
            pl.BlockSpec((4, width), lambda j: (0, j)),
            pl.BlockSpec((width // group, group, 4 * group), lambda j: (j, 0, 0)),
            pl.BlockSpec((2, width), lambda j: (0, j)),
        ],
        out_specs=pl.BlockSpec((length, width), lambda j: (0, j)),
        scratch_shapes=[f32((length + 16, width)), f32((length, width))]
        + [f32((width // group, length, group)) for i in range(4)],
        compiler_params=pltpu.CompilerParams(vmem_limit_bytes=VMEM_BYTES),
        cost_estimate=pl.CostEstimate(
            flops=4 * length * model * channels + 16 * length * group * channels * 8,
            bytes_accessed=2 * (length * model + 2 * model * channels + length * channels),
            transcendentals=12 * length * channels,
        ),
    )(x, weights, weights, conv_weight, gates, coef)


def ffn_kernel(x_ref, gate_ref, up_ref, down_ref, out_ref, total):
    step = pl.program_id(0)
    gate = jnp.dot(x_ref[...], gate_ref[...], preferred_element_type=jnp.float32)
    up = jnp.dot(x_ref[...], up_ref[...], preferred_element_type=jnp.float32)
    hidden = (jax.nn.silu(gate) * up).astype(jnp.bfloat16)
    partial = lax.dot_general(
        hidden, down_ref[...], (((1,), (1,)), ((), ())), preferred_element_type=jnp.float32
    )

    @pl.when(step == 0)
    def _():
        total[...] = partial

    @pl.when(step > 0)
    def _():
        total[...] += partial

    @pl.when(step == pl.num_programs(0) - 1)
    def _():
        out_ref[...] = total[...].astype(jnp.bfloat16)


def ffn(x, weights):
    rows, model = x.shape
    units = weights.shape[1] // 3
    width = 256 if units % 256 == 0 else 128
    count = units // width
    return pl.pallas_call(
        ffn_kernel,
        grid=(count,),
        out_shape=jax.ShapeDtypeStruct((rows, model), jnp.bfloat16),
        in_specs=[
            pl.BlockSpec((rows, model), lambda j: (0, 0)),
            pl.BlockSpec((model, width), lambda j: (0, j)),
            pl.BlockSpec((model, width), lambda j: (0, count + j)),
            pl.BlockSpec((model, width), lambda j: (0, 2 * count + j)),
        ],
        out_specs=pl.BlockSpec((rows, model), lambda j: (0, 0)),
        scratch_shapes=[pltpu.VMEM((rows, model), jnp.float32)],
        compiler_params=pltpu.CompilerParams(vmem_limit_bytes=VMEM_BYTES),
        cost_estimate=pl.CostEstimate(
            flops=6 * rows * model * units,
            bytes_accessed=2 * (2 * rows * model + 3 * model * units),
            transcendentals=rows * units,
        ),
    )(x, weights, weights, weights)


def matmul_t(rows, weight_t):
    return lax.dot_general(
        rows, weight_t, (((1,), (1,)), ((), ())), preferred_element_type=jnp.float32
    )


def ring_chip(place, chips):
    half = chips // 2
    turned = place // half
    row = place * (1 - turned) + (chips - 1 - place) * turned
    return row * 2 + turned


def remote(src, dst, sent, landed, device):
    return pltpu.make_async_remote_copy(
        src_ref=src,
        dst_ref=dst,
        send_sem=sent,
        recv_sem=landed,
        device_id=device,
        device_id_type=pl.DeviceIdType.MESH,
    )


def branch_on(condition, body):
    if isinstance(condition, bool):
        if condition:
            body()
    else:
        pl.when(condition)(body)


def both(first, second):
    if isinstance(first, bool) and isinstance(second, bool):
        return first and second
    return jnp.logical_and(first, second)


def either(first, second):
    if isinstance(first, bool) and isinstance(second, bool):
        return first or second
    return jnp.logical_or(first, second)


def layer_kernel(
    size,
    tokens_ref,
    branch_ref,
    gelu_ref,
    outw_ref,
    gate_ref,
    up_ref,
    down_ref,
    gain0_ref,
    gain1_ref,
    gain2_ref,
    gain3_ref,
    taps_ref,
    rec_ref,
    inp_ref,
    decay_ref,
    out_ref,
    mine,
    gains,
    conv_ref,
    gates_ref,
    coef_ref,
    full,
    far_out,
    other,
    xm,
    pad,
    gel,
    a0,
    u0,
    a1,
    u1,
    hid,
    got,
    total,
    squares,
    hf,
    part,
    back,
    ring_send,
    ring_recv,
    near_send,
    near_recv,
    own_sem,
    small_sem,
    mine_sem,
    out_sem,
    tok_send,
    tok_recv,
    cross_send,
    cross_recv,
    share_send,
    share_recv,
    hid_send,
    hid_recv,
    back_send,
    back_recv,
):
    chips = size // 2
    reach = chips // 2
    stages = full.shape[0]
    depth, channels = branch_ref.shape
    prow = depth // PIECES
    half, model = tokens_ref.shape
    blocks, width = pad.shape[0], pad.shape[2]
    group = gates_ref.shape[1]
    units = hf.shape[2]
    span = 2 * depth

    me = lax.axis_index("fs")
    core = me % 2
    turned = (me // 2) % 2
    row = me // 4
    place = row * (1 - turned) + (chips - 1 - row) * turned
    column = lax.axis_index("tp")

    def chip_at(offset):
        return ring_chip((place + chips + offset) % chips, chips)

    targets = ({"fs": chip_at(1) * 2 + core}, {"fs": chip_at(-1) * 2 + core})
    partner = {"fs": me + 1 - 2 * core}
    across = {"tp": 1 - column}

    cut = units // 2
    own_rows = pl.ds(pl.multiple_of(me * depth, depth), depth)

    def own_part(g, source, lanes, at):
        place_at = full.at[g, own_rows, pl.ds(at, lanes.size)]
        return pltpu.make_async_copy(source.at[:, lanes], place_at, own_sem.at[g])

    every = pl.ds(0, channels)
    ucols = 256
    unit_chunks = cut // ucols

    def unit_parts(first):
        found = []
        for c in range(unit_chunks):
            for side, source in enumerate((gate_ref, up_ref)):
                at = (2 * c + side) * ucols
                found.append((source, pl.ds(first + c * ucols, ucols), at))
        return found

    own_copies = [
        [own_part(0, source, every, i * channels) for i, source in enumerate((branch_ref, gelu_ref, outw_ref))],
        [own_part(1, *pair) for pair in unit_parts(0)],
        [own_part(2, *pair) for pair in unit_parts(cut)],
        [own_part(3, down_ref, pl.ds(0, units), 0)],
    ]
    for copy in own_copies[0]:
        copy.start()
    chunk = 128
    mine_copy = pltpu.make_async_copy(tokens_ref, mine, mine_sem.at[0])
    mine_copy.start()
    small = [(source, gains.at[i]) for i, source in enumerate((gain0_ref, gain1_ref, gain2_ref, gain3_ref))]
    small += [(taps_ref, conv_ref), (decay_ref, coef_ref)]
    for d in range(2):
        for i, source in enumerate((rec_ref, inp_ref)):
            lanes = pl.ds((2 * d + i) * group, group)
            small.append((source.at[d], gates_ref.at[:, :, lanes]))
    small = [
        pltpu.make_async_copy(source, place_at, small_sem.at[i])
        for i, (source, place_at) in enumerate(small)
    ]
    for copy in small:
        copy.start()
    for copies in own_copies[1:]:
        for copy in copies:
            copy.start()

    barrier = pltpu.get_barrier_semaphore()
    for device in (*targets, partner, across):
        pl.semaphore_signal(barrier, inc=1, device_id=device, device_id_type=pl.DeviceIdType.MESH)
    pl.semaphore_wait(barrier, 4)

    def piece(g, chip, p):
        start = pl.multiple_of((chip * 2 + core) * depth + p * prow, prow)
        return full.at[g, pl.ds(start, prow), :]

    def shard_rows(g, chip, which):
        start = pl.multiple_of((chip * 2 + which) * depth, depth)
        return full.at[g, pl.ds(start, depth), :]

    def start_piece(g, p):
        src = piece(g, me // 2, p)
        dst = src
        for way in range(2):
            remote(src, dst, ring_send.at[way, g], ring_recv.at[g, 0, p], targets[way]).start()
        remote(src, dst, near_send.at[g], near_recv.at[g, 0], partner).start()

    def landed(g, s, p):
        rows = full.at[g, pl.ds(0, 2 * prow), :]
        remote(rows, rows, ring_send.at[0, g], ring_recv.at[g, s, p], targets[0]).wait_recv()

    def pass_piece(g, s, p):
        landed(g, s - 1, p)
        for way in range(2):
            ref = piece(g, chip_at(-s if way == 0 else s), p)
            slot = 2 * s - 1 + way

            def forward():
                index = jnp.where(s < reach - 1, p, p // 2)
                remote(
                    ref, ref, ring_send.at[way, g], ring_recv.at[g, s, index], targets[way]
                ).start()

            mine = p % 2 == way
            branch_on(either(s < reach - 1, mine), forward)
            remote(ref, ref, near_send.at[g], near_recv.at[g, slot], partner).start()

    def last_piece(g, q):
        landed(g, reach - 1, q)
        for way in range(2):
            ref = piece(g, chip_at(reach), 2 * q + way)
            remote(ref, ref, near_send.at[g], near_recv.at[g, chips - 1], partner).start()

    head = PIECES + PIECES // 2
    per_stage = head + (reach - 1) * PIECES

    def tick(e):
        g = e // per_stage
        k = e % per_stage
        branch_on(both(k < PIECES, g < stages), lambda: start_piece(g, k))
        branch_on(
            both(both(k >= PIECES, k < head), g > 0), lambda: last_piece(g - 1, k - PIECES)
        )
        branch_on(
            both(k >= head, g < stages),
            lambda: pass_piece(g, (k - head) // PIECES + 1, (k - head) % PIECES),
        )

    def ticks(first, last):
        @pl.loop(first, last)
        def _(e):
            tick(e)

    def near_wait(g, slot):
        ref = shard_rows(g, 0, 0)
        remote(ref, ref, near_send.at[g], near_recv.at[g, slot], partner).wait_recv()

    token_rows = half // TOKEN_PIECES
    for i in range(TOKEN_PIECES):
        rows = pl.ds(i * token_rows, token_rows)
        remote(tokens_ref.at[rows, :], other.at[rows, :], tok_send.at[0], tok_recv.at[i], across).start()
    def own_wait(g):
        rows = shard_rows(g, me // 2, core)
        pltpu.make_async_copy(rows, rows, own_sem.at[g]).wait()

    own_wait(0)
    ticks(0, PIECES)
    for copy in (*small, mine_copy):
        copy.wait()
    for g in range(1, stages):
        own_wait(g)
    slow = coef_ref[...]
    coef_ref[...] = -8.0 * (jnp.maximum(-slow, 0.0) + jnp.log1p(jnp.exp(-jnp.abs(slow))))

    def norm_rows(source, h, at):
        rows = pl.ds(at, chunk)
        values = source[rows, :].astype(jnp.float32)
        xm[h, rows, :] = normed(values, gains[0]).astype(jnp.bfloat16)

    @pl.loop(0, half // chunk)
    def _(i):
        norm_rows(mine, 0, pl.multiple_of(i * chunk, chunk))

    length = 2 * half
    for b in range(blocks):
        pad[b, 0:8, :] = jnp.zeros((8, width), jnp.float32)
        pad[b, 8 + length : 16 + length, :] = jnp.zeros((8, width), jnp.float32)

    done0 = per_stage + head
    ticks(PIECES, done0)

    @pl.loop(0, chips)
    def _(slot):
        near_wait(0, slot)

    @pl.loop(0, chips)
    def _(chip):
        src = shard_rows(0, chip, core).at[:, pl.ds(2 * channels, channels)]
        dst = far_out.at[pl.ds(pl.multiple_of((chip * 2 + core) * depth, depth), depth), :]
        remote(src, dst, cross_send.at[0], cross_recv.at[0], across).start()

    prows = 256
    scan0 = done0 + 2 * (2 * (half // prows) - 1) + 1

    @pl.loop(0, 2)
    def _(h):
        @pl.loop(0, half // prows)
        def _(i):
            at = pl.multiple_of(i * prows, prows)

            @pl.when(h == 1)
            def _():
                @pl.loop(0, prows // token_rows)
                def _(q):
                    n = i * (prows // token_rows) + q
                    rows = pl.ds(pl.multiple_of(n * token_rows, token_rows), token_rows)
                    remote(
                        tokens_ref.at[rows, :],
                        other.at[rows, :],
                        tok_send.at[0],
                        tok_recv.at[n],
                        across,
                    ).wait_recv()

                @pl.loop(0, prows // chunk)
                def _(q):
                    norm_rows(other, 1, pl.multiple_of(at + q * chunk, chunk))

                @pl.when(i == half // prows - 1)
                def _():
                    tick(scan0 - 1)

            x = xm[h, pl.ds(at, prows), :]
            side = jnp.where(h == 0, column, 1 - column)
            base = pl.multiple_of(8 + side * half + at, 8)
            for b in range(blocks):
                lanes = slice(b * width, (b + 1) * width)
                branch = jnp.dot(x, full[0, :, lanes], preferred_element_type=jnp.float32)
                pad[b, pl.ds(base, prows), :] = branch.astype(jnp.bfloat16).astype(jnp.float32)
                lanes = slice(channels + b * width, channels + (b + 1) * width)
                gelu_in = jnp.dot(x, full[0, :, lanes], preferred_element_type=jnp.float32)
                gelu_in = gelu_in.astype(jnp.bfloat16).astype(jnp.float32)
                gel[h, b, pl.ds(at, prows), :] = jax.nn.gelu(gelu_in).astype(jnp.bfloat16)

            @pl.when(h * (half // prows) + i < 2 * (half // prows) - 1)
            def _():
                ticks(done0 + h * 4 + i * 2, done0 + h * 4 + i * 2 + 2)

    parts = width // group
    steps = length // SEGMENTS
    pitch = steps + PITCH_PAD
    crows = 256

    quarter = half // 2

    def hid_copies(b, h):
        copies = []
        for r in range(2):
            rows = pl.ds(r * quarter, quarter)
            copies.append(
                remote(
                    hid.at[b, h, rows, :],
                    got.at[b, h, rows, :],
                    hid_send.at[0],
                    hid_recv.at[b, h, r],
                    across,
                )
            )
        return copies

    @pl.loop(0, blocks)
    def _(b):
        at = scan0 + b * SCAN_TICKS
        count = 0
        for n in range(parts):
            lanes = slice(n * group, (n + 1) * group)
            table = pl.ds(pl.multiple_of(b * width + n * group, group), group)
            taps = conv_ref[:, table].astype(jnp.float32)
            coef = coef_ref[:, table]
            for start in range(0, length, crows):
                summed = taps[0:1] * pad[b, 6 + start : 6 + start + crows, lanes]
                for j in range(1, 4):
                    first = 6 + j + start
                    summed = summed + taps[j : j + 1] * pad[b, first : first + crows, lanes]
                conv = summed.astype(jnp.bfloat16)
                wide = conv.astype(jnp.float32)
                for d, (a_ref, u_ref) in enumerate(((a0, u0), (a1, u1))):
                    gate = jnp.dot(
                        conv,
                        gates_ref[b * parts + n, :, 2 * d * group : 2 * (d + 1) * group],
                        preferred_element_type=jnp.float32,
                    )
                    rate = jax.nn.sigmoid(gate[:, :group])
                    inflow = jax.nn.sigmoid(gate[:, group:])
                    log_retain = rate * coef[d : d + 1]
                    retain = jnp.exp(log_retain)
                    left = one_minus_exp(2.0 * log_retain, retain * retain)
                    feed = jnp.sqrt(left) * inflow * wide
                    for q in range(crows // steps):
                        first = (start // steps + q) * pitch
                        a_ref[n, first : first + steps, :] = retain[q * steps : (q + 1) * steps]
                        u_ref[n, first : first + steps, :] = feed[q * steps : (q + 1) * steps]
                if (start // crows) % 2 == 1:
                    tick(at + count)
                    count += 1

        def step(t, carry):
            out = []
            for (state, decayed), (a_ref, u_ref), when in (
                (carry[0], (a0, u0), t),
                (carry[1], (a1, u1), steps - 1 - t),
            ):
                where = pl.ds(when, SEGMENTS, stride=pitch)
                nstate, ndecayed = [], []
                for n in range(parts):
                    retain = a_ref[n, where, :]
                    h = retain * state[n] + u_ref[n, where, :]
                    p = retain * decayed[n]
                    u_ref[n, where, :] = h
                    a_ref[n, where, :] = p
                    nstate.append(h)
                    ndecayed.append(p)
                out.append((tuple(nstate), tuple(ndecayed)))
            return tuple(out)

        zero = tuple(jnp.zeros((SEGMENTS, group), jnp.float32) for n in range(parts))
        one = tuple(jnp.ones((SEGMENTS, group), jnp.float32) for n in range(parts))
        ended = ((zero, one), (zero, one))
        for run in range(2):
            first, last = run * steps // 2, (run + 1) * steps // 2
            ended = lax.fori_loop(first, last, step, ended, unroll=8)
            if run == 0:
                tick(at + count)
                count += 1
        per_half = SEGMENTS // 2
        for n in range(parts):
            lanes = slice(n * group, (n + 1) * group)
            blank = jnp.zeros((1, group), jnp.float32)
            entry = [[None] * SEGMENTS, [None] * SEGMENTS]
            for d, order in ((0, range(SEGMENTS)), (1, range(SEGMENTS - 1, -1, -1))):
                carry = blank
                for s in order:
                    entry[d][s] = carry
                    carry = ended[d][0][n][s : s + 1] + ended[d][1][n][s : s + 1] * carry
            for s in range(SEGMENTS):
                rows = slice(s * pitch, s * pitch + steps)
                local = slice((s % per_half) * steps, (s % per_half + 1) * steps)
                which = jnp.where(column == s // per_half, 0, 1)
                forward = u0[n, rows, :] + a0[n, rows, :] * entry[0][s]
                backward = u1[n, rows, :] + a1[n, rows, :] * entry[1][s]
                gate = gel[which, b, local, lanes].astype(jnp.float32)
                hid[b, which, local, lanes] = (gate * (forward + backward)).astype(jnp.bfloat16)
        tick(at + count)
        count += 1
        assert count == SCAN_TICKS
        for copy in hid_copies(b, 0):
            copy.start()

    for b in range(blocks):
        for copy in hid_copies(b, 1):
            copy.start()
    out0 = scan0 + blocks * SCAN_TICKS


    whole = slice(0, half)

    def mixed(h, own_blocks, far_blocks, fresh, e0=0, count=0, tall=whole, ocols=512):
        left = [hid[b, h, tall] for b in own_blocks]
        left = jnp.concatenate(left, axis=1) if left else None
        right = [got[b, 1 - h, tall] for b in far_blocks]
        right = jnp.concatenate(right, axis=1) if right else None
        parts_n = model // ocols

        @pl.loop(0, parts_n)
        def _(n):
            rows = pl.ds(pl.multiple_of(n * ocols, ocols), ocols)
            lanes = rows
            summed = None if fresh else total[tall, lanes]
            if left is not None:
                first = 2 * channels + own_blocks[0] * width
                term = matmul_t(left, full[0, rows, first : first + len(own_blocks) * width])
                summed = term if summed is None else summed + term
            if right is not None:
                first = far_blocks[0] * width
                term = matmul_t(right, far_out[rows, first : first + len(far_blocks) * width])
                summed = term if summed is None else summed + term
            total[tall, lanes] = summed
            if count:
                every_n = parts_n // count

                @pl.when(n % every_n == every_n - 1)
                def _():
                    tick(e0 + n // every_n)

    def settle(h, source, tall=whole):
        @pl.loop(tall.start // chunk, tall.stop // chunk)
        def _(i):
            rows = pl.ds(pl.multiple_of(i * chunk, chunk), chunk)
            stream = source[rows, :].astype(jnp.float32)
            residual = stream + normed(total[rows, :], gains[1])
            residual = residual.astype(jnp.bfloat16)
            if h == 0:
                source[rows, :] = residual
            middle = normed(residual.astype(jnp.float32), gains[2])
            xm[h, rows, :] = middle.astype(jnp.bfloat16)

    all_blocks = tuple(range(blocks))
    mixed(1, all_blocks, (), True, out0, 2)
    tick(out0 + 2)

    ref = far_out.at[pl.ds(0, chips * depth), :]
    remote(ref, ref, cross_send.at[0], cross_recv.at[0], across).wait_recv()

    @pl.loop(0, chips)
    def _(chip):
        ref = far_out.at[pl.ds(pl.multiple_of((chip * 2 + core) * depth, depth), depth), :]
        remote(ref, ref, share_send.at[0], share_recv.at[0], partner).start()

    ffn0 = out0 + 3
    for b in all_blocks[:-1]:
        ticks(ffn0, ffn0 + 2)
        for copy in hid_copies(b, 0):
            copy.wait_recv()
        if b == 0:
            ref = far_out.at[pl.ds(0, chips * depth), :]
            remote(ref, ref, share_send.at[0], share_recv.at[0], partner).wait_recv()
        mixed(1, (), (b,), False, ffn0 + 2, 1)
        ffn0 += 3
    for r, copy in enumerate(hid_copies(blocks - 1, 0)):
        tall = slice(r * quarter, (r + 1) * quarter)
        copy.wait_recv()
        if r == 1:
            tick(ffn0)
            ffn0 += 1
        mixed(1, (), (blocks - 1,), False, tall=tall, ocols=model // 2)
        if r == 0:
            tick(ffn0)
            ffn0 += 1
        settle(1, other, tall)

    def activate(g, h, c, product):
        lanes = pl.ds(pl.multiple_of((g - 1) * cut + c * ucols, ucols), ucols)
        hidden = jax.nn.silu(product[:, :ucols]) * product[:, ucols:]
        hf[h, :, lanes] = hidden.astype(jnp.bfloat16)

    def expand(g, h, c):
        lanes = pl.ds(pl.multiple_of(2 * c * ucols, 2 * ucols), 2 * ucols)
        activate(g, h, c, jnp.dot(xm[h], full[g, :, lanes], preferred_element_type=jnp.float32))

    first_done = 2 * per_stage + head
    second_done = 3 * per_stage + head
    ticks(min(ffn0, first_done), first_done)
    ffn1 = max(ffn0, first_done)

    @pl.loop(0, chips)
    def _(slot):
        near_wait(1, slot)

    def feature_chip(slot):
        d = (slot + 1) // 2
        return chip_at(jnp.where(slot % 2 == 1, -d, d))

    def expand_part(g, h, c, slots, fresh, last):
        rows = [pl.ds(pl.multiple_of(feature_chip(slot) * span, span), span) for slot in slots]
        x = jnp.concatenate([xm[h, :, at] for at in rows], axis=1)
        lanes = pl.ds(pl.multiple_of(2 * c * ucols, 2 * ucols), 2 * ucols)
        w = jnp.concatenate([full[g, at, lanes] for at in rows], axis=0)
        term = jnp.dot(x, w, preferred_element_type=jnp.float32)
        if not fresh:
            term = total[:, lanes] + term
        if last:
            activate(g, h, c, term)
        else:
            total[:, lanes] = term

    ffn2 = ffn1 + 2
    before = second_done - PIECES // 2
    parts_b = (tuple(range(chips - 3)), (chips - 3, chips - 2), (chips - 1,))

    @pl.loop(0, unit_chunks)
    def _(c):
        expand(1, 1, c)

        @pl.when(c < 2)
        def _():
            tick(ffn1 + c)

    for slot in parts_b[0]:
        near_wait(2, slot)

    @pl.loop(0, unit_chunks)
    def _(c):
        expand_part(2, 1, c, parts_b[0], True, False)

        @pl.when(c == 0)
        def _():
            tick(ffn2)

        @pl.when(c == 1)
        def _():
            ticks(ffn2 + 1, before)

        @pl.when(c == 2)
        def _():
            tick(before)

    for n in (1, 2):
        if n == 2:
            tick(before + 1)
        for slot in parts_b[n]:
            near_wait(2, slot)
        for c in range(unit_chunks):
            expand_part(2, 1, c, parts_b[n], False, n == 2)

    def partial_of(h, chip):
        weight = full[stages - 1, pl.ds(pl.multiple_of(chip * span, span), span), :]
        return matmul_t(hf[h], weight)

    def back_copy(slot):
        chip = feature_chip(slot)
        return remote(part.at[chip], back.at[chip], back_send.at[0], back_recv.at[slot], across)

    distance1 = (stages - 1) * per_stage + head

    def last_copy(i):
        chip = feature_chip(chips - 1)
        rows = pl.ds(pl.multiple_of(i * chunk, chunk), chunk)
        return remote(
            part.at[chip, rows, :],
            back.at[chip, rows, :],
            back_send.at[0],
            back_recv.at[chips - 1 + i],
            across,
        )

    def send_back(slot):
        near_wait(stages - 1, slot)
        chip = feature_chip(slot)
        part[chip] = partial_of(1, chip).astype(jnp.bfloat16)
        if isinstance(slot, int) and slot == chips - 1:
            for i in range(half // chunk):
                last_copy(i).start()
        else:
            back_copy(slot).start()

    def send_pair(d):
        @pl.loop(2 * d - 1, 2 * d + 1)
        def _(slot):
            send_back(slot)

    send_back(0)
    for b in all_blocks:
        for copy in hid_copies(b, 1):
            copy.wait_recv()
    mixed(0, all_blocks, (), True, distance1, PIECES)
    send_pair(1)
    mixed(0, (), all_blocks, False, distance1 + PIECES, 2)
    settle(0, mine)
    tick(distance1 + PIECES + 2)

    @pl.loop(0, unit_chunks)
    def _(c):
        expand(1, 0, c)

        @pl.when(c == 1)
        def _():
            tick(distance1 + PIECES + 3)

    send_pair(2)

    @pl.loop(0, unit_chunks)
    def _(c):
        expand(2, 0, c)
        tick(distance1 + 2 * PIECES + c)

    ticks(distance1 + 2 * PIECES + unit_chunks, distance1 + 3 * PIECES)
    send_pair(3)
    ticks(stages * per_stage + PIECES, stages * per_stage + head)
    send_back(chips - 1)

    @pl.loop(0, chips)
    def _(chip):
        lanes = pl.ds(pl.multiple_of(chip * span, span), span)
        total[:, lanes] = partial_of(0, chip).astype(jnp.bfloat16).astype(jnp.float32)

    squares[...] = jnp.zeros_like(squares)

    def add_back(slot, i):
        chip = feature_chip(slot)
        lanes = pl.ds(pl.multiple_of(chip * span, span), span)
        rows = pl.ds(pl.multiple_of(i * chunk, chunk), chunk)
        summed = total[rows, lanes] + back[chip, rows, :].astype(jnp.float32)
        total[rows, lanes] = summed
        square = summed * summed
        folded = square[:, :128]
        for at in range(128, span, 128):
            folded = folded + square[:, at : at + 128]
        squares[rows, :] += folded

    @pl.loop(0, chips - 1)
    def _(slot):
        back_copy(slot).wait_recv()

        @pl.loop(0, half // chunk)
        def _(i):
            add_back(slot, i)

    @pl.loop(0, half // chunk)
    def _(i):
        last_copy(i).wait_recv()
        add_back(chips - 1, i)
        rows = pl.ds(pl.multiple_of(i * chunk, chunk), chunk)
        mean = jnp.sum(squares[rows, :], axis=-1, keepdims=True) * (1.0 / model)
        scaled = total[rows, :] * lax.rsqrt(mean + EPS) * gains[3]
        middle = mine[rows, :].astype(jnp.float32)
        mine[rows, :] = (middle + scaled).astype(jnp.bfloat16)
        pltpu.make_async_copy(mine.at[rows, :], out_ref.at[rows, :], out_sem.at[0]).start()

    for g in range(stages):
        rows = full.at[g, pl.ds(0, (reach - 1) * depth + depth // 2), :]
        for way in range(2):
            remote(
                rows, rows, ring_send.at[way, g], ring_recv.at[g, 0, 0], targets[way]
            ).wait_send()
        rows = full.at[g, pl.ds(0, chips * depth), :]
        remote(rows, rows, near_send.at[g], near_recv.at[g, 0], partner).wait_send()
    remote(mine, other, tok_send.at[0], tok_recv.at[0], across).wait_send()
    ref = far_out.at[pl.ds(0, chips * depth), :]
    remote(ref, ref, cross_send.at[0], cross_recv.at[0], across).wait_send()
    remote(ref, ref, share_send.at[0], share_recv.at[0], partner).wait_send()
    remote(hid, got, hid_send.at[0], hid_recv.at[0, 0, 0], across).wait_send()
    remote(part, back, back_send.at[0], back_recv.at[0], across).wait_send()
    pltpu.make_async_copy(mine, out_ref, out_sem.at[0]).wait()


def paired_device(
    tokens,
    pre_mix_gain,
    post_mix_gain,
    pre_ffn_gain,
    post_ffn_gain,
    w_branch,
    w_gelu,
    conv_weight,
    w_rec,
    w_inp,
    decay,
    out_weight_t,
    w_gate,
    w_up,
    down_weight_t,
):
    half, model = tokens.shape
    depth, channels = w_branch.shape
    units = w_gate.shape[1]
    size = lax.axis_size("fs")
    chips = size // 2
    group = w_rec.shape[2]
    width = min(256, channels)
    blocks = channels // width
    length = 2 * half
    bf16 = functools.partial(pltpu.VMEM, dtype=jnp.bfloat16)
    f32 = functools.partial(pltpu.VMEM, dtype=jnp.float32)
    dma = pltpu.SemaphoreType.DMA
    stages = 4
    groups = channels // group
    reach = chips // 2
    hbm = pl.BlockSpec(memory_space=pl.ANY)
    gains = (pre_mix_gain, post_mix_gain, pre_ffn_gain, post_ffn_gain)
    return pl.pallas_call(
        functools.partial(layer_kernel, size),
        out_shape=jax.ShapeDtypeStruct((half, model), jnp.bfloat16),
        in_specs=[hbm] * 15,
        out_specs=hbm,
        scratch_shapes=[
            bf16((half, model)),
            f32((4, 1, model)),
            bf16(conv_weight.shape),
            bf16((groups, group, 4 * group)),
            f32(decay.shape),
            bf16((stages, model, 3 * channels)),
            bf16((model, channels)),
            bf16((half, model)),
            bf16((2, half, model)),
            f32((blocks, length + 16, width)),
            bf16((2, blocks, half, width)),
        ]
        + [f32((width // group, length + SEGMENTS * PITCH_PAD, group)) for i in range(4)]
        + [
            bf16((blocks, 2, half, width)),
            bf16((blocks, 2, half, width)),
            f32((half, model)),
            f32((half, 128)),
            bf16((2, half, units)),
            bf16((chips, half, 2 * depth)),
            bf16((chips, half, 2 * depth)),
            dma((2, stages)),
            dma((stages, reach, PIECES)),
            dma((stages,)),
            dma((stages, chips)),
            dma((stages,)),
            dma((10,)),
            dma((1,)),
            dma((1,)),
            dma((1,)),
            dma((TOKEN_PIECES,)),
            dma((1,)),
            dma((1,)),
            dma((1,)),
            dma((1,)),
            dma((1,)),
            dma((blocks, 2, 2)),
            dma((1,)),
            dma((chips - 1 + half // 128,)),
        ],
        compiler_params=pltpu.CompilerParams(
            collective_id=0, has_side_effects=True, vmem_limit_bytes=MOST_VMEM
        ),
        cost_estimate=pl.CostEstimate(
            flops=1 << 34, bytes_accessed=1 << 26, transcendentals=1 << 24
        ),
    )(
        tokens,
        w_branch,
        w_gelu,
        out_weight_t,
        w_gate,
        w_up,
        down_weight_t,
        *(gain.reshape(1, model) for gain in gains),
        conv_weight,
        w_rec,
        w_inp,
        decay,
    )


def wide_device(
    tokens,
    pre_mix_gain,
    post_mix_gain,
    pre_ffn_gain,
    post_ffn_gain,
    w_branch,
    w_gelu,
    conv_weight,
    w_rec,
    w_inp,
    decay,
    out_weight_t,
    w_gate,
    w_up,
    down_weight_t,
):
    channels = conv_weight.shape[1]
    mix_shard = jnp.concatenate([w_branch, w_gelu, out_weight_t], axis=1)
    ffn_shard = jnp.concatenate([w_gate, w_up, down_weight_t], axis=1)
    stream = tokens.astype(jnp.float32)
    normed_in = normed(stream, pre_mix_gain).astype(jnp.bfloat16)
    mix_all = lax.all_gather(mix_shard, "fs", axis=0, tiled=True)
    whole = lax.all_gather(normed_in, "tp", axis=0, tiled=True)
    ffn_all = lax.all_gather(ffn_shard, "fs", axis=0, tiled=True)
    out_own = mix_all[:, 2 * channels :]
    hidden = mixer(whole, mix_all, conv_weight, w_rec, w_inp, decay)
    own_hidden = lax.all_to_all(hidden, "tp", split_axis=0, concat_axis=1, tiled=True)
    out_whole = lax.all_gather(out_own, "tp", axis=1, tiled=True)
    mixer_sum = matmul_t(own_hidden, out_whole)
    residual = (stream + normed(mixer_sum, post_mix_gain)).astype(jnp.bfloat16)
    middle = residual.astype(jnp.float32)
    normed_mid = normed(middle, pre_ffn_gain).astype(jnp.bfloat16)
    all_mid = lax.all_gather(normed_mid, "tp", axis=0, tiled=True)
    ffn_sum = lax.psum_scatter(
        ffn(all_mid, ffn_all), "tp", scatter_dimension=0, tiled=True
    ).astype(jnp.float32)
    return (middle + normed(ffn_sum, post_ffn_gain)).astype(jnp.bfloat16)


def solution(mesh):
    return jax.shard_map(
        paired_device if mesh.shape["tp"] == 2 else wide_device,
        mesh=mesh,
        in_specs=(
            P(("fs", "tp"), None),
            P(),
            P(),
            P(),
            P(),
            P("fs", "tp"),
            P("fs", "tp"),
            P(None, "tp"),
            P(None, "tp", None, None),
            P(None, "tp", None, None),
            P(None, "tp"),
            P("fs", "tp"),
            P("fs", "tp"),
            P("fs", "tp"),
            P("fs", "tp"),
        ),
        out_specs=P(("fs", "tp"), None),
        check_vma=False,
    )
```

```python
import functools

import jax
import jax.numpy as jnp
from jax import lax
from jax.experimental import pallas as pl
from jax.experimental.pallas import tpu as pltpu
from jax.sharding import PartitionSpec as P

EPS = 1e-06
SEGMENTS = 8
PIECES = 4
TOKEN_PIECES = 4
SCAN_TICKS = 6
PITCH_PAD = 8
MOST_VMEM = 67043328
VMEM_BYTES = 60 * 1024 * 1024


def normed(values, gain):
    factor = lax.rsqrt(jnp.mean(values * values, axis=-1, keepdims=True) + EPS)
    return values * factor * gain


def one_minus_exp(y, exp_y):
    series = 1.0 + y * (1.0 / 8.0)
    for order in (7, 6, 5, 4, 3, 2):
        series = 1.0 + y * (1.0 / order) * series
    return jnp.where(y > -0.5, -y * series, 1.0 - exp_y)


def mixer_kernel(
    x_ref, wb_ref, wg_ref, conv_ref, gates_ref, coef_ref, out_ref, pad, gel, a0, u0, a1, u1
):
    length, width = out_ref.shape
    group = gates_ref.shape[1]
    rows = 256
    pad[0:8, :] = jnp.zeros((8, width), jnp.float32)
    pad[8 + length : 16 + length, :] = jnp.zeros((8, width), jnp.float32)
    sources = ((x_ref, 0),)
    for source, base in sources:
        for start in range(0, source.shape[0], rows):
            piece = source[start : start + rows, :]
            branch = jnp.dot(piece, wb_ref[...], preferred_element_type=jnp.float32)
            gelu_in = jnp.dot(piece, wg_ref[...], preferred_element_type=jnp.float32)
            at = pl.multiple_of(base + start, rows)
            pad[pl.ds(8 + at, rows), :] = branch.astype(jnp.bfloat16).astype(jnp.float32)
            gel[pl.ds(at, rows), :] = jax.nn.gelu(
                gelu_in.astype(jnp.bfloat16).astype(jnp.float32)
            )

    for part in range(width // group):
        cols = slice(part * group, (part + 1) * group)
        taps = conv_ref[:, cols].astype(jnp.float32)
        coef = coef_ref[:, cols]
        for start in range(0, length, rows):
            summed = taps[0:1] * pad[6 + start : 6 + start + rows, cols]
            for j in range(1, 4):
                summed = summed + taps[j : j + 1] * pad[6 + j + start : 6 + j + start + rows, cols]
            conv = summed.astype(jnp.bfloat16)
            wide = conv.astype(jnp.float32)
            for d, (a_ref, u_ref) in enumerate(((a0, u0), (a1, u1))):
                gate = jnp.dot(
                    conv,
                    gates_ref[part, :, 2 * d * group : 2 * (d + 1) * group],
                    preferred_element_type=jnp.float32,
                )
                rate = jax.nn.sigmoid(gate[:, :group])
                inflow = jax.nn.sigmoid(gate[:, group:])
                log_retain = rate * coef[d : d + 1]
                retain = jnp.exp(log_retain)
                left = one_minus_exp(2.0 * log_retain, retain * retain)
                a_ref[part, start : start + rows, :] = retain
                u_ref[part, start : start + rows, :] = jnp.sqrt(left) * inflow * wide

    steps = length // SEGMENTS

    def step(t, carry):
        out = []
        for (state, decayed), (a_ref, u_ref), at in (
            (carry[0], (a0, u0), t),
            (carry[1], (a1, u1), steps - 1 - t),
        ):
            where = pl.ds(at, SEGMENTS, stride=steps)
            nstate, ndecayed = [], []
            for c in range(n):
                retain = a_ref[c, where, :]
                h = retain * state[c] + u_ref[c, where, :]
                p = retain * decayed[c]
                u_ref[c, where, :] = h
                a_ref[c, where, :] = p
                nstate.append(h)
                ndecayed.append(p)
            out.append((tuple(nstate), tuple(ndecayed)))
        return tuple(out)

    n = width // group
    zero = tuple(jnp.zeros((SEGMENTS, group), jnp.float32) for c in range(n))
    one = tuple(jnp.ones((SEGMENTS, group), jnp.float32) for c in range(n))
    ended = lax.fori_loop(0, steps, step, ((zero, one), (zero, one)), unroll=8)
    for c in range(n):
        lanes = slice(c * group, (c + 1) * group)
        blank = jnp.zeros((1, group), jnp.float32)
        entry = [[None] * SEGMENTS, [None] * SEGMENTS]
        for d, order in ((0, range(SEGMENTS)), (1, range(SEGMENTS - 1, -1, -1))):
            carry = blank
            for s in order:
                entry[d][s] = carry
                carry = ended[d][0][c][s : s + 1] + ended[d][1][c][s : s + 1] * carry
        for s in range(SEGMENTS):
            span = slice(s * steps, (s + 1) * steps)
            forward = u0[c, span, :] + a0[c, span, :] * entry[0][s]
            backward = u1[c, span, :] + a1[c, span, :] * entry[1][s]
            out_ref[span, lanes] = (gel[span, lanes] * (forward + backward)).astype(jnp.bfloat16)


def mixer(x, weights, conv_weight, w_rec, w_inp, decay):
    length, model = x.shape
    channels = conv_weight.shape[1]
    group = w_rec.shape[2]
    width = min(256, channels)
    count = channels // width
    gates = jnp.concatenate([w_rec[0], w_inp[0], w_rec[1], w_inp[1]], axis=-1)
    coef = -8.0 * jax.nn.softplus(-decay)
    f32 = functools.partial(pltpu.VMEM, dtype=jnp.float32)
    return pl.pallas_call(
        mixer_kernel,
        grid=(count,),
        out_shape=jax.ShapeDtypeStruct((length, channels), jnp.bfloat16),
        in_specs=[
            pl.BlockSpec((length, model), lambda j: (0, 0)),
            pl.BlockSpec((model, width), lambda j: (0, j)),
            pl.BlockSpec((model, width), lambda j: (0, count + j)),
            pl.BlockSpec((4, width), lambda j: (0, j)),
            pl.BlockSpec((width // group, group, 4 * group), lambda j: (j, 0, 0)),
            pl.BlockSpec((2, width), lambda j: (0, j)),
        ],
        out_specs=pl.BlockSpec((length, width), lambda j: (0, j)),
        scratch_shapes=[f32((length + 16, width)), f32((length, width))]
        + [f32((width // group, length, group)) for i in range(4)],
        compiler_params=pltpu.CompilerParams(vmem_limit_bytes=VMEM_BYTES),
        cost_estimate=pl.CostEstimate(
            flops=4 * length * model * channels + 16 * length * group * channels * 8,
            bytes_accessed=2 * (length * model + 2 * model * channels + length * channels),
            transcendentals=12 * length * channels,
        ),
    )(x, weights, weights, conv_weight, gates, coef)


def ffn_kernel(x_ref, gate_ref, up_ref, down_ref, out_ref, total):
    step = pl.program_id(0)
    gate = jnp.dot(x_ref[...], gate_ref[...], preferred_element_type=jnp.float32)
    up = jnp.dot(x_ref[...], up_ref[...], preferred_element_type=jnp.float32)
    hidden = (jax.nn.silu(gate) * up).astype(jnp.bfloat16)
    partial = lax.dot_general(
        hidden, down_ref[...], (((1,), (1,)), ((), ())), preferred_element_type=jnp.float32
    )

    @pl.when(step == 0)
    def _():
        total[...] = partial

    @pl.when(step > 0)
    def _():
        total[...] += partial

    @pl.when(step == pl.num_programs(0) - 1)
    def _():
        out_ref[...] = total[...].astype(jnp.bfloat16)


def ffn(x, weights):
    rows, model = x.shape
    units = weights.shape[1] // 3
    width = 256 if units % 256 == 0 else 128
    count = units // width
    return pl.pallas_call(
        ffn_kernel,
        grid=(count,),
        out_shape=jax.ShapeDtypeStruct((rows, model), jnp.bfloat16),
        in_specs=[
            pl.BlockSpec((rows, model), lambda j: (0, 0)),
            pl.BlockSpec((model, width), lambda j: (0, j)),
            pl.BlockSpec((model, width), lambda j: (0, count + j)),
            pl.BlockSpec((model, width), lambda j: (0, 2 * count + j)),
        ],
        out_specs=pl.BlockSpec((rows, model), lambda j: (0, 0)),
        scratch_shapes=[pltpu.VMEM((rows, model), jnp.float32)],
        compiler_params=pltpu.CompilerParams(vmem_limit_bytes=VMEM_BYTES),
        cost_estimate=pl.CostEstimate(
            flops=6 * rows * model * units,
            bytes_accessed=2 * (2 * rows * model + 3 * model * units),
            transcendentals=rows * units,
        ),
    )(x, weights, weights, weights)


def matmul_t(rows, weight_t):
    return lax.dot_general(
        rows, weight_t, (((1,), (1,)), ((), ())), preferred_element_type=jnp.float32
    )


def ring_chip(place, chips):
    half = chips // 2
    turned = place // half
    row = place * (1 - turned) + (chips - 1 - place) * turned
    return row * 2 + turned


def remote(src, dst, sent, landed, device):
    return pltpu.make_async_remote_copy(
        src_ref=src,
        dst_ref=dst,
        send_sem=sent,
        recv_sem=landed,
        device_id=device,
        device_id_type=pl.DeviceIdType.MESH,
    )


def branch_on(condition, body):
    if isinstance(condition, bool):
        if condition:
            body()
    else:
        pl.when(condition)(body)


def both(first, second):
    if isinstance(first, bool) and isinstance(second, bool):
        return first and second
    return jnp.logical_and(first, second)


def either(first, second):
    if isinstance(first, bool) and isinstance(second, bool):
        return first or second
    return jnp.logical_or(first, second)


def layer_kernel(
    size,
    tokens_ref,
    branch_ref,
    gelu_ref,
    outw_ref,
    gate_ref,
    up_ref,
    down_ref,
    gain0_ref,
    gain1_ref,
    gain2_ref,
    gain3_ref,
    taps_ref,
    rec_ref,
    inp_ref,
    decay_ref,
    out_ref,
    mine,
    gains,
    conv_ref,
    gates_ref,
    coef_ref,
    full,
    far_out,
    other,
    xm,
    pad,
    gel,
    a0,
    u0,
    a1,
    u1,
    hid,
    got,
    total,
    squares,
    hf,
    part,
    back,
    ring_send,
    ring_recv,
    near_send,
    near_recv,
    own_sem,
    small_sem,
    mine_sem,
    out_sem,
    tok_send,
    tok_recv,
    cross_send,
    cross_recv,
    share_send,
    share_recv,
    hid_send,
    hid_recv,
    back_send,
    back_recv,
):
    chips = size // 2
    reach = chips // 2
    stages = full.shape[0]
    depth, channels = branch_ref.shape
    prow = depth // PIECES
    half, model = tokens_ref.shape
    blocks, width = pad.shape[0], pad.shape[2]
    group = gates_ref.shape[1]
    units = hf.shape[2]
    span = 2 * depth

    me = lax.axis_index("fs")
    core = me % 2
    turned = (me // 2) % 2
    row = me // 4
    place = row * (1 - turned) + (chips - 1 - row) * turned
    column = lax.axis_index("tp")

    def chip_at(offset):
        return ring_chip((place + chips + offset) % chips, chips)

    targets = ({"fs": chip_at(1) * 2 + core}, {"fs": chip_at(-1) * 2 + core})
    partner = {"fs": me + 1 - 2 * core}
    across = {"tp": 1 - column}

    cut = units // 2
    own_rows = pl.ds(pl.multiple_of(me * depth, depth), depth)

    def own_part(g, source, lanes, at):
        place_at = full.at[g, own_rows, pl.ds(at, lanes.size)]
        return pltpu.make_async_copy(source.at[:, lanes], place_at, own_sem.at[g])

    every = pl.ds(0, channels)
    ucols = 256
    unit_chunks = cut // ucols

    def unit_parts(first):
        found = []
        for c in range(unit_chunks):
            for side, source in enumerate((gate_ref, up_ref)):
                at = (2 * c + side) * ucols
                found.append((source, pl.ds(first + c * ucols, ucols), at))
        return found

    own_copies = [
        [own_part(0, source, every, i * channels) for i, source in enumerate((branch_ref, gelu_ref, outw_ref))],
        [own_part(1, *pair) for pair in unit_parts(0)],
        [own_part(2, *pair) for pair in unit_parts(cut)],
        [own_part(3, down_ref, pl.ds(0, units), 0)],
    ]
    for copy in own_copies[0]:
        copy.start()
    chunk = 128
    mine_copy = pltpu.make_async_copy(tokens_ref, mine, mine_sem.at[0])
    mine_copy.start()
    small = [(source, gains.at[i]) for i, source in enumerate((gain0_ref, gain1_ref, gain2_ref, gain3_ref))]
    small += [(taps_ref, conv_ref), (decay_ref, coef_ref)]
    for d in range(2):
        for i, source in enumerate((rec_ref, inp_ref)):
            lanes = pl.ds((2 * d + i) * group, group)
            small.append((source.at[d], gates_ref.at[:, :, lanes]))
    small = [
        pltpu.make_async_copy(source, place_at, small_sem.at[i])
        for i, (source, place_at) in enumerate(small)
    ]
    for copy in small:
        copy.start()
    for copies in own_copies[1:]:
        for copy in copies:
            copy.start()

    barrier = pltpu.get_barrier_semaphore()
    for device in (*targets, partner, across):
        pl.semaphore_signal(barrier, inc=1, device_id=device, device_id_type=pl.DeviceIdType.MESH)
    pl.semaphore_wait(barrier, 4)

    def piece(g, chip, p):
        start = pl.multiple_of((chip * 2 + core) * depth + p * prow, prow)
        return full.at[g, pl.ds(start, prow), :]

    def shard_rows(g, chip, which):
        start = pl.multiple_of((chip * 2 + which) * depth, depth)
        return full.at[g, pl.ds(start, depth), :]

    def start_piece(g, p):
        src = piece(g, me // 2, p)
        dst = src
        for way in range(2):
            remote(src, dst, ring_send.at[way, g], ring_recv.at[g, 0, p], targets[way]).start()
        remote(src, dst, near_send.at[g], near_recv.at[g, 0], partner).start()

    def landed(g, s, p):
        rows = full.at[g, pl.ds(0, 2 * prow), :]
        remote(rows, rows, ring_send.at[0, g], ring_recv.at[g, s, p], targets[0]).wait_recv()

    def pass_piece(g, s, p):
        landed(g, s - 1, p)
        for way in range(2):
            ref = piece(g, chip_at(-s if way == 0 else s), p)
            slot = 2 * s - 1 + way

            def forward():
                index = jnp.where(s < reach - 1, p, p // 2)
                remote(
                    ref, ref, ring_send.at[way, g], ring_recv.at[g, s, index], targets[way]
                ).start()

            mine = p % 2 == way
            branch_on(either(s < reach - 1, mine), forward)
            remote(ref, ref, near_send.at[g], near_recv.at[g, slot], partner).start()

    def last_piece(g, q):
        landed(g, reach - 1, q)
        for way in range(2):
            ref = piece(g, chip_at(reach), 2 * q + way)
            remote(ref, ref, near_send.at[g], near_recv.at[g, chips - 1], partner).start()

    head = PIECES + PIECES // 2
    per_stage = head + (reach - 1) * PIECES

    def tick(e):
        g = e // per_stage
        k = e % per_stage
        branch_on(both(k < PIECES, g < stages), lambda: start_piece(g, k))
        branch_on(
            both(both(k >= PIECES, k < head), g > 0), lambda: last_piece(g - 1, k - PIECES)
        )
        branch_on(
            both(k >= head, g < stages),
            lambda: pass_piece(g, (k - head) // PIECES + 1, (k - head) % PIECES),
        )

    def ticks(first, last):
        @pl.loop(first, last)
        def _(e):
            tick(e)

    def near_wait(g, slot):
        ref = shard_rows(g, 0, 0)
        remote(ref, ref, near_send.at[g], near_recv.at[g, slot], partner).wait_recv()

    token_rows = half // TOKEN_PIECES
    for i in range(TOKEN_PIECES):
        rows = pl.ds(i * token_rows, token_rows)
        remote(tokens_ref.at[rows, :], other.at[rows, :], tok_send.at[0], tok_recv.at[i], across).start()
    def own_wait(g):
        rows = shard_rows(g, me // 2, core)
        pltpu.make_async_copy(rows, rows, own_sem.at[g]).wait()

    own_wait(0)
    ticks(0, PIECES)
    for copy in (*small, mine_copy):
        copy.wait()
    for g in range(1, stages):
        own_wait(g)
    slow = coef_ref[...]
    coef_ref[...] = -8.0 * (jnp.maximum(-slow, 0.0) + jnp.log1p(jnp.exp(-jnp.abs(slow))))

    def norm_rows(source, h, at):
        rows = pl.ds(at, chunk)
        values = source[rows, :].astype(jnp.float32)
        xm[h, rows, :] = normed(values, gains[0]).astype(jnp.bfloat16)

    @pl.loop(0, half // chunk)
    def _(i):
        norm_rows(mine, 0, pl.multiple_of(i * chunk, chunk))

    length = 2 * half
    for b in range(blocks):
        pad[b, 0:8, :] = jnp.zeros((8, width), jnp.float32)
        pad[b, 8 + length : 16 + length, :] = jnp.zeros((8, width), jnp.float32)

    done0 = per_stage + head
    ticks(PIECES, done0)

    @pl.loop(0, chips)
    def _(slot):
        near_wait(0, slot)

    @pl.loop(0, chips)
    def _(chip):
        src = shard_rows(0, chip, core).at[:, pl.ds(2 * channels, channels)]
        dst = far_out.at[pl.ds(pl.multiple_of((chip * 2 + core) * depth, depth), depth), :]
        remote(src, dst, cross_send.at[0], cross_recv.at[0], across).start()

    prows = 256
    scan0 = done0 + 2 * (2 * (half // prows) - 1) + 1

    @pl.loop(0, 2)
    def _(h):
        @pl.loop(0, half // prows)
        def _(i):
            at = pl.multiple_of(i * prows, prows)

            @pl.when(h == 1)
            def _():
                @pl.loop(0, prows // token_rows)
                def _(q):
                    n = i * (prows // token_rows) + q
                    rows = pl.ds(pl.multiple_of(n * token_rows, token_rows), token_rows)
                    remote(
                        tokens_ref.at[rows, :],
                        other.at[rows, :],
                        tok_send.at[0],
                        tok_recv.at[n],
                        across,
                    ).wait_recv()

                @pl.loop(0, prows // chunk)
                def _(q):
                    norm_rows(other, 1, pl.multiple_of(at + q * chunk, chunk))

                @pl.when(i == half // prows - 1)
                def _():
                    tick(scan0 - 1)

            x = xm[h, pl.ds(at, prows), :]
            side = jnp.where(h == 0, column, 1 - column)
            base = pl.multiple_of(8 + side * half + at, 8)
            for b in range(blocks):
                lanes = slice(b * width, (b + 1) * width)
                branch = jnp.dot(x, full[0, :, lanes], preferred_element_type=jnp.float32)
                pad[b, pl.ds(base, prows), :] = branch.astype(jnp.bfloat16).astype(jnp.float32)
                lanes = slice(channels + b * width, channels + (b + 1) * width)
                gelu_in = jnp.dot(x, full[0, :, lanes], preferred_element_type=jnp.float32)
                gelu_in = gelu_in.astype(jnp.bfloat16).astype(jnp.float32)
                gel[h, b, pl.ds(at, prows), :] = jax.nn.gelu(gelu_in).astype(jnp.bfloat16)

            @pl.when(h * (half // prows) + i < 2 * (half // prows) - 1)
            def _():
                ticks(done0 + h * 4 + i * 2, done0 + h * 4 + i * 2 + 2)

    parts = width // group
    steps = length // SEGMENTS
    pitch = steps + PITCH_PAD
    crows = 256

    quarter = half // 2

    def hid_copies(b, h):
        copies = []
        for r in range(2):
            rows = pl.ds(r * quarter, quarter)
            copies.append(
                remote(
                    hid.at[b, h, rows, :],
                    got.at[b, h, rows, :],
                    hid_send.at[0],
                    hid_recv.at[b, h, r],
                    across,
                )
            )
        return copies

    @pl.loop(0, blocks)
    def _(b):
        at = scan0 + b * SCAN_TICKS
        count = 0
        for n in range(parts):
            lanes = slice(n * group, (n + 1) * group)
            table = pl.ds(pl.multiple_of(b * width + n * group, group), group)
            taps = conv_ref[:, table].astype(jnp.float32)
            coef = coef_ref[:, table]
            for start in range(0, length, crows):
                summed = taps[0:1] * pad[b, 6 + start : 6 + start + crows, lanes]
                for j in range(1, 4):
                    first = 6 + j + start
                    summed = summed + taps[j : j + 1] * pad[b, first : first + crows, lanes]
                conv = summed.astype(jnp.bfloat16)
                wide = conv.astype(jnp.float32)
                for d, (a_ref, u_ref) in enumerate(((a0, u0), (a1, u1))):
                    gate = jnp.dot(
                        conv,
                        gates_ref[b * parts + n, :, 2 * d * group : 2 * (d + 1) * group],
                        preferred_element_type=jnp.float32,
                    )
                    rate = jax.nn.sigmoid(gate[:, :group])
                    inflow = jax.nn.sigmoid(gate[:, group:])
                    log_retain = rate * coef[d : d + 1]
                    retain = jnp.exp(log_retain)
                    left = one_minus_exp(2.0 * log_retain, retain * retain)
                    feed = jnp.sqrt(left) * inflow * wide
                    for q in range(crows // steps):
                        first = (start // steps + q) * pitch
                        a_ref[n, first : first + steps, :] = retain[q * steps : (q + 1) * steps]
                        u_ref[n, first : first + steps, :] = feed[q * steps : (q + 1) * steps]
                if (start // crows) % 2 == 1:
                    tick(at + count)
                    count += 1

        def step(t, carry):
            out = []
            for (state, decayed), (a_ref, u_ref), when in (
                (carry[0], (a0, u0), t),
                (carry[1], (a1, u1), steps - 1 - t),
            ):
                where = pl.ds(when, SEGMENTS, stride=pitch)
                nstate, ndecayed = [], []
                for n in range(parts):
                    retain = a_ref[n, where, :]
                    h = retain * state[n] + u_ref[n, where, :]
                    p = retain * decayed[n]
                    u_ref[n, where, :] = h
                    a_ref[n, where, :] = p
                    nstate.append(h)
                    ndecayed.append(p)
                out.append((tuple(nstate), tuple(ndecayed)))
            return tuple(out)

        zero = tuple(jnp.zeros((SEGMENTS, group), jnp.float32) for n in range(parts))
        one = tuple(jnp.ones((SEGMENTS, group), jnp.float32) for n in range(parts))
        ended = ((zero, one), (zero, one))
        for run in range(2):
            first, last = run * steps // 2, (run + 1) * steps // 2
            ended = lax.fori_loop(first, last, step, ended, unroll=8)
            if run == 0:
                tick(at + count)
                count += 1
        per_half = SEGMENTS // 2
        for n in range(parts):
            lanes = slice(n * group, (n + 1) * group)
            blank = jnp.zeros((1, group), jnp.float32)
            entry = [[None] * SEGMENTS, [None] * SEGMENTS]
            for d, order in ((0, range(SEGMENTS)), (1, range(SEGMENTS - 1, -1, -1))):
                carry = blank
                for s in order:
                    entry[d][s] = carry
                    carry = ended[d][0][n][s : s + 1] + ended[d][1][n][s : s + 1] * carry
            for s in range(SEGMENTS):
                rows = slice(s * pitch, s * pitch + steps)
                local = slice((s % per_half) * steps, (s % per_half + 1) * steps)
                which = jnp.where(column == s // per_half, 0, 1)
                forward = u0[n, rows, :] + a0[n, rows, :] * entry[0][s]
                backward = u1[n, rows, :] + a1[n, rows, :] * entry[1][s]
                gate = gel[which, b, local, lanes].astype(jnp.float32)
                hid[b, which, local, lanes] = (gate * (forward + backward)).astype(jnp.bfloat16)
        tick(at + count)
        count += 1
        assert count == SCAN_TICKS
        for copy in hid_copies(b, 0):
            copy.start()

    for b in range(blocks):
        for copy in hid_copies(b, 1):
            copy.start()
    out0 = scan0 + blocks * SCAN_TICKS


    whole = slice(0, half)

    def mixed(h, own_blocks, far_blocks, fresh, e0=0, count=0, tall=whole, ocols=512):
        left = [hid[b, h, tall] for b in own_blocks]
        left = jnp.concatenate(left, axis=1) if left else None
        right = [got[b, 1 - h, tall] for b in far_blocks]
        right = jnp.concatenate(right, axis=1) if right else None
        parts_n = model // ocols

        @pl.loop(0, parts_n)
        def _(n):
            rows = pl.ds(pl.multiple_of(n * ocols, ocols), ocols)
            lanes = rows
            summed = None if fresh else total[tall, lanes]
            if left is not None:
                first = 2 * channels + own_blocks[0] * width
                term = matmul_t(left, full[0, rows, first : first + len(own_blocks) * width])
                summed = term if summed is None else summed + term
            if right is not None:
                first = far_blocks[0] * width
                term = matmul_t(right, far_out[rows, first : first + len(far_blocks) * width])
                summed = term if summed is None else summed + term
            total[tall, lanes] = summed
            if count:
                every_n = parts_n // count

                @pl.when(n % every_n == every_n - 1)
                def _():
                    tick(e0 + n // every_n)

    def settle(h, source, tall=whole):
        @pl.loop(tall.start // chunk, tall.stop // chunk)
        def _(i):
            rows = pl.ds(pl.multiple_of(i * chunk, chunk), chunk)
            stream = source[rows, :].astype(jnp.float32)
            residual = stream + normed(total[rows, :], gains[1])
            residual = residual.astype(jnp.bfloat16)
            if h == 0:
                source[rows, :] = residual
            middle = normed(residual.astype(jnp.float32), gains[2])
            xm[h, rows, :] = middle.astype(jnp.bfloat16)

    all_blocks = tuple(range(blocks))
    mixed(1, all_blocks, (), True, out0, 2)
    tick(out0 + 2)

    ref = far_out.at[pl.ds(0, chips * depth), :]
    remote(ref, ref, cross_send.at[0], cross_recv.at[0], across).wait_recv()

    @pl.loop(0, chips)
    def _(chip):
        ref = far_out.at[pl.ds(pl.multiple_of((chip * 2 + core) * depth, depth), depth), :]
        remote(ref, ref, share_send.at[0], share_recv.at[0], partner).start()

    ffn0 = out0 + 3
    for b in all_blocks[:-1]:
        ticks(ffn0, ffn0 + 2)
        for copy in hid_copies(b, 0):
            copy.wait_recv()
        if b == 0:
            ref = far_out.at[pl.ds(0, chips * depth), :]
            remote(ref, ref, share_send.at[0], share_recv.at[0], partner).wait_recv()
        mixed(1, (), (b,), False, ffn0 + 2, 1)
        ffn0 += 3
    for r, copy in enumerate(hid_copies(blocks - 1, 0)):
        tall = slice(r * quarter, (r + 1) * quarter)
        copy.wait_recv()
        if r == 1:
            tick(ffn0)
            ffn0 += 1
        mixed(1, (), (blocks - 1,), False, tall=tall, ocols=model // 2)
        if r == 0:
            tick(ffn0)
            ffn0 += 1
        settle(1, other, tall)

    def activate(g, h, c, product):
        lanes = pl.ds(pl.multiple_of((g - 1) * cut + c * ucols, ucols), ucols)
        hidden = jax.nn.silu(product[:, :ucols]) * product[:, ucols:]
        hf[h, :, lanes] = hidden.astype(jnp.bfloat16)

    def expand(g, h, c):
        lanes = pl.ds(pl.multiple_of(2 * c * ucols, 2 * ucols), 2 * ucols)
        activate(g, h, c, jnp.dot(xm[h], full[g, :, lanes], preferred_element_type=jnp.float32))

    first_done = 2 * per_stage + head
    second_done = 3 * per_stage + head
    ticks(min(ffn0, first_done), first_done)
    ffn1 = max(ffn0, first_done)

    @pl.loop(0, chips)
    def _(slot):
        near_wait(1, slot)

    def feature_chip(slot):
        d = (slot + 1) // 2
        return chip_at(jnp.where(slot % 2 == 1, -d, d))

    def expand_part(g, h, c, slots, fresh, last):
        rows = [pl.ds(pl.multiple_of(feature_chip(slot) * span, span), span) for slot in slots]
        x = jnp.concatenate([xm[h, :, at] for at in rows], axis=1)
        lanes = pl.ds(pl.multiple_of(2 * c * ucols, 2 * ucols), 2 * ucols)
        w = jnp.concatenate([full[g, at, lanes] for at in rows], axis=0)
        term = jnp.dot(x, w, preferred_element_type=jnp.float32)
        if not fresh:
            term = total[:, lanes] + term
        if last:
            activate(g, h, c, term)
        else:
            total[:, lanes] = term

    ffn2 = ffn1 + 2
    before = second_done - PIECES // 2
    parts_b = (tuple(range(chips - 3)), (chips - 3, chips - 2), (chips - 1,))

    @pl.loop(0, unit_chunks)
    def _(c):
        expand(1, 1, c)

        @pl.when(c < 2)
        def _():
            tick(ffn1 + c)

    for slot in parts_b[0]:
        near_wait(2, slot)

    @pl.loop(0, unit_chunks)
    def _(c):
        expand_part(2, 1, c, parts_b[0], True, False)

        @pl.when(c == 0)
        def _():
            tick(ffn2)

        @pl.when(c == 1)
        def _():
            ticks(ffn2 + 1, before)

        @pl.when(c == 2)
        def _():
            tick(before)

    for n in (1, 2):
        if n == 2:
            tick(before + 1)
        for slot in parts_b[n]:
            near_wait(2, slot)
        for c in range(unit_chunks):
            expand_part(2, 1, c, parts_b[n], False, n == 2)

    def partial_of(h, chip):
        weight = full[stages - 1, pl.ds(pl.multiple_of(chip * span, span), span), :]
        return matmul_t(hf[h], weight)

    def back_copy(slot):
        chip = feature_chip(slot)
        return remote(part.at[chip], back.at[chip], back_send.at[0], back_recv.at[slot], across)

    distance1 = (stages - 1) * per_stage + head

    def last_copy(i):
        chip = feature_chip(chips - 1)
        rows = pl.ds(pl.multiple_of(i * chunk, chunk), chunk)
        return remote(
            part.at[chip, rows, :],
            back.at[chip, rows, :],
            back_send.at[0],
            back_recv.at[chips - 1 + i],
            across,
        )

    def send_back(slot):
        near_wait(stages - 1, slot)
        chip = feature_chip(slot)
        part[chip] = partial_of(1, chip).astype(jnp.bfloat16)
        if isinstance(slot, int) and slot == chips - 1:
            for i in range(half // chunk):
                last_copy(i).start()
        else:
            back_copy(slot).start()

    def send_pair(d):
        @pl.loop(2 * d - 1, 2 * d + 1)
        def _(slot):
            send_back(slot)

    send_back(0)
    for b in all_blocks:
        for copy in hid_copies(b, 1):
            copy.wait_recv()
    mixed(0, all_blocks, (), True, distance1, PIECES)
    send_pair(1)
    mixed(0, (), all_blocks, False, distance1 + PIECES, 2)
    settle(0, mine)
    tick(distance1 + PIECES + 2)

    @pl.loop(0, unit_chunks)
    def _(c):
        expand(1, 0, c)

        @pl.when(c == 1)
        def _():
            tick(distance1 + PIECES + 3)

    send_pair(2)

    @pl.loop(0, unit_chunks)
    def _(c):
        expand(2, 0, c)
        tick(distance1 + 2 * PIECES + c)

    ticks(distance1 + 2 * PIECES + unit_chunks, distance1 + 3 * PIECES)
    send_pair(3)
    ticks(stages * per_stage + PIECES, stages * per_stage + head)
    send_back(chips - 1)

    @pl.loop(0, chips)
    def _(chip):
        lanes = pl.ds(pl.multiple_of(chip * span, span), span)
        total[:, lanes] = partial_of(0, chip).astype(jnp.bfloat16).astype(jnp.float32)

    squares[...] = jnp.zeros_like(squares)

    def add_back(slot, i):
        chip = feature_chip(slot)
        lanes = pl.ds(pl.multiple_of(chip * span, span), span)
        rows = pl.ds(pl.multiple_of(i * chunk, chunk), chunk)
        summed = total[rows, lanes] + back[chip, rows, :].astype(jnp.float32)
        total[rows, lanes] = summed
        square = summed * summed
        folded = square[:, :128]
        for at in range(128, span, 128):
            folded = folded + square[:, at : at + 128]
        squares[rows, :] += folded

    @pl.loop(0, chips - 1)
    def _(slot):
        back_copy(slot).wait_recv()

        @pl.loop(0, half // chunk)
        def _(i):
            add_back(slot, i)

    @pl.loop(0, half // chunk)
    def _(i):
        last_copy(i).wait_recv()
        add_back(chips - 1, i)
        rows = pl.ds(pl.multiple_of(i * chunk, chunk), chunk)
        mean = jnp.sum(squares[rows, :], axis=-1, keepdims=True) * (1.0 / model)
        scaled = total[rows, :] * lax.rsqrt(mean + EPS) * gains[3]
        middle = mine[rows, :].astype(jnp.float32)
        mine[rows, :] = (middle + scaled).astype(jnp.bfloat16)
        pltpu.make_async_copy(mine.at[rows, :], out_ref.at[rows, :], out_sem.at[0]).start()

    for g in range(stages):
        rows = full.at[g, pl.ds(0, (reach - 1) * depth + depth // 2), :]
        for way in range(2):
            remote(
                rows, rows, ring_send.at[way, g], ring_recv.at[g, 0, 0], targets[way]
            ).wait_send()
        rows = full.at[g, pl.ds(0, chips * depth), :]
        remote(rows, rows, near_send.at[g], near_recv.at[g, 0], partner).wait_send()
    remote(mine, other, tok_send.at[0], tok_recv.at[0], across).wait_send()
    ref = far_out.at[pl.ds(0, chips * depth), :]
    remote(ref, ref, cross_send.at[0], cross_recv.at[0], across).wait_send()
    remote(ref, ref, share_send.at[0], share_recv.at[0], partner).wait_send()
    remote(hid, got, hid_send.at[0], hid_recv.at[0, 0, 0], across).wait_send()
    remote(part, back, back_send.at[0], back_recv.at[0], across).wait_send()
    pltpu.make_async_copy(mine, out_ref, out_sem.at[0]).wait()


def store_kernel(source_ref, out_ref, held, in_sem, out_sem):
    count = held.shape[0]
    rows = held.shape[1]
    pieces = [pl.ds(i * rows, rows) for i in range(count)]
    loads = [
        pltpu.make_async_copy(source_ref.at[at, :], held.at[i], in_sem.at[i])
        for i, at in enumerate(pieces)
    ]
    stores = [
        pltpu.make_async_copy(held.at[i], out_ref.at[at, :], out_sem.at[i])
        for i, at in enumerate(pieces)
    ]
    for load in loads:
        load.start()
    for load, store in zip(loads, stores):
        load.wait()
        store.start()
    for store in stores:
        store.wait()


def store(values):
    rows, model = values.shape
    count = 8
    hbm = pl.BlockSpec(memory_space=pl.ANY)
    return pl.pallas_call(
        store_kernel,
        out_shape=jax.ShapeDtypeStruct(values.shape, values.dtype),
        in_specs=[hbm],
        out_specs=hbm,
        scratch_shapes=[
            pltpu.VMEM((count, rows // count, model), values.dtype),
            pltpu.SemaphoreType.DMA((count,)),
            pltpu.SemaphoreType.DMA((count,)),
        ],
    )(values)


def paired_device(
    tokens,
    pre_mix_gain,
    post_mix_gain,
    pre_ffn_gain,
    post_ffn_gain,
    w_branch,
    w_gelu,
    conv_weight,
    w_rec,
    w_inp,
    decay,
    out_weight_t,
    w_gate,
    w_up,
    down_weight_t,
):
    half, model = tokens.shape
    depth, channels = w_branch.shape
    units = w_gate.shape[1]
    size = lax.axis_size("fs")
    chips = size // 2
    group = w_rec.shape[2]
    width = min(256, channels)
    blocks = channels // width
    length = 2 * half
    bf16 = functools.partial(pltpu.VMEM, dtype=jnp.bfloat16)
    f32 = functools.partial(pltpu.VMEM, dtype=jnp.float32)
    dma = pltpu.SemaphoreType.DMA
    stages = 4
    groups = channels // group
    reach = chips // 2
    hbm = pl.BlockSpec(memory_space=pl.ANY)
    gains = (pre_mix_gain, post_mix_gain, pre_ffn_gain, post_ffn_gain)
    result = pl.pallas_call(
        functools.partial(layer_kernel, size),
        out_shape=jax.ShapeDtypeStruct((half, model), jnp.bfloat16),
        in_specs=[hbm] * 15,
        out_specs=hbm,
        scratch_shapes=[
            bf16((half, model)),
            f32((4, 1, model)),
            bf16(conv_weight.shape),
            bf16((groups, group, 4 * group)),
            f32(decay.shape),
            bf16((stages, model, 3 * channels)),
            bf16((model, channels)),
            bf16((half, model)),
            bf16((2, half, model)),
            f32((blocks, length + 16, width)),
            bf16((2, blocks, half, width)),
        ]
        + [f32((width // group, length + SEGMENTS * PITCH_PAD, group)) for i in range(4)]
        + [
            bf16((blocks, 2, half, width)),
            bf16((blocks, 2, half, width)),
            f32((half, model)),
            f32((half, 128)),
            bf16((2, half, units)),
            bf16((chips, half, 2 * depth)),
            bf16((chips, half, 2 * depth)),
            dma((2, stages)),
            dma((stages, reach, PIECES)),
            dma((stages,)),
            dma((stages, chips)),
            dma((stages,)),
            dma((10,)),
            dma((1,)),
            dma((1,)),
            dma((1,)),
            dma((TOKEN_PIECES,)),
            dma((1,)),
            dma((1,)),
            dma((1,)),
            dma((1,)),
            dma((1,)),
            dma((blocks, 2, 2)),
            dma((1,)),
            dma((chips - 1 + half // 128,)),
        ],
        compiler_params=pltpu.CompilerParams(
            collective_id=0, has_side_effects=True, vmem_limit_bytes=MOST_VMEM
        ),
        cost_estimate=pl.CostEstimate(
            flops=1 << 34, bytes_accessed=1 << 26, transcendentals=1 << 24
        ),
    )(
        tokens,
        w_branch,
        w_gelu,
        out_weight_t,
        w_gate,
        w_up,
        down_weight_t,
        *(gain.reshape(1, model) for gain in gains),
        conv_weight,
        w_rec,
        w_inp,
        decay,
    )
    return store(result)


def wide_device(
    tokens,
    pre_mix_gain,
    post_mix_gain,
    pre_ffn_gain,
    post_ffn_gain,
    w_branch,
    w_gelu,
    conv_weight,
    w_rec,
    w_inp,
    decay,
    out_weight_t,
    w_gate,
    w_up,
    down_weight_t,
):
    channels = conv_weight.shape[1]
    mix_shard = jnp.concatenate([w_branch, w_gelu, out_weight_t], axis=1)
    ffn_shard = jnp.concatenate([w_gate, w_up, down_weight_t], axis=1)
    stream = tokens.astype(jnp.float32)
    normed_in = normed(stream, pre_mix_gain).astype(jnp.bfloat16)
    mix_all = lax.all_gather(mix_shard, "fs", axis=0, tiled=True)
    whole = lax.all_gather(normed_in, "tp", axis=0, tiled=True)
    ffn_all = lax.all_gather(ffn_shard, "fs", axis=0, tiled=True)
    out_own = mix_all[:, 2 * channels :]
    hidden = mixer(whole, mix_all, conv_weight, w_rec, w_inp, decay)
    own_hidden = lax.all_to_all(hidden, "tp", split_axis=0, concat_axis=1, tiled=True)
    out_whole = lax.all_gather(out_own, "tp", axis=1, tiled=True)
    mixer_sum = matmul_t(own_hidden, out_whole)
    residual = (stream + normed(mixer_sum, post_mix_gain)).astype(jnp.bfloat16)
    middle = residual.astype(jnp.float32)
    normed_mid = normed(middle, pre_ffn_gain).astype(jnp.bfloat16)
    all_mid = lax.all_gather(normed_mid, "tp", axis=0, tiled=True)
    ffn_sum = lax.psum_scatter(
        ffn(all_mid, ffn_all), "tp", scatter_dimension=0, tiled=True
    ).astype(jnp.float32)
    return (middle + normed(ffn_sum, post_ffn_gain)).astype(jnp.bfloat16)


def solution(mesh):
    return jax.shard_map(
        paired_device if mesh.shape["tp"] == 2 else wide_device,
        mesh=mesh,
        in_specs=(
            P(("fs", "tp"), None),
            P(),
            P(),
            P(),
            P(),
            P("fs", "tp"),
            P("fs", "tp"),
            P(None, "tp"),
            P(None, "tp", None, None),
            P(None, "tp", None, None),
            P(None, "tp"),
            P("fs", "tp"),
            P("fs", "tp"),
            P("fs", "tp"),
            P("fs", "tp"),
        ),
        out_specs=P(("fs", "tp"), None),
        check_vma=False,
    )
```
